256 devices in a mesh: kv: 32 (over z, x), tp: 8 (over y, core).
Axes of the slice: x: 4, y: 4, z: 8, core: 2. Of those that a mesh axis runs over, the one named last changes fastest.
Arguments:
- tokens: bfloat16 [384, 2048], P(None, 'kv'), may hold values from -40 to 40
- norm_gain: float32 [2048], P('kv'), may hold values from 0.1 to 1.9
- w_query: bfloat16 [2048, 1024], P('kv', 'tp'), may hold values from -0.088388348 to 0.088388348
- w_key: bfloat16 [2048, 1024], P('kv', 'tp'), may hold values from -0.125 to 0.125
- w_value: bfloat16 [2048, 1024], P('kv', 'tp'), may hold values from -0.125 to 0.125
- w_gate: bfloat16 [2048, 16], replicated, may hold values from -0.125 to 0.125
- gate_bias: float32 [16], replicated, may hold values from -1 to 3
- w_out: bfloat16 [1024, 2048], P('tp', 'kv'), may hold values from -0.1875 to 0.1875
- keys_cache: bfloat16 [24, 16384, 1024], P(None, 'kv', 'tp'), may hold values from -512 to 512
- values_cache: bfloat16 [24, 16384, 1024], P(None, 'kv', 'tp'), may hold values from -6 to 6
- cum_gates: float32 [24, 16, 16384], P(None, 'tp', 'kv'), may hold values from -16784 to 0, as said below
- prior_len: int32 [24], replicated, may hold values from 8192 to 16362, as said below
- accepted: int32 [24], replicated, may hold values from 0 to 6
- parents: int32 [24, 16], replicated, may hold values from -1 to 14, as said below
Outputs:
- mixed_rows: bfloat16 [384, 2048], P('tp', 'kv')
- keys_out: bfloat16 [24, 16384, 1024], P(None, 'kv', 'tp')
- values_out: bfloat16 [24, 16384, 1024], P(None, 'kv', 'tp')
The draws below stay inside these ranges and needn't reach their ends.
Inputs may be any that keep to these rules, and one draw needn't show every extreme that they name: parents[b, 0] = -1 and 0 <= parents[b, j] < j for later j. prior_len is at least half of 16384, and prior_len + accepted + 16 <= 16384. `cum_gates`: non-increasing along positions.
All inputs are finite; a program needn't handle non-finite values.
Results may differ from the reference program's by a relative error of at most 0.04.
Values may be sent and summed in bfloat16 or wider, within the bound.
No kernel may reach another device: no remote copies, remote signals or barrier semaphores. Data moves between devices by JAX's collectives and lax.ppermute only.
A program may use at most 64 MiB of HBM per device.

```python
import jax
import jax.numpy as jnp
from jax import lax

D = 2048
H = 16
HEAD = 64
PROPS = 16
MOST_ACCEPTED = 6
SEQUENCE_TOTAL = 24
LEN_DEV = 512
CACHE_POSITIONS = 16384
ROWS = 384
N_KV = 32
N_TP = 8


def token_floats(token_key):
    random_keys = jax.random.split(token_key, 3)
    normal_part = jax.random.normal(random_keys[0], (ROWS, D), jnp.float32)
    row_scale = jnp.exp(jax.random.uniform(random_keys[1], (ROWS, 1), jnp.float32, jnp.log(0.3), jnp.log(3.0)))
    column_rise = jnp.exp(jnp.log(3.0) * jnp.arange(D, dtype=jnp.float32)[None, :] / D)
    column_spread = jnp.exp(jax.random.uniform(random_keys[2], (1, D), jnp.float32, jnp.log(0.5), jnp.log(2.0)))
    return jnp.clip(normal_part * row_scale * column_rise * column_spread, -40.0, 40.0)


def query_floats(weight_key):
    drawn = jax.random.truncated_normal(weight_key, -4.0, 4.0, (D, H * HEAD), jnp.float32)
    return drawn * D ** (-0.5)


def draw_tokens(key, part):
    return token_floats(jax.random.fold_in(key, 101)).astype(jnp.bfloat16)


def draw_w_query(key, part):
    return query_floats(jax.random.fold_in(key, 202)).astype(jnp.bfloat16)


def draw_keys_cache(key, part):
    random_keys = jax.random.split(jax.random.fold_in(key, 303), 1)
    result = jax.random.normal(random_keys[0], (SEQUENCE_TOTAL, CACHE_POSITIONS, H * HEAD), jnp.float32)
    result = jnp.clip(result, -6.0, 6.0)
    return jnp.clip(result, -512.0, 512.0).astype(jnp.bfloat16)


def draw_cum_gates(key, part):
    random_keys = jax.random.split(key, 8)
    ranking = jax.random.permutation(random_keys[0], H)
    quick_count = H // 2
    fast_decay_heads = (ranking < quick_count)[None, :, None]
    quick_rate = jnp.exp(jax.random.uniform(random_keys[1], (SEQUENCE_TOTAL, H, 1), jnp.float32, jnp.log(1.0 / 100.0), jnp.log(1.0 / 30.0)))
    slow_rate = jnp.exp(jax.random.uniform(random_keys[2], (SEQUENCE_TOTAL, H, 1), jnp.float32, jnp.log(0.1), jnp.log(0.4))) / CACHE_POSITIONS
    decay_rates = jnp.where(fast_decay_heads, quick_rate, slow_rate)
    block_count = CACHE_POSITIONS // LEN_DEV
    block_multiplier = jnp.exp(jax.random.uniform(random_keys[3], (SEQUENCE_TOTAL, 1, block_count, 1), jnp.float32, 0.0, jnp.log(4.0)))
    block_multiplier = jnp.broadcast_to(block_multiplier, (SEQUENCE_TOTAL, 1, block_count, LEN_DEV)).reshape(SEQUENCE_TOTAL, 1, CACHE_POSITIONS)
    jitter_level = jax.random.uniform(random_keys[4], (SEQUENCE_TOTAL, H, CACHE_POSITIONS), jnp.float32, 0.4, 1.6)
    spike_position = jax.random.randint(random_keys[5], (SEQUENCE_TOTAL, 1, CACHE_POSITIONS), 0, CACHE_POSITIONS) < 2
    dropped_fraction = jax.random.uniform(random_keys[6], (SEQUENCE_TOTAL, H, CACHE_POSITIONS), jnp.float32, 0.2, 0.5)
    spike_events = jnp.where(spike_position & jnp.logical_not(fast_decay_heads), jnp.log(1.0 - dropped_fraction), 0.0)
    gate_increments = spike_events - decay_rates * block_multiplier * jitter_level
    head_offset = jax.random.uniform(random_keys[7], (SEQUENCE_TOTAL, H, 1), jnp.float32, 0.0, 320.0)
    return (jnp.cumsum(gate_increments, axis=2) - head_offset).astype(jnp.float32)


def draw_prior_len(key, part):
    return jax.random.randint(key, (SEQUENCE_TOTAL,), CACHE_POSITIONS // 2, CACHE_POSITIONS - PROPS - MOST_ACCEPTED + 1, dtype=jnp.int32)


def draw_parents(key, part):
    columns = jnp.arange(PROPS, dtype=jnp.int32)
    random_bits = jax.random.randint(key, (SEQUENCE_TOTAL, PROPS), 0, 1 << 20, dtype=jnp.int32)
    picked = random_bits % jnp.maximum(columns, 1)[None, :]
    return jnp.where(columns[None, :] == 0, -1, picked).astype(jnp.int32)


def set_ends(values, own_key, smallest, largest):
    place = [jax.random.randint(jax.random.fold_in(own_key, axis), (), 0, length) for axis, length in enumerate(values.shape)]
    longest = values.shape.index(max(values.shape))
    next_to = place[:longest] + [(place[longest] + 1) % values.shape[longest]] + place[longest + 1:]
    return values.at[tuple(place)].set(smallest).at[tuple(next_to)].set(largest)


def steps_of(key, shape, pieces, least, high):
    loudness = 1.0
    for axis_at, parts in pieces:
        heights = jax.random.uniform(jax.random.fold_in(jax.random.fold_in(key, 6), axis_at), (parts,), jnp.float32, least / len(pieces), high / len(pieces))
        loudness = loudness * jnp.repeat(jnp.exp(heights), shape[axis_at] // parts).reshape((-1,) + (1,) * (len(shape) - 1 - axis_at))
    return loudness


def centred(stream_key, extent, spread, limit, cuts=(), held_as=jnp.bfloat16):
    values = jax.random.normal(stream_key, extent, jnp.float32) * spread
    if len(cuts) > 0:
        values = steps_of(stream_key, extent, cuts, -0.22, 0.18) * values
    return jnp.clip(values, min=-limit, max=limit).astype(held_as)


def setup_inputs(seed: int = 0) -> dict:
    streams_of = jax.random.split(jax.random.key(seed), 15)
    tokens = draw_tokens(jax.random.fold_in(streams_of[14], 71), 0)
    norm_gain = jnp.clip(1.0 + 0.18 * jax.random.normal(streams_of[1], (D,), jnp.float32), 0.1, 1.9)
    w_query = draw_w_query(jax.random.fold_in(streams_of[14], 71), 0)
    w_key = centred(streams_of[3], (D, H * HEAD), D ** -0.5, 0.125, ((0, 32), (1, 8)))
    w_value = centred(streams_of[4], (D, H * HEAD), D ** -0.5, 0.125, ((0, 32), (1, 8)))
    w_gate = centred(streams_of[5], (D, H), D ** -0.5, 0.125)
    gate_bias = jnp.clip(jax.random.uniform(streams_of[6], (H,), jnp.float32, -1.0, 3.0), -1.0, 3.0)
    w_out = centred(streams_of[7], (H * HEAD, D), (H * HEAD) ** -0.5, 0.1875, ((0, 8), (1, 32)))
    keys_cache = draw_keys_cache(jax.random.fold_in(streams_of[14], 71), 0)
    values_cache = centred(streams_of[9], (SEQUENCE_TOTAL, CACHE_POSITIONS, H * HEAD), 1.0, 6.0, ((1, 32), (2, 8)))
    cum_gates = draw_cum_gates(jax.random.fold_in(streams_of[14], 71), 0)
    prior_len = draw_prior_len(jax.random.fold_in(streams_of[14], 71), 0)
    accepted = set_ends(jax.random.randint(streams_of[12], (SEQUENCE_TOTAL,), 0, MOST_ACCEPTED + 1), jax.random.fold_in(streams_of[12], 1), 0, MOST_ACCEPTED).astype(jnp.int32)
    parents = draw_parents(jax.random.fold_in(streams_of[14], 71), 0)
    return {"tokens": tokens, "norm_gain": norm_gain, "w_query": w_query, "w_key": w_key, "w_value": w_value, "w_gate": w_gate, "gate_bias": gate_bias, "w_out": w_out, "keys_cache": keys_cache, "values_cache": values_cache, "cum_gates": cum_gates, "prior_len": prior_len, "accepted": accepted, "parents": parents}


masked_score = -1e+30
norm_eps = 1e-06

def ancestry(parents):
    columns = jnp.arange(PROPS, dtype=jnp.int32)
    parent_link = (parents[:, :, None] == columns[None, None, :]).astype(jnp.float32)
    reached = jnp.eye(PROPS, dtype=jnp.float32)[None] + parent_link
    for squaring in range(PROPS.bit_length()):
        reached = jnp.minimum(jnp.einsum('bij,bjk->bik', reached, reached, precision=lax.Precision.HIGHEST), 1.0)
    return reached

def reference(tokens, norm_gain, w_query, w_key, w_value, w_gate, gate_bias, w_out, keys_cache, values_cache, cum_gates, prior_len, accepted, parents):
    floats = tokens.astype(jnp.float32)
    inv_rms = lax.rsqrt(lax.optimization_barrier(jnp.sum(floats * floats, axis=1)) / D + norm_eps)
    scaled = (floats * norm_gain).astype(jnp.bfloat16)

    def project(weight):
        return inv_rms[:, None] * jnp.dot(scaled, weight, preferred_element_type=jnp.float32)
    queries = project(w_query).astype(jnp.bfloat16)
    new_keys = project(w_key).astype(jnp.bfloat16)
    new_values = project(w_value).astype(jnp.bfloat16)
    log_gates = jax.nn.log_sigmoid(project(w_gate) + gate_bias).reshape(SEQUENCE_TOTAL, PROPS, H)
    reached = ancestry(parents)
    tree_gates = jnp.einsum('bij,bjh->bih', reached, log_gates, precision=lax.Precision.HIGHEST)
    filled = prior_len + accepted
    last_pos = filled - 1
    index_last = jnp.broadcast_to(last_pos[:, None, None], (SEQUENCE_TOTAL, H, 1))
    last_gate = jnp.take_along_axis(cum_gates, index_last, axis=2)[:, :, 0]
    prop_cum = last_gate[:, None, :] + tree_gates
    owners = (last_pos // LEN_DEV).astype(jnp.int32)
    scale = HEAD ** (-0.5)

    def attend(packed):
        seq_query, seq_keys, seq_values, seq_cum, seq_newk, seq_newv, seq_prop, seq_reach, seq_fill, seq_owner = packed
        query_f = seq_query.reshape(PROPS, H, HEAD).astype(jnp.float32)
        keys_f = seq_keys.reshape(CACHE_POSITIONS, H, HEAD).astype(jnp.float32)
        scores = jnp.einsum('ihd,phd->hip', query_f, keys_f) * scale - seq_cum[:, None, :]
        positions = jnp.arange(CACHE_POSITIONS, dtype=jnp.int32)
        valid_keys = positions < seq_fill
        scores = jnp.where(valid_keys[None, None, :], scores, masked_score)
        blocked = scores.reshape(H, PROPS, N_KV, LEN_DEV)
        newk_f = seq_newk.reshape(PROPS, H, HEAD).astype(jnp.float32)
        tree_scores = jnp.einsum('ihd,jhd->hij', query_f, newk_f) * scale - jnp.transpose(seq_prop)[:, None, :]
        tree_live = (seq_reach > 0.5)[None]
        tree_scores = jnp.where(tree_live, tree_scores, masked_score)
        is_owner = jnp.arange(N_KV, dtype=jnp.int32) == seq_owner
        block_max = lax.optimization_barrier(jnp.max(blocked, axis=3))
        tree_max = lax.optimization_barrier(jnp.max(tree_scores, axis=2))
        block_max = jnp.where(is_owner[None, None, :], jnp.maximum(block_max, tree_max[:, :, None]), block_max)
        owner_max = lax.optimization_barrier(jnp.max(jnp.where(is_owner[None, None, :], block_max, masked_score), axis=2))
        valid_blocks = valid_keys.reshape(N_KV, LEN_DEV)[None, None]
        weights = jnp.where(valid_blocks, jnp.exp(blocked - block_max[..., None]), 0.0)
        tree_weights = jnp.where(tree_live, jnp.exp(tree_scores - owner_max[:, :, None]), 0.0)
        block_sums = lax.optimization_barrier(jnp.sum(weights, axis=3)) + jnp.where(is_owner[None, None, :], lax.optimization_barrier(jnp.sum(tree_weights, axis=2))[:, :, None], 0.0)
        values_f = seq_values.reshape(N_KV, LEN_DEV, H, HEAD).astype(jnp.float32)
        newv_f = seq_newv.reshape(PROPS, H, HEAD).astype(jnp.float32)
        rounded = lax.optimization_barrier(weights.astype(jnp.bfloat16)).astype(jnp.float32)
        tree_rounded = lax.optimization_barrier(tree_weights.astype(jnp.bfloat16)).astype(jnp.float32)
        block_values = jnp.einsum('hinp,nphd->hind', rounded, values_f)
        tree_values = jnp.einsum('hij,jhd->hid', tree_rounded, newv_f)
        block_values = block_values + jnp.where(is_owner[None, None, :, None], tree_values[:, :, None, :], 0.0)
        block_values = lax.optimization_barrier(block_values.astype(jnp.bfloat16)).astype(jnp.float32)
        top_score = lax.optimization_barrier(jnp.max(block_max, axis=2))
        rescale = jnp.exp(block_max - top_score[..., None])
        grand_total = lax.optimization_barrier(jnp.sum(rescale * block_sums, axis=2))
        result = lax.optimization_barrier(jnp.sum(rescale[..., None] * block_values, axis=2)) / grand_total[..., None]
        return jnp.transpose(result, (1, 0, 2)).astype(jnp.bfloat16)
    packed = (queries.reshape(SEQUENCE_TOTAL, PROPS, H * HEAD), keys_cache, values_cache, cum_gates, new_keys.reshape(SEQUENCE_TOTAL, PROPS, H * HEAD), new_values.reshape(SEQUENCE_TOTAL, PROPS, H * HEAD), prop_cum, reached, filled, owners)
    attended = lax.map(attend, packed).reshape(ROWS, H * HEAD)
    group = H // N_TP * HEAD
    parted = attended.reshape(ROWS, N_TP, group).astype(jnp.float32)
    weight_groups = w_out.reshape(N_TP, group, D).astype(jnp.float32)
    head_parts = jnp.einsum('rgc,gcd->grd', parted, weight_groups)
    head_parts = lax.optimization_barrier(head_parts.astype(jnp.bfloat16)).astype(jnp.float32)
    mixed_rows = lax.optimization_barrier(jnp.sum(head_parts, axis=0)).astype(jnp.bfloat16)

    def write(cache, new_rows, start):
        return lax.dynamic_update_slice(cache, new_rows, (start.astype(jnp.int32), jnp.zeros((), jnp.int32)))
    keys_out = jax.vmap(write)(keys_cache, new_keys.reshape(SEQUENCE_TOTAL, PROPS, H * HEAD), filled)
    values_out = jax.vmap(write)(values_cache, new_values.reshape(SEQUENCE_TOTAL, PROPS, H * HEAD), filled)
    return (mixed_rows, keys_out, values_out)
```

```python
import jax
import jax.numpy as jnp
from jax import lax
from jax.experimental import pallas as pl
from jax.experimental.pallas import tpu as pltpu
from jax.sharding import Mesh
from jax.sharding import PartitionSpec as P

D = 2048
HEAD = 64
PROPS = 16
ROWS = 384
SEQS = 24
LEN = 512
WIDTH = 128
N_KV = 32
N_TP = 8
STATS = 24
WINDOW = 32
KV = ("kv_0", "kv_1")

masked_score = -1e30
lowest_max = -1e20
norm_eps = 1e-06

VM = pl.BlockSpec(memory_space=pltpu.VMEM)
SM = pl.BlockSpec(memory_space=pltpu.SMEM)
ANY = pl.BlockSpec(memory_space=pl.ANY)
bf16 = jnp.bfloat16
f32 = jnp.float32


def iota(shape, dim):
    return lax.broadcasted_iota(jnp.int32, shape, dim)


def high_low(x):
    high = x.astype(bf16).astype(f32)
    return high, (x - high).astype(bf16).astype(f32)


def dot_t(a, b):
    return lax.dot_general(a, b, (((1,), (1,)), ((), ())), preferred_element_type=f32)


def project_kernel(
    ids, prior, accepted, tokens, gain, w_q, w_k, w_v, w_gate, cum, out, gate_rows, gates, sem
):
    kv, tp = ids[0], ids[1]
    copy = pltpu.make_async_copy(
        w_gate.at[pl.ds(pl.multiple_of(kv * 64, 64), 64)], gate_rows, sem
    )
    copy.start()
    floats = tokens[...].astype(f32)
    scaled = (floats * gain[...]).astype(bf16)
    for n, w in enumerate((w_q, w_k, w_v)):
        part = jnp.dot(scaled, w[...], preferred_element_type=f32).astype(bf16)
        out[0:SEQS, :, n * WIDTH : (n + 1) * WIDTH] = part.reshape(SEQS, PROPS, WIDTH)
    squares = floats * floats
    sq_high, sq_low = high_low(squares)
    ones = jnp.ones((8, 64), bf16)
    square_sum = dot_t(ones, sq_high.astype(bf16)) + dot_t(ones, sq_low.astype(bf16))
    lane = iota((2, WIDTH), 1)
    position = iota((2, LEN), 1)
    last = jnp.zeros((2, WIDTH), f32)
    for b in range(SEQS):
        at = prior[b] + accepted[b] - 1 - kv * LEN
        found = jnp.sum(jnp.where(position == at, cum[b], 0.0), axis=1, keepdims=True)
        last = jnp.where(lane == b, found, last)
    last_high, last_low = high_low(last)
    rest = last - last_high - last_low
    copy.wait()
    gates[...] = lax.dot_general(
        gate_rows[...], scaled, (((0,), (1,)), ((), ())), preferred_element_type=f32
    )
    row = iota((8, ROWS), 0)
    gate_0 = gates[pl.ds(2 * tp, 1), :]
    gate_1 = gates[pl.ds(2 * tp + 1, 1), :]
    stats = jnp.where(row == 0, gate_0, jnp.where(row == 1, gate_1, 0.0))
    stats = jnp.where(row == 2, square_sum, stats)
    wide = jnp.zeros((2, ROWS - WIDTH), f32)
    last = jnp.concatenate([last, wide], axis=1)
    rest = jnp.concatenate([rest, wide], axis=1)
    stats = jnp.where(row == 3, last[0:1], jnp.where(row == 4, last[1:2], stats))
    stats = jnp.where(row == 5, rest[0:1], jnp.where(row == 6, rest[1:2], stats))
    out[STATS] = jnp.concatenate(high_low(stats), axis=0).astype(bf16)
    out[STATS + 1 :] = jnp.zeros((N_KV - STATS - 1, PROPS, ROWS), bf16)


def share_kernel(ids, bias, parts, out):
    kv, tp = ids[0], ids[1]
    total = jnp.zeros((PROPS, ROWS), f32)
    for k in range(N_KV):
        total = total + parts[k].astype(f32)
    stats = total[0:8] + total[8:16]
    row = iota((8, ROWS), 0)
    inv_rms = lax.rsqrt(stats[2:3] / D + norm_eps)
    logits = inv_rms * stats + jnp.where(row == 0, bias[2 * tp], bias[2 * tp + 1])
    log_gates = jnp.minimum(logits, 0.0) - jnp.log1p(jnp.exp(-jnp.abs(logits)))
    stats = jnp.where(row < 2, log_gates, jnp.where(row == 2, inv_rms, stats))
    stats = jnp.concatenate(high_low(stats), axis=0)
    block = jnp.where(kv == STATS, stats, total).astype(bf16)
    for k in range(N_KV):
        out[k] = block


def attention_kernel(
    ids,
    prior,
    accepted,
    parents,
    joined,
    cum,
    keys,
    values,
    out,
    k_buf,
    v_buf,
    columns,
    k_sem,
    v_sem,
):
    kv = ids[0]
    k_copies = []
    v_copies = []
    for t in range(N_TP):
        three = pl.ds(3 * t, 3)
        k_copies.append(pltpu.make_async_copy(keys.at[three], k_buf.at[three], k_sem.at[t]))
        v_copies.append(pltpu.make_async_copy(values.at[three], v_buf.at[three], v_sem.at[t]))
        k_copies[t].start()
        v_copies[t].start()
    coded = joined[STATS].astype(f32)
    columns[...] = jnp.transpose(coded[0:8] + coded[8:16])
    lane = iota((PROPS, WIDTH), 1)
    first_head = lane < HEAD
    lane_out = iota((2 * PROPS, WIDTH), 1)
    row_out = iota((2 * PROPS, WIDTH), 0)
    own_lanes = (lane_out < HEAD) == (row_out < PROPS)
    stat_lane = jnp.where(row_out < PROPS, lane_out - HEAD, lane_out)
    position = iota((2, LEN), 1)
    scale = HEAD**-0.5

    def both_heads(b_rows, b_block):
        inv = columns[b_rows, 2:3]
        q = (inv * joined[b_block, :, 0:WIDTH].astype(f32)).astype(bf16).astype(f32) * scale
        zero = jnp.zeros_like(q)
        return jnp.concatenate(
            [jnp.where(first_head, q, zero), jnp.where(first_head, zero, q)], axis=0
        ).astype(bf16)

    def packed(v, top, total):
        top_high, top_low = high_low(top)
        sum_high, sum_low = high_low(total)
        stats = jnp.where(
            stat_lane == 0,
            top_high,
            jnp.where(stat_lane == 1, top_low, jnp.where(stat_lane == 2, sum_high, sum_low)),
        )
        return jnp.where(own_lanes, v, stats).astype(bf16)

    def sendable(top):
        high, low = high_low(jnp.maximum(top, lowest_max))
        return high + low

    for t in range(N_TP):
        k_copies[t].wait()
        v_copies[t].wait()
        for s in range(3):
            b = 3 * t + s
            q = both_heads(pl.ds(PROPS * b, PROPS), b)
            filled_here = prior[b] + accepted[b] - kv * LEN
            bias = jnp.where(position < filled_here, -cum[b], masked_score)
            bias = jnp.concatenate(
                [
                    jnp.broadcast_to(bias[0:1], (PROPS, LEN)),
                    jnp.broadcast_to(bias[1:2], (PROPS, LEN)),
                ],
                axis=0,
            )
            scores = dot_t(q, k_buf[b]) + bias
            top = sendable(jnp.max(scores, axis=1, keepdims=True))
            weights = jnp.exp(scores - top)
            total = jnp.sum(weights, axis=1, keepdims=True)
            v = jnp.dot(weights.astype(bf16), v_buf[b], preferred_element_type=f32)
            out[t, 32 * s : 32 * s + 32, :] = packed(v, top, total)
        out[t, 96:128, :] = jnp.zeros((32, WIDTH), bf16)

    @pl.when(kv < SEQS)
    def _():
        square = iota((PROPS, WIDTH), 0)
        link = jnp.where(lane == square, 1.0, 0.0)
        for i in range(PROPS):
            link = jnp.where((square == i) & (lane == parents[kv, i]), 1.0, link)
        reached = link
        pad = jnp.zeros((WIDTH - PROPS, WIDTH), f32)
        for _ in range(PROPS.bit_length()):
            other = jnp.concatenate([reached, pad], axis=0).astype(bf16)
            reached = jnp.minimum(
                jnp.dot(reached.astype(bf16), other, preferred_element_type=f32), 1.0
            )
        mine = pl.ds(pl.multiple_of(PROPS * kv, PROPS), PROPS)
        picks = (iota((ROWS, WIDTH), 0) == iota((ROWS, WIDTH), 1) + PROPS * kv) & (
            iota((ROWS, WIDTH), 1) < PROPS
        )
        own_gates = jnp.dot(
            joined[STATS], jnp.where(picks, 1.0, 0.0).astype(bf16), preferred_element_type=f32
        ).astype(bf16)
        tree = dot_t(own_gates, jnp.concatenate([reached, pad], axis=0).astype(bf16))
        tree = tree[0:8] + tree[8:16]
        whole = (coded[0:8] + coded[8:16])[:, 0:WIDTH]
        last = jnp.sum(
            jnp.where(iota((8, WIDTH), 1) == kv, whole, 0.0), axis=1, keepdims=True
        )
        bias = jnp.concatenate(
            [
                jnp.broadcast_to(-(last[3:4] + last[5:6] + tree[0:1]), (PROPS, WIDTH)),
                jnp.broadcast_to(-(last[4:5] + last[6:7] + tree[1:2]), (PROPS, WIDTH)),
            ],
            axis=0,
        )
        q = both_heads(mine, kv)
        inv = columns[mine, 2:3]
        new_keys = inv * joined[kv, :, WIDTH : 2 * WIDTH].astype(f32)
        new_values = inv * joined[kv, :, 2 * WIDTH : 3 * WIDTH].astype(f32)
        new_keys = jnp.concatenate([new_keys, pad], axis=0).astype(bf16)
        new_values = jnp.concatenate([new_values, pad], axis=0).astype(bf16)
        live = jnp.concatenate([reached, reached], axis=0) > 0.5
        scores = jnp.where(live, dot_t(q, new_keys) + bias, masked_score)
        tree_top = jnp.max(scores, axis=1, keepdims=True)
        at = pl.ds(pl.multiple_of(32 * lax.rem(kv, 3), 32), 32)
        held = out[lax.div(kv, 3), at, :].astype(f32)

        def stat(n):
            pick = (stat_lane == n) & jnp.logical_not(own_lanes)
            return jnp.sum(jnp.where(pick, held, 0.0), axis=1, keepdims=True)

        old_top = stat(0) + stat(1)
        old_sum = stat(2) + stat(3)
        top = sendable(jnp.maximum(old_top, tree_top))
        weights = jnp.exp(scores - top)
        keep = jnp.exp(old_top - top)
        total = keep * old_sum + jnp.sum(weights, axis=1, keepdims=True)
        v = keep * held + jnp.dot(
            weights.astype(bf16), new_values, preferred_element_type=f32
        )
        out[lax.div(kv, 3), at, :] = packed(v, top, total)


def combine_kernel(ids, parts, out):
    kv = ids[0]
    head = lax.rem(lax.div(kv, 4), 2)
    start = HEAD * (1 - head)
    row = iota((WIDTH, 2 * WIDTH), 0) - start
    row = row - jnp.where(iota((WIDTH, 2 * WIDTH), 1) < WIDTH, 0, 2)
    spread = jnp.where((row == 0) | (row == 1), 1.0, 0.0).astype(bf16)
    results = []
    for g in range(N_TP):
        block = parts[128 * g : 128 * g + 128]
        stats = jnp.dot(block, spread, preferred_element_type=f32)
        tops = stats[:, 0:WIDTH].reshape(16, 8, WIDTH)
        sums = stats[:, WIDTH:].reshape(16, 8, WIDTH)
        floats = block.astype(f32).reshape(16, 8, WIDTH)
        top = jnp.max(tops, axis=0)
        top = jnp.maximum(top, pltpu.roll(top, 4, 0))
        factor = jnp.exp(tops - top[None])
        above = jnp.sum(factor * floats, axis=0)
        below = jnp.sum(factor * sums, axis=0)
        above = above + pltpu.roll(above, 4, 0)
        below = below + pltpu.roll(below, 4, 0)
        results.append(above / below)
    lane = iota((8, WIDTH), 1)
    first = iota((8, WIDTH), 0) < 4
    pairs = []
    for p in range(4):
        even, odd = results[2 * p], results[2 * p + 1]
        even = jnp.where(head == 0, even, pltpu.roll(even, HEAD, 1))
        odd = jnp.where(head == 1, odd, pltpu.roll(odd, HEAD, 1))
        pairs.append(jnp.where(lane < HEAD, even, odd))
    block = jnp.concatenate(
        [jnp.where(first, pairs[0], pairs[1]), jnp.where(first, pairs[2], pairs[3])], axis=0
    ).astype(bf16)
    for k in range(N_KV):
        out[k] = block


def output_kernel(shared, w_out, out, rows):
    for s in range(3):
        for h in range(2):
            for i in range(4):
                block = shared[8 * s + 4 * h + i].astype(f32)
                for p in range(4):
                    rows[16 * s + 4 * i : 16 * s + 4 * i + 4, pl.ds((2 * p + h) * WIDTH, WIDTH)] = (
                        block[4 * p : 4 * p + 4]
                    )
    total = jnp.zeros((48, 64), f32)
    for p in range(4):
        for h in range(2):
            weight = jnp.concatenate(
                [
                    w_out[2 * p, HEAD * h : HEAD * h + HEAD, :],
                    w_out[2 * p + 1, HEAD * h : HEAD * h + HEAD, :],
                ],
                axis=0,
            )
            block = rows[:, (2 * p + h) * WIDTH : (2 * p + h + 1) * WIDTH].astype(bf16)
            total = total + jnp.dot(block, weight, preferred_element_type=f32)
    out[...] = total.astype(bf16)


def copy_kernel(after, keys, values, keys_out, values_out, sems):
    copies = []
    for n, (source, target) in enumerate(((keys, keys_out), (values, values_out))):
        for t in range(8):
            three = pl.ds(3 * t, 3)
            copies.append(
                pltpu.make_async_copy(source.at[three], target.at[three], sems.at[8 * n + t])
            )
    for copy in copies:
        copy.start()
    for copy in copies:
        copy.wait()


def write_kernel(
    ids, prior, accepted, joined, after, keys_in, values_in, keys, values, buf, columns, in_sem, out_sem
):
    offset = ids[0] * LEN
    coded = joined[STATS].astype(f32)
    columns[...] = jnp.transpose(coded[0:8] + coded[8:16])

    def place(b):
        start = prior[b] + accepted[b] - offset
        base = jnp.clip(lax.div(jnp.maximum(start, 0), 16) * 16, 0, LEN - WINDOW)
        hit = (start > -PROPS) & (start < LEN)
        return start, pl.multiple_of(base, 16), hit

    def copy_in(n, b, base):
        source = (keys, values)[n].at[b, pl.ds(base, WINDOW), :]
        return pltpu.make_async_copy(source, buf.at[n, b], in_sem.at[n, b])

    def copy_out(n, b, base):
        target = (keys, values)[n].at[b, pl.ds(base, WINDOW), :]
        return pltpu.make_async_copy(buf.at[n, b], target, out_sem.at[n, b])

    @pl.loop(0, SEQS)
    def _(b):
        start, base, hit = place(b)

        @pl.when(hit)
        def _():
            for n in range(2):
                copy_in(n, b, base).start()

    @pl.loop(0, SEQS)
    def _(b):
        start, base, hit = place(b)

        @pl.when(hit)
        def _():
            inv = columns[pl.ds(pl.multiple_of(PROPS * b, PROPS), PROPS), 2:3]
            slot = iota((WINDOW, PROPS), 0) + (base - start)
            selector = jnp.where(slot == iota((WINDOW, PROPS), 1), 1.0, 0.0).astype(bf16)
            slot = iota((WINDOW, WIDTH), 0) + (base - start)
            inside = (slot >= 0) & (slot < PROPS)
            for n in range(2):
                raw = joined[b, :, (n + 1) * WIDTH : (n + 2) * WIDTH].astype(f32)
                rows = jnp.dot(selector, (inv * raw).astype(bf16), preferred_element_type=f32)
                copy_in(n, b, base).wait()
                held = buf[n, b].astype(f32)
                buf[n, b] = jnp.where(inside, rows, held).astype(bf16)
                copy_out(n, b, base).start()

    @pl.loop(0, SEQS)
    def _(b):
        start, base, hit = place(b)

        @pl.when(hit)
        def _():
            for n in range(2):
                copy_out(n, b, base).wait()


def shards(
    tokens,
    norm_gain,
    w_query,
    w_key,
    w_value,
    w_gate,
    gate_bias,
    w_out,
    keys_cache,
    values_cache,
    cum_gates,
    prior_len,
    accepted,
    parents,
):
    ids = jnp.stack([lax.axis_index(KV), lax.axis_index("tp")]).astype(jnp.int32)
    cache = jax.ShapeDtypeStruct(keys_cache.shape, bf16)

    parts = pl.pallas_call(
        project_kernel,
        out_shape=jax.ShapeDtypeStruct((N_KV, PROPS, ROWS), bf16),
        in_specs=[SM, SM, SM, VM, VM, VM, VM, VM, ANY, VM],
        out_specs=VM,
        scratch_shapes=[
            pltpu.VMEM((64, 16), bf16),
            pltpu.VMEM((16, ROWS), f32),
            pltpu.SemaphoreType.DMA,
        ],
        name="project",
    )(
        ids,
        prior_len,
        accepted,
        tokens,
        norm_gain[None],
        w_query,
        w_key,
        w_value,
        w_gate,
        cum_gates,
    )
    arrived = lax.all_to_all(parts, KV, 0, 0, tiled=True)

    keys_copy, values_copy = pl.pallas_call(
        copy_kernel,
        out_shape=(cache, cache),
        in_specs=[ANY, ANY, ANY],
        out_specs=(ANY, ANY),
        scratch_shapes=[pltpu.SemaphoreType.DMA((16,))],
        cost_estimate=pl.CostEstimate(
            flops=8_000_000_000, bytes_accessed=12_600_000, transcendentals=0
        ),
        name="copy",
    )(parts, keys_cache, values_cache)

    block = pl.pallas_call(
        share_kernel,
        out_shape=jax.ShapeDtypeStruct((N_KV, PROPS, ROWS), bf16),
        in_specs=[SM, SM, VM],
        out_specs=VM,
        name="share",
    )(ids, gate_bias, arrived)
    joined = lax.all_to_all(block, KV, 0, 0, tiled=True)

    w_all = lax.all_to_all(
        jnp.broadcast_to(w_out[None], (N_TP, *w_out.shape)), "tp", 0, 0, tiled=True
    )

    sent = pl.pallas_call(
        attention_kernel,
        out_shape=jax.ShapeDtypeStruct((N_TP, 128, WIDTH), bf16),
        in_specs=[SM, SM, SM, SM, VM, VM, ANY, ANY],
        out_specs=VM,
        scratch_shapes=[
            pltpu.VMEM((SEQS, LEN, WIDTH), bf16),
            pltpu.VMEM((SEQS, LEN, WIDTH), bf16),
            pltpu.VMEM((ROWS, 8), f32),
            pltpu.SemaphoreType.DMA((8,)),
            pltpu.SemaphoreType.DMA((8,)),
        ],
        name="attention",
    )(ids, prior_len, accepted, parents, joined, cum_gates, keys_cache, values_cache)
    pieces = lax.all_to_all(sent.reshape(256, 4, WIDTH), ("tp", *KV), 0, 0, tiled=True)

    keys_out, values_out = pl.pallas_call(
        write_kernel,
        out_shape=(cache, cache),
        in_specs=[SM, SM, SM, VM, ANY, ANY, ANY],
        out_specs=(ANY, ANY),
        input_output_aliases={5: 0, 6: 1},
        scratch_shapes=[
            pltpu.VMEM((2, SEQS, WINDOW, WIDTH), bf16),
            pltpu.VMEM((ROWS, 8), f32),
            pltpu.SemaphoreType.DMA((2, SEQS)),
            pltpu.SemaphoreType.DMA((2, SEQS)),
        ],
        cost_estimate=pl.CostEstimate(
            flops=8_000_000_000, bytes_accessed=100_000, transcendentals=0
        ),
        name="write",
    )(ids, prior_len, accepted, joined, sent, keys_copy, values_copy)

    combined = pl.pallas_call(
        combine_kernel,
        out_shape=jax.ShapeDtypeStruct((N_KV, PROPS, WIDTH), bf16),
        in_specs=[SM, VM],
        out_specs=VM,
        name="combine",
    )(ids, pieces.reshape(1024, WIDTH))
    shared = lax.all_to_all(combined, KV, 0, 0, tiled=True)

    mixed_rows = pl.pallas_call(
        output_kernel,
        out_shape=jax.ShapeDtypeStruct((48, 64), bf16),
        in_specs=[VM, VM],
        out_specs=VM,
        scratch_shapes=[pltpu.VMEM((48, 1024), f32)],
        name="output",
    )(shared, w_all)
    return (mixed_rows, keys_out, values_out)


def solution(mesh):
    torus = Mesh(mesh.devices.reshape(8, 4, mesh.shape["tp"]), ("kv_0", "kv_1", "tp"))
    in_specs = (
        P(None, KV),
        P(KV),
        P(KV, "tp"),
        P(KV, "tp"),
        P(KV, "tp"),
        P(),
        P(),
        P("tp", KV),
        P(None, KV, "tp"),
        P(None, KV, "tp"),
        P(None, "tp", KV),
        P(),
        P(),
        P(),
    )
    out_specs = (P("tp", KV), P(None, KV, "tp"), P(None, KV, "tp"))
    return jax.shard_map(
        shards, mesh=torus, in_specs=in_specs, out_specs=out_specs, check_vma=False
    )
```

```python
import jax
import jax.numpy as jnp
from jax import lax
from jax.experimental import pallas as pl
from jax.experimental.pallas import tpu as pltpu
from jax.sharding import Mesh
from jax.sharding import PartitionSpec as P

D = 2048
HEAD = 64
PROPS = 16
ROWS = 384
SEQS = 24
LEN = 512
WIDTH = 128
N_KV = 32
N_TP = 8
STATS = 24
WINDOW = 32
KV = ("kv_0", "kv_1")

masked_score = -1e30
lowest_max = -1e20
norm_eps = 1e-06

VM = pl.BlockSpec(memory_space=pltpu.VMEM)
SM = pl.BlockSpec(memory_space=pltpu.SMEM)
ANY = pl.BlockSpec(memory_space=pl.ANY)
bf16 = jnp.bfloat16
f32 = jnp.float32


def iota(shape, dim):
    return lax.broadcasted_iota(jnp.int32, shape, dim)


def high_low(x):
    high = x.astype(bf16).astype(f32)
    return high, (x - high).astype(bf16).astype(f32)


def dot_t(a, b):
    return lax.dot_general(a, b, (((1,), (1,)), ((), ())), preferred_element_type=f32)


def project_kernel(
    prior, accepted, tokens, gain, w_q, w_k, w_v, w_gate, cum, out, bias, gate_rows, gates, sem
):
    kv, tp = lax.axis_index(KV), lax.axis_index("tp")
    columns = pl.ds(pl.multiple_of(lax.div(kv, 2) * WIDTH, WIDTH), WIDTH)
    copy = pltpu.make_async_copy(w_gate.at[:, columns], gate_rows, sem)
    copy.start()
    floats = tokens[...].astype(f32)
    same = iota((64, 64), 0) == iota((64, 64), 1)
    gain_column = jnp.sum(jnp.where(same, gain[...], 0.0), axis=1, keepdims=True)
    scaled = floats * gain_column
    rows = jnp.transpose(scaled).astype(bf16)
    scaled = scaled.astype(bf16)
    for n, w in enumerate((w_q, w_k, w_v)):
        part = jnp.dot(rows, w[...], preferred_element_type=f32).astype(bf16)
        out[0:SEQS, :, n * WIDTH : (n + 1) * WIDTH] = part.reshape(SEQS, PROPS, WIDTH)
    sq_high, sq_low = high_low(floats * floats)
    ones = jnp.ones((8, 64), bf16)
    square_sum = jnp.dot(ones, sq_high.astype(bf16), preferred_element_type=f32) + jnp.dot(
        ones, sq_low.astype(bf16), preferred_element_type=f32
    )
    lane = iota((2, WIDTH), 1)
    position = iota((2, LEN), 1)
    last = jnp.zeros((2, WIDTH), f32)
    for b in range(SEQS):
        at = prior[b] + accepted[b] - 1 - kv * LEN
        here = cum[b]
        bias[b] = jnp.where(position <= at, -here, masked_score)
        found = jnp.sum(jnp.where(position == at, here, 0.0), axis=1, keepdims=True)
        last = jnp.where(lane == b, found, last)
    last_high, last_low = high_low(last)
    rest = last - last_high - last_low
    odd = lax.rem(kv, 2)
    zero = jnp.zeros_like(scaled)
    both = jnp.concatenate(
        [jnp.where(odd == 0, scaled, zero), jnp.where(odd == 1, scaled, zero)], axis=0
    )
    copy.wait()
    gates[...] = jnp.dot(gate_rows[...], both, preferred_element_type=f32)
    row = iota((8, ROWS), 0)
    gate_0 = gates[pl.ds(2 * tp, 1), :]
    gate_1 = gates[pl.ds(2 * tp + 1, 1), :]
    stats = jnp.where(row == 0, gate_0, jnp.where(row == 1, gate_1, 0.0))
    stats = jnp.where(row == 2, square_sum, stats)
    wide = jnp.zeros((2, ROWS - WIDTH), f32)
    last = jnp.concatenate([last, wide], axis=1)
    rest = jnp.concatenate([rest, wide], axis=1)
    stats = jnp.where(row == 3, last[0:1], jnp.where(row == 4, last[1:2], stats))
    stats = jnp.where(row == 5, rest[0:1], jnp.where(row == 6, rest[1:2], stats))
    out[STATS] = jnp.concatenate(high_low(stats), axis=0).astype(bf16)
    out[STATS + 1 :] = jnp.zeros((N_KV - STATS - 1, PROPS, ROWS), bf16)


def share_kernel(bias, parts, after, after_w, out):
    kv, tp = lax.axis_index(KV), lax.axis_index("tp")
    total = jnp.zeros((PROPS, ROWS), f32)
    for k in range(N_KV):
        total = total + parts[k].astype(f32)
    stats = total[0:8] + total[8:16]
    row = iota((8, ROWS), 0)
    inv_rms = lax.rsqrt(stats[2:3] / D + norm_eps)
    logits = inv_rms * stats + jnp.where(row == 0, bias[2 * tp], bias[2 * tp + 1])
    log_gates = jnp.minimum(logits, 0.0) - jnp.log1p(jnp.exp(-jnp.abs(logits)))
    stats = jnp.where(row < 2, log_gates, jnp.where(row == 2, inv_rms, stats))
    stats = jnp.concatenate(high_low(stats), axis=0)
    block = jnp.where(kv == STATS, stats, total).astype(bf16)
    for k in range(N_KV):
        out[k] = block


def attention_kernel(
    ancestors,
    joined,
    biases,
    keys_far,
    values_far,
    out,
    columns,
    scores_buf,
    weights_buf,
    keys,
    values,
    sems,
):
    kv = lax.axis_index(KV)
    moves = []
    for n, (source, target) in enumerate(((keys_far, keys), (values_far, values))):
        for t in range(N_TP):
            three = pl.ds(3 * t, 3)
            moves.append(
                pltpu.make_async_copy(source.at[three], target.at[three], sems.at[n, t])
            )
    for move in moves:
        move.start()
    coded = joined[STATS].astype(f32)
    stats = coded[0:8] + coded[8:16]
    columns[...] = jnp.transpose(stats)
    lane = iota((PROPS, WIDTH), 1)
    first_head = lane < HEAD
    lane_out = iota((2 * PROPS, WIDTH), 1)
    row_out = iota((2 * PROPS, WIDTH), 0)
    own_lanes = (lane_out < HEAD) == (row_out < PROPS)
    stat_lane = jnp.where(row_out < PROPS, lane_out - HEAD, lane_out)
    scale = HEAD**-0.5

    def both_heads(b_rows, b_block):
        inv = columns[b_rows, 2:3]
        q = (inv * joined[b_block, :, 0:WIDTH].astype(f32)).astype(bf16).astype(f32) * scale
        zero = jnp.zeros_like(q)
        return jnp.concatenate(
            [jnp.where(first_head, q, zero), jnp.where(first_head, zero, q)], axis=0
        ).astype(bf16)

    def packed(v, top, total):
        top_high, top_low = high_low(top)
        sum_high, sum_low = high_low(total)
        stats = jnp.where(
            stat_lane == 0,
            top_high,
            jnp.where(stat_lane == 1, top_low, jnp.where(stat_lane == 2, sum_high, sum_low)),
        )
        return jnp.where(own_lanes, v, stats).astype(bf16)

    def sendable(top):
        high, low = high_low(jnp.maximum(top, lowest_max))
        return high + low

    own = jnp.minimum(kv, SEQS - 1)
    mine = pl.ds(pl.multiple_of(PROPS * own, PROPS), PROPS)
    pad = jnp.zeros((WIDTH - PROPS, WIDTH), f32)
    picks = (iota((ROWS, WIDTH), 0) == iota((ROWS, WIDTH), 1) + PROPS * own) & (
        iota((ROWS, WIDTH), 1) < PROPS
    )
    own_gates = jnp.dot(
        joined[STATS], jnp.where(picks, 1.0, 0.0).astype(bf16), preferred_element_type=f32
    ).astype(bf16)
    reached = ancestors[...]
    tree = dot_t(own_gates, jnp.concatenate([reached, pad], axis=0).astype(bf16))
    tree = tree[0:8] + tree[8:16]
    last = jnp.sum(
        jnp.where(iota((8, WIDTH), 1) == own, stats[:, 0:WIDTH], 0.0), axis=1, keepdims=True
    )
    tree_bias = jnp.concatenate(
        [
            jnp.broadcast_to(-(last[3:4] + last[5:6] + tree[0:1]), (PROPS, WIDTH)),
            jnp.broadcast_to(-(last[4:5] + last[6:7] + tree[1:2]), (PROPS, WIDTH)),
        ],
        axis=0,
    )
    own_inv = columns[mine, 2:3]
    new_keys = own_inv * joined[own, :, WIDTH : 2 * WIDTH].astype(f32)
    new_values = own_inv * joined[own, :, 2 * WIDTH : 3 * WIDTH].astype(f32)
    new_keys = jnp.concatenate([new_keys, pad], axis=0).astype(bf16)
    new_values = jnp.concatenate([new_values, pad], axis=0).astype(bf16)
    needed = jnp.where(kv < SEQS, 0.5, 2.0)
    live = jnp.concatenate([reached, reached], axis=0) > needed
    tree_scores = jnp.where(live, dot_t(both_heads(mine, own), new_keys) + tree_bias, masked_score)
    tree_top = jnp.max(tree_scores, axis=1, keepdims=True)

    for b in range(SEQS):
        if b % 3 == 0:
            moves[b // 3].wait()
        q = both_heads(pl.ds(PROPS * b, PROPS), b)
        bias = biases[b]
        bias = jnp.concatenate(
            [
                jnp.broadcast_to(bias[0:1], (PROPS, LEN)),
                jnp.broadcast_to(bias[1:2], (PROPS, LEN)),
            ],
            axis=0,
        )
        scores_buf[b] = dot_t(q, keys[b]) + bias
    tops = []
    totals = []
    for b in range(SEQS):
        scores = scores_buf[b]
        top = sendable(jnp.max(scores, axis=1, keepdims=True))
        weights = jnp.exp(scores - top)
        totals.append(jnp.sum(weights, axis=1, keepdims=True))
        tops.append(top)
        weights_buf[b] = weights.astype(bf16)
    for t in range(N_TP):
        moves[N_TP + t].wait()
    for b in range(SEQS):
        v = jnp.dot(weights_buf[b], values[b], preferred_element_type=f32)
        t, s = divmod(b, 3)
        out[t, 32 * s : 32 * s + 32, :] = packed(v, tops[b], totals[b])
    for t in range(N_TP):
        out[t, 96:128, :] = jnp.zeros((32, WIDTH), bf16)

    at = pl.ds(pl.multiple_of(32 * lax.rem(own, 3), 32), 32)
    held = out[lax.div(own, 3), at, :].astype(f32)

    def stat(n):
        pick = (stat_lane == n) & jnp.logical_not(own_lanes)
        return jnp.sum(jnp.where(pick, held, 0.0), axis=1, keepdims=True)

    old_top = stat(0) + stat(1)
    old_sum = stat(2) + stat(3)
    top = sendable(jnp.maximum(old_top, tree_top))
    weights = jnp.exp(tree_scores - top)
    keep = jnp.exp(old_top - top)
    total = keep * old_sum + jnp.sum(weights, axis=1, keepdims=True)
    v = keep * held + jnp.dot(weights.astype(bf16), new_values, preferred_element_type=f32)
    out[lax.div(own, 3), at, :] = packed(v, top, total)


def combine_kernel(parts, after_w, after, out):
    kv = lax.axis_index(KV)
    head = lax.rem(lax.div(kv, 4), 2)
    start = HEAD * (1 - head)
    row = iota((WIDTH, 2 * WIDTH), 0) - start
    row = row - jnp.where(iota((WIDTH, 2 * WIDTH), 1) < WIDTH, 0, 2)
    spread = jnp.where((row == 0) | (row == 1), 1.0, 0.0).astype(bf16)
    results = []
    for g in range(N_TP):
        block = parts[128 * g : 128 * g + 128]
        stats = jnp.dot(block, spread, preferred_element_type=f32)
        tops = stats[:, 0:WIDTH].reshape(16, 8, WIDTH)
        sums = stats[:, WIDTH:].reshape(16, 8, WIDTH)
        floats = block.astype(f32).reshape(16, 8, WIDTH)
        top = jnp.max(tops, axis=0)
        top = jnp.maximum(top, pltpu.roll(top, 4, 0))
        factor = jnp.exp(tops - top[None])
        above = jnp.sum(factor * floats, axis=0)
        below = jnp.sum(factor * sums, axis=0)
        above = above + pltpu.roll(above, 4, 0)
        below = below + pltpu.roll(below, 4, 0)
        results.append(above / below)
    lane = iota((8, WIDTH), 1)
    first = iota((8, WIDTH), 0) < 4
    pairs = []
    for p in range(4):
        even, odd = results[2 * p], results[2 * p + 1]
        even = jnp.where(head == 0, even, pltpu.roll(even, HEAD, 1))
        odd = jnp.where(head == 1, odd, pltpu.roll(odd, HEAD, 1))
        pairs.append(jnp.where(lane < HEAD, even, odd))
    block = jnp.concatenate(
        [jnp.where(first, pairs[0], pairs[1]), jnp.where(first, pairs[2], pairs[3])], axis=0
    ).astype(bf16)
    for k in range(N_KV):
        out[k] = block


def output_kernel(shared, w_0, w_1, w_2, w_4, out, rows):
    tp = lax.axis_index("tp")
    for s in range(3):
        for h in range(2):
            for i in range(4):
                block = shared[8 * s + 4 * h + i].astype(f32)
                for p in range(4):
                    rows[16 * s + 4 * i : 16 * s + 4 * i + 4, pl.ds((2 * p + h) * WIDTH, WIDTH)] = (
                        block[4 * p : 4 * p + 4]
                    )
    near = (w_0[...], w_1[...], w_2[0], w_2[1], w_4[0], w_4[1], w_4[2], w_4[3])
    near = [w.astype(f32) for w in near]
    for bit in (1, 2, 4):
        swap = (tp & bit) != 0
        near = [jnp.where(swap, near[g ^ bit], near[g]) for g in range(N_TP)]
    lane = iota((64, WIDTH), 1)
    total = jnp.zeros((48, 64), f32)
    for p in range(4):
        even, odd = near[2 * p], near[2 * p + 1]
        for h in range(2):
            if h == 0:
                weight = jnp.where(lane < HEAD, even, pltpu.roll(odd, HEAD, 1))
            else:
                weight = jnp.where(lane < HEAD, pltpu.roll(even, HEAD, 1), odd)
            block = rows[:, (2 * p + h) * WIDTH : (2 * p + h + 1) * WIDTH].astype(bf16)
            total = total + dot_t(block, weight.astype(bf16))
    out[...] = total.astype(bf16)


def join_kernel(first, second, out):
    count = first.shape[0]
    out[0:count] = first[...]
    out[count:] = second[...]


def copy_kernel(
    after, parents, keys, values, keys_out, values_out, ancestors, keys_near, values_near, sems
):
    moves = []
    for n, (source, near, target) in enumerate(
        ((keys, keys_near, keys_out), (values, values_near, values_out))
    ):
        for t in range(8):
            three = pl.ds(3 * t, 3)
            moves.append(
                (
                    pltpu.make_async_copy(source.at[three], near.at[three], sems.at[0, 8 * n + t]),
                    pltpu.make_async_copy(near.at[three], target.at[three], sems.at[1, 8 * n + t]),
                )
            )
    for move in moves:
        move[0].start()
    own = jnp.minimum(lax.axis_index(KV), SEQS - 1)
    row = iota((PROPS, WIDTH), 0)
    lane = iota((PROPS, WIDTH), 1)
    reached = jnp.where(lane == row, 1.0, 0.0)
    for i in range(PROPS):
        reached = jnp.where((row == i) & (lane == parents[i, own]), 1.0, reached)
    pad = jnp.zeros((WIDTH - PROPS, WIDTH), f32)
    for _ in range(4):
        other = jnp.concatenate([reached, pad], axis=0).astype(bf16)
        reached = jnp.minimum(jnp.dot(reached.astype(bf16), other, preferred_element_type=f32), 1.0)
    ancestors[...] = reached
    for move in moves:
        move[0].wait()
        move[1].start()
    for move in moves:
        move[1].wait()


def write_kernel(
    prior, accepted, joined, after, keys_in, values_in, keys, values, buf, columns, in_sem, out_sem
):
    offset = lax.axis_index(KV) * LEN
    coded = joined[STATS].astype(f32)
    columns[...] = jnp.transpose(coded[0:8] + coded[8:16])

    def place(b):
        start = prior[b] + accepted[b] - offset
        base = jnp.clip(lax.div(jnp.maximum(start, 0), 16) * 16, 0, LEN - WINDOW)
        hit = (start > -PROPS) & (start < LEN)
        return start, pl.multiple_of(base, 16), hit

    def copy_in(n, b, base):
        source = (keys, values)[n].at[b, pl.ds(base, WINDOW), :]
        return pltpu.make_async_copy(source, buf.at[n, b], in_sem.at[n, b])

    def copy_out(n, b, base):
        target = (keys, values)[n].at[b, pl.ds(base, WINDOW), :]
        return pltpu.make_async_copy(buf.at[n, b], target, out_sem.at[n, b])

    @pl.loop(0, SEQS)
    def _(b):
        start, base, hit = place(b)

        @pl.when(hit)
        def _():
            for n in range(2):
                copy_in(n, b, base).start()

    @pl.loop(0, SEQS)
    def _(b):
        start, base, hit = place(b)

        @pl.when(hit)
        def _():
            inv = columns[pl.ds(pl.multiple_of(PROPS * b, PROPS), PROPS), 2:3]
            slot = iota((WINDOW, PROPS), 0) + (base - start)
            selector = jnp.where(slot == iota((WINDOW, PROPS), 1), 1.0, 0.0).astype(bf16)
            slot = iota((WINDOW, WIDTH), 0) + (base - start)
            inside = (slot >= 0) & (slot < PROPS)
            for n in range(2):
                raw = joined[b, :, (n + 1) * WIDTH : (n + 2) * WIDTH].astype(f32)
                rows = jnp.dot(selector, (inv * raw).astype(bf16), preferred_element_type=f32)
                copy_in(n, b, base).wait()
                held = buf[n, b].astype(f32)
                buf[n, b] = jnp.where(inside, rows, held).astype(bf16)
                copy_out(n, b, base).start()

    @pl.loop(0, SEQS)
    def _(b):
        start, base, hit = place(b)

        @pl.when(hit)
        def _():
            for n in range(2):
                copy_out(n, b, base).wait()


def shards(
    tokens,
    norm_gain,
    w_query,
    w_key,
    w_value,
    w_gate,
    gate_bias,
    w_out,
    keys_cache,
    values_cache,
    cum_gates,
    prior_len,
    accepted,
    parents,
):
    cache = jax.ShapeDtypeStruct(keys_cache.shape, bf16)

    def near(*arrays):
        return [pltpu.with_memory_space_constraint(a, pltpu.VMEM) for a in arrays]

    def far(*arrays):
        return [pltpu.with_memory_space_constraint(a, pltpu.HBM) for a in arrays]

    def limit(mib):
        return pltpu.CompilerParams(vmem_limit_bytes=mib << 20)

    parts, biases = pl.pallas_call(
        project_kernel,
        out_shape=(
            jax.ShapeDtypeStruct((N_KV, PROPS, ROWS), bf16),
            pltpu.VMEM(cum_gates.shape, f32),
        ),
        in_specs=[SM, SM, VM, VM, VM, VM, VM, ANY, VM],
        out_specs=(VM, VM),
        scratch_shapes=[
            pltpu.VMEM((16, WIDTH), bf16),
            pltpu.VMEM((16, ROWS), f32),
            pltpu.SemaphoreType.DMA,
        ],
        name="project",
    )(
        prior_len,
        accepted,
        tokens.T,
        norm_gain[None],
        w_query,
        w_key,
        w_value,
        w_gate.T,
        cum_gates,
    )
    arrived = lax.all_to_all(parts, KV, 0, 0, tiled=True)

    keys_copy, values_copy, ancestors = pl.pallas_call(
        copy_kernel,
        out_shape=(
            cache,
            cache,
            pltpu.VMEM((PROPS, WIDTH), f32),
        ),
        in_specs=[ANY, SM, ANY, ANY],
        out_specs=(ANY, ANY, VM),
        scratch_shapes=[
            pltpu.VMEM(keys_cache.shape, bf16),
            pltpu.VMEM(keys_cache.shape, bf16),
            pltpu.SemaphoreType.DMA((2, 16)),
        ],
        compiler_params=limit(8),
        cost_estimate=pl.CostEstimate(
            flops=2_000_000_000, bytes_accessed=12_600_000, transcendentals=0
        ),
        name="copy",
    )(*far(parts), parents.T, *far(keys_cache, values_cache))

    tp_count = lax.axis_size("tp")

    def gathered(name, *pieces):
        return pl.pallas_call(
            join_kernel,
            out_shape=pltpu.VMEM((sum(len(p) for p in pieces), *pieces[0].shape[1:]), bf16),
            in_specs=[VM, VM],
            out_specs=VM,
            compiler_params=limit(2),
            name=name,
        )(*near(*pieces))

    def across(x, bit):
        return lax.ppermute(x, "tp", [(i, i ^ bit) for i in range(tp_count)])

    w_0 = w_out.T
    w_1 = across(w_0, 1)
    w_pair = gathered("pair", w_0[None], w_1[None])
    w_2 = across(w_pair, 2)
    w_4 = across(gathered("four", w_pair, w_2), 4)

    block = pl.pallas_call(
        share_kernel,
        out_shape=pltpu.VMEM((N_KV, PROPS, ROWS), bf16),
        in_specs=[SM, VM, VM, VM],
        out_specs=VM,
        compiler_params=limit(8),
        name="share",
    )(gate_bias, *near(arrived, ancestors, w_2))
    joined = lax.all_to_all(block, KV, 0, 0, tiled=True)

    sent = pl.pallas_call(
        attention_kernel,
        out_shape=jax.ShapeDtypeStruct((N_TP, 128, WIDTH), bf16),
        in_specs=[VM, VM, VM, ANY, ANY],
        out_specs=VM,
        scratch_shapes=[
            pltpu.VMEM((ROWS, 8), f32),
            pltpu.VMEM((SEQS, 2 * PROPS, LEN), f32),
            pltpu.VMEM((SEQS, 2 * PROPS, LEN), bf16),
            pltpu.VMEM(keys_cache.shape, bf16),
            pltpu.VMEM(keys_cache.shape, bf16),
            pltpu.SemaphoreType.DMA((2, N_TP)),
        ],
        compiler_params=limit(20),
        name="attention",
    )(*near(ancestors, joined, biases), *far(keys_cache, values_cache))
    pieces = lax.all_to_all(sent.reshape(256, 4, WIDTH), ("tp", *KV), 0, 0, tiled=True)

    keys_out, values_out = pl.pallas_call(
        write_kernel,
        out_shape=(cache, cache),
        in_specs=[SM, SM, VM, ANY, ANY, ANY],
        out_specs=(ANY, ANY),
        input_output_aliases={4: 0, 5: 1},
        scratch_shapes=[
            pltpu.VMEM((2, SEQS, WINDOW, WIDTH), bf16),
            pltpu.VMEM((ROWS, 8), f32),
            pltpu.SemaphoreType.DMA((2, SEQS)),
            pltpu.SemaphoreType.DMA((2, SEQS)),
        ],
        compiler_params=limit(8),
        cost_estimate=pl.CostEstimate(
            flops=2_000_000_000, bytes_accessed=100_000, transcendentals=0
        ),
        name="write",
    )(
        *far(prior_len, accepted),
        *near(joined),
        *far(sent, keys_copy, values_copy),
    )

    combined = pl.pallas_call(
        combine_kernel,
        out_shape=pltpu.VMEM((N_KV, PROPS, WIDTH), bf16),
        in_specs=[VM, VM, ANY],
        out_specs=VM,
        compiler_params=limit(8),
        name="combine",
    )(*near(pieces.reshape(1024, WIDTH), w_4), *far(keys_out))
    shared = lax.all_to_all(combined, KV, 0, 0, tiled=True)

    mixed_rows = pl.pallas_call(
        output_kernel,
        out_shape=jax.ShapeDtypeStruct((48, 64), bf16),
        in_specs=[VM] * 5,
        out_specs=VM,
        scratch_shapes=[pltpu.VMEM((48, 1024), f32)],
        compiler_params=limit(8),
        name="output",
    )(*near(shared, w_0, w_1, w_2, w_4))
    return (mixed_rows, keys_out, values_out)


def solution(mesh):
    torus = Mesh(mesh.devices.reshape(8, 4, mesh.shape["tp"]), ("kv_0", "kv_1", "tp"))
    in_specs = (
        P(None, KV),
        P(KV),
        P(KV, "tp"),
        P(KV, "tp"),
        P(KV, "tp"),
        P(),
        P(),
        P("tp", KV),
        P(None, KV, "tp"),
        P(None, KV, "tp"),
        P(None, "tp", KV),
        P(),
        P(),
        P(),
    )
    out_specs = (P("tp", KV), P(None, KV, "tp"), P(None, KV, "tp"))
    return jax.shard_map(
        shards, mesh=torus, in_specs=in_specs, out_specs=out_specs, check_vma=False
    )
```

```python
import jax
import jax.numpy as jnp
from jax import lax
from jax.experimental import pallas as pl
from jax.experimental.pallas import tpu as pltpu
from jax.sharding import Mesh
from jax.sharding import PartitionSpec as P

D = 2048
HEAD = 64
PROPS = 16
ROWS = 384
SEQS = 24
LEN = 512
WIDTH = 128
N_KV = 32
N_TP = 8
STATS = 24
WINDOW = 32
KV = ("kv_0", "kv_1")

masked_score = -1e30
lowest_max = -1e20
norm_eps = 1e-06

VM = pl.BlockSpec(memory_space=pltpu.VMEM)
SM = pl.BlockSpec(memory_space=pltpu.SMEM)
ANY = pl.BlockSpec(memory_space=pl.ANY)
bf16 = jnp.bfloat16
f32 = jnp.float32


def iota(shape, dim):
    return lax.broadcasted_iota(jnp.int32, shape, dim)


def high_low(x):
    high = x.astype(bf16).astype(f32)
    return high, (x - high).astype(bf16).astype(f32)


def dot_t(a, b):
    return lax.dot_general(a, b, (((1,), (1,)), ((), ())), preferred_element_type=f32)


def project_kernel(
    prior, accepted, tokens, gain, w_q, w_k, w_v, w_gate, cum, out, bias, gate_rows, gates, sem
):
    kv, tp = lax.axis_index(KV), lax.axis_index("tp")
    columns = pl.ds(pl.multiple_of(lax.div(kv, 2) * WIDTH, WIDTH), WIDTH)
    copy = pltpu.make_async_copy(w_gate.at[:, columns], gate_rows, sem)
    copy.start()
    floats = tokens[...].astype(f32)
    same = iota((64, 64), 0) == iota((64, 64), 1)
    gain_column = jnp.sum(jnp.where(same, gain[...], 0.0), axis=1, keepdims=True)
    scaled = floats * gain_column
    rows = jnp.transpose(scaled).astype(bf16)
    scaled = scaled.astype(bf16)
    for n, w in enumerate((w_q, w_k, w_v)):
        part = jnp.dot(rows, w[...], preferred_element_type=f32).astype(bf16)
        out[0:SEQS, :, n * WIDTH : (n + 1) * WIDTH] = part.reshape(SEQS, PROPS, WIDTH)
    sq_high, sq_low = high_low(floats * floats)
    ones = jnp.ones((8, 64), bf16)
    square_sum = jnp.dot(ones, sq_high.astype(bf16), preferred_element_type=f32) + jnp.dot(
        ones, sq_low.astype(bf16), preferred_element_type=f32
    )
    lane = iota((2, WIDTH), 1)
    position = iota((2, LEN), 1)
    last = jnp.zeros((2, WIDTH), f32)
    for b in range(SEQS):
        at = prior[b] + accepted[b] - 1 - kv * LEN
        here = cum[b]
        bias[b] = jnp.where(position <= at, -here, masked_score)
        found = jnp.sum(jnp.where(position == at, here, 0.0), axis=1, keepdims=True)
        last = jnp.where(lane == b, found, last)
    last_high, last_low = high_low(last)
    rest = last - last_high - last_low
    odd = lax.rem(kv, 2)
    zero = jnp.zeros_like(scaled)
    both = jnp.concatenate(
        [jnp.where(odd == 0, scaled, zero), jnp.where(odd == 1, scaled, zero)], axis=0
    )
    copy.wait()
    gates[...] = jnp.dot(gate_rows[...], both, preferred_element_type=f32)
    row = iota((8, ROWS), 0)
    gate_0 = gates[pl.ds(2 * tp, 1), :]
    gate_1 = gates[pl.ds(2 * tp + 1, 1), :]
    stats = jnp.where(row == 0, gate_0, jnp.where(row == 1, gate_1, 0.0))
    stats = jnp.where(row == 2, square_sum, stats)
    wide = jnp.zeros((2, ROWS - WIDTH), f32)
    last = jnp.concatenate([last, wide], axis=1)
    rest = jnp.concatenate([rest, wide], axis=1)
    stats = jnp.where(row == 3, last[0:1], jnp.where(row == 4, last[1:2], stats))
    stats = jnp.where(row == 5, rest[0:1], jnp.where(row == 6, rest[1:2], stats))
    out[STATS] = jnp.concatenate(high_low(stats), axis=0).astype(bf16)
    out[STATS + 1 :] = jnp.zeros((N_KV - STATS - 1, PROPS, ROWS), bf16)


def share_kernel(bias, parts, after, after_w, out):
    kv, tp = lax.axis_index(KV), lax.axis_index("tp")
    total = jnp.zeros((PROPS, ROWS), f32)
    for k in range(N_KV):
        total = total + parts[k].astype(f32)
    stats = total[0:8] + total[8:16]
    row = iota((8, ROWS), 0)
    inv_rms = lax.rsqrt(stats[2:3] / D + norm_eps)
    logits = inv_rms * stats + jnp.where(row == 0, bias[2 * tp], bias[2 * tp + 1])
    log_gates = jnp.minimum(logits, 0.0) - jnp.log1p(jnp.exp(-jnp.abs(logits)))
    stats = jnp.where(row < 2, log_gates, jnp.where(row == 2, inv_rms, stats))
    stats = jnp.concatenate(high_low(stats), axis=0)
    block = jnp.where(kv == STATS, stats, total).astype(bf16)
    for k in range(N_KV):
        out[k] = block


def attention_kernel(
    ancestors,
    joined,
    biases,
    keys_far,
    values_far,
    out,
    columns,
    scores_buf,
    weights_buf,
    keys,
    values,
    v_buf,
    stat_buf,
    mixed,
    sems,
):
    kv = lax.axis_index(KV)
    moves = []
    for n, (source, target) in enumerate(((keys_far, keys), (values_far, values))):
        for t in range(N_TP):
            three = pl.ds(3 * t, 3)
            moves.append(
                pltpu.make_async_copy(source.at[three], target.at[three], sems.at[n, t])
            )
    for move in moves:
        move.start()
    coded = joined[STATS].astype(f32)
    stats = coded[0:8] + coded[8:16]
    columns[...] = jnp.transpose(stats)
    lane = iota((PROPS, WIDTH), 1)
    first_head = lane < HEAD
    lane_out = iota((2 * PROPS, WIDTH), 1)
    first_row = iota((2 * PROPS, WIDTH), 0) < PROPS
    scale = HEAD**-0.5

    def both_heads(b_rows, b_block):
        inv = columns[b_rows, 2:3]
        q = (inv * joined[b_block, :, 0:WIDTH].astype(f32)).astype(bf16).astype(f32) * scale
        zero = jnp.zeros_like(q)
        return jnp.concatenate(
            [jnp.where(first_head, q, zero), jnp.where(first_head, zero, q)], axis=0
        ).astype(bf16)

    def coded_stats(s, top, total):
        place = lane_out - (HEAD + 4 * s)
        top_high, top_low = high_low(top)
        sum_high, sum_low = high_low(total)
        stats = jnp.where(place == 0, top_high, jnp.where(place == 1, top_low, 0.0))
        return jnp.where(place == 2, sum_high, jnp.where(place == 3, sum_low, stats))

    def sendable(top):
        high, low = high_low(jnp.maximum(top, lowest_max))
        return high + low

    own = jnp.minimum(kv, SEQS - 1)
    mine = pl.ds(pl.multiple_of(PROPS * own, PROPS), PROPS)
    pad = jnp.zeros((WIDTH - PROPS, WIDTH), f32)
    picks = (iota((ROWS, WIDTH), 0) == iota((ROWS, WIDTH), 1) + PROPS * own) & (
        iota((ROWS, WIDTH), 1) < PROPS
    )
    own_gates = jnp.dot(
        joined[STATS], jnp.where(picks, 1.0, 0.0).astype(bf16), preferred_element_type=f32
    ).astype(bf16)
    reached = ancestors[...]
    tree = dot_t(own_gates, jnp.concatenate([reached, pad], axis=0).astype(bf16))
    tree = tree[0:8] + tree[8:16]
    last = jnp.sum(
        jnp.where(iota((8, WIDTH), 1) == own, stats[:, 0:WIDTH], 0.0), axis=1, keepdims=True
    )
    tree_bias = jnp.concatenate(
        [
            jnp.broadcast_to(-(last[3:4] + last[5:6] + tree[0:1]), (PROPS, WIDTH)),
            jnp.broadcast_to(-(last[4:5] + last[6:7] + tree[1:2]), (PROPS, WIDTH)),
        ],
        axis=0,
    )
    own_inv = columns[mine, 2:3]
    new_keys = own_inv * joined[own, :, WIDTH : 2 * WIDTH].astype(f32)
    new_values = own_inv * joined[own, :, 2 * WIDTH : 3 * WIDTH].astype(f32)
    new_keys = jnp.concatenate([new_keys, pad], axis=0).astype(bf16)
    new_values = jnp.concatenate([new_values, pad], axis=0).astype(bf16)
    needed = jnp.where(kv < SEQS, 0.5, 2.0)
    live = jnp.concatenate([reached, reached], axis=0) > needed
    tree_scores = jnp.where(live, dot_t(both_heads(mine, own), new_keys) + tree_bias, masked_score)
    tree_top = jnp.max(tree_scores, axis=1, keepdims=True)

    for b in range(SEQS):
        if b % 3 == 0:
            moves[b // 3].wait()
        q = both_heads(pl.ds(PROPS * b, PROPS), b)
        bias = biases[b]
        bias = jnp.concatenate(
            [
                jnp.broadcast_to(bias[0:1], (PROPS, LEN)),
                jnp.broadcast_to(bias[1:2], (PROPS, LEN)),
            ],
            axis=0,
        )
        scores_buf[b] = dot_t(q, keys[b]) + bias
    for b in range(SEQS):
        scores = scores_buf[b]
        top = sendable(jnp.max(scores, axis=1, keepdims=True))
        weights = jnp.exp(scores - top)
        total = jnp.sum(weights, axis=1, keepdims=True)
        weights_buf[b] = weights.astype(bf16)
        stat_buf[b] = coded_stats(b % 3, top, total)
    for t in range(N_TP):
        moves[N_TP + t].wait()
    for b in range(SEQS):
        v_buf[b] = jnp.dot(weights_buf[b], values[b], preferred_element_type=f32)

    scores = scores_buf[own]
    top = jnp.maximum(jnp.max(scores, axis=1, keepdims=True), tree_top)
    top = sendable(top)
    weights = jnp.exp(scores - top)
    tree_weights = jnp.exp(tree_scores - top)
    total = jnp.sum(weights, axis=1, keepdims=True) + jnp.sum(tree_weights, axis=1, keepdims=True)
    stat_buf[own] = coded_stats(lax.rem(own, 3), top, total)
    v_buf[own] = jnp.dot(
        weights.astype(bf16), values[own], preferred_element_type=f32
    ) + jnp.dot(tree_weights.astype(bf16), new_values, preferred_element_type=f32)

    low = lane_out < HEAD
    for t in range(N_TP):
        v = [v_buf[3 * t + s] for s in range(3)]
        turned = [pltpu.roll(x, HEAD, 1) for x in v]
        first = jnp.where(first_row, v[0], turned[0])
        second = jnp.where(first_row, turned[1], v[1])
        third = jnp.where(first_row, v[2], turned[2])
        stats = stat_buf[3 * t] + stat_buf[3 * t + 1] + stat_buf[3 * t + 2]
        mixed[pl.ds(2 * t, N_KV, stride=16), :] = jnp.where(low, first, second)
        mixed[pl.ds(2 * t + 1, N_KV, stride=16), :] = jnp.where(low, third, stats)
    out[...] = mixed[...].astype(bf16)


def combine_kernel(parts, after_w, after, out, tops, sums):
    row = iota((WIDTH, 4 * WIDTH), 0) - HEAD
    column = iota((WIDTH, 4 * WIDTH), 1)
    unit = jnp.where(column < 2 * WIDTH, lax.rem(lax.div(column, HEAD), 2), 2)
    kind = lax.rem(lax.div(column, WIDTH), 2)
    row = row - 4 * unit - 2 * kind
    spread = jnp.where((row == 0) | (row == 1), 1.0, 0.0).astype(bf16)
    even = lax.rem(iota((8, WIDTH), 0), 2) == 0
    for n in range(4):
        stats = jnp.dot(parts[128 * n : 128 * n + 128], spread, preferred_element_type=f32)
        for v in range(16):
            rows = stats[8 * v : 8 * v + 8]
            near = pltpu.roll(rows[:, 0 : 2 * WIDTH], 7, 0)
            tops[16 * n + v] = jnp.where(even, near[:, 0:WIDTH], rows[:, 2 * WIDTH : 3 * WIDTH])
            sums[16 * n + v] = jnp.where(even, near[:, WIDTH:], rows[:, 3 * WIDTH :])
    results = []
    for half in range(2):
        top = tops[half]
        for k in range(1, N_KV):
            top = jnp.maximum(top, tops[2 * k + half])
        above = jnp.zeros((8, WIDTH), f32)
        below = jnp.zeros((8, WIDTH), f32)
        for k in range(N_KV):
            v = 2 * k + half
            factor = jnp.exp(tops[v] - top)
            above = above + factor * parts[8 * v : 8 * v + 8, :].astype(f32)
            below = below + factor * sums[v]
        results.append(above / below)
    block = jnp.concatenate(results, axis=0).astype(bf16)
    for k in range(N_KV):
        out[k] = block


def output_kernel(shared, w_0, w_1, w_2, w_4, out, rows):
    tp = lax.axis_index("tp")
    rows[...] = shared[...].astype(f32)
    near = (w_0[...], w_1[...], w_2[0], w_2[1], w_4[0], w_4[1], w_4[2], w_4[3])
    near = [w.astype(f32) for w in near]
    for bit in (1, 2, 4):
        swap = (tp & bit) != 0
        near = [jnp.where(swap, near[g ^ bit], near[g]) for g in range(N_TP)]
    low = iota((PROPS, WIDTH), 1) < HEAD
    total = jnp.zeros((48, 64), f32)
    for g in range(N_TP):
        pair_0 = rows[pl.ds(2 * g, PROPS, stride=16), :]
        pair_1 = rows[pl.ds(256 + 2 * g, PROPS, stride=16), :]
        last_0 = rows[pl.ds(2 * g + 1, PROPS, stride=16), :]
        last_1 = rows[pl.ds(257 + 2 * g, PROPS, stride=16), :]
        block = jnp.concatenate(
            [
                jnp.where(low, pair_0, pltpu.roll(pair_1, HEAD, 1)),
                jnp.where(low, pltpu.roll(pair_0, HEAD, 1), pair_1),
                jnp.where(low, last_0, pltpu.roll(last_1, HEAD, 1)),
            ],
            axis=0,
        )
        total = total + dot_t(block.astype(bf16), near[g].astype(bf16))
    out[...] = total.astype(bf16)


def join_kernel(first, second, out):
    count = first.shape[0]
    out[0:count] = first[...]
    out[count:] = second[...]


def copy_kernel(after, parents, keys, keys_out, ancestors, keys_near, sems):
    moves = []
    for t in range(8):
        three = pl.ds(3 * t, 3)
        moves.append(
            (
                pltpu.make_async_copy(keys.at[three], keys_near.at[three], sems.at[0, t]),
                pltpu.make_async_copy(keys_near.at[three], keys_out.at[three], sems.at[1, t]),
            )
        )
    for move in moves:
        move[0].start()
    own = jnp.minimum(lax.axis_index(KV), SEQS - 1)
    row = iota((PROPS, WIDTH), 0)
    lane = iota((PROPS, WIDTH), 1)
    reached = jnp.where(lane == row, 1.0, 0.0)
    for i in range(PROPS):
        reached = jnp.where((row == i) & (lane == parents[i, own]), 1.0, reached)
    pad = jnp.zeros((WIDTH - PROPS, WIDTH), f32)
    for _ in range(4):
        other = jnp.concatenate([reached, pad], axis=0).astype(bf16)
        reached = jnp.minimum(jnp.dot(reached.astype(bf16), other, preferred_element_type=f32), 1.0)
    ancestors[...] = reached
    for move in moves:
        move[0].wait()
        move[1].start()
    for move in moves:
        move[1].wait()


def write_kernel(
    prior,
    accepted,
    joined,
    after,
    keys_in,
    values_in,
    keys,
    values,
    buf,
    near,
    columns,
    in_sem,
    out_sem,
    near_sem,
):
    moves = []
    for t in range(8):
        three = pl.ds(3 * t, 3)
        moves.append(
            (
                pltpu.make_async_copy(values_in.at[three], near.at[three], near_sem.at[0, t]),
                pltpu.make_async_copy(near.at[three], values.at[three], near_sem.at[1, t]),
            )
        )
    offset = lax.axis_index(KV) * LEN

    def place(b):
        start = prior[b] + accepted[b] - offset
        base = jnp.clip(lax.div(jnp.maximum(start, 0), 16) * 16, 0, LEN - WINDOW)
        hit = (start > -PROPS) & (start < LEN)
        return start, pl.multiple_of(base, 16), hit

    def copy_in(b, base):
        return pltpu.make_async_copy(
            keys.at[b, pl.ds(base, WINDOW), :], buf.at[b], in_sem.at[b]
        )

    def copy_out(b, base):
        return pltpu.make_async_copy(
            buf.at[b], keys.at[b, pl.ds(base, WINDOW), :], out_sem.at[b]
        )

    @pl.loop(0, SEQS)
    def _(b):
        start, base, hit = place(b)

        @pl.when(hit)
        def _():
            copy_in(b, base).start()

    for move in moves:
        move[0].start()
    coded = joined[STATS].astype(f32)
    columns[...] = jnp.transpose(coded[0:8] + coded[8:16])

    def patched(b, start, base):
        inv = columns[pl.ds(pl.multiple_of(PROPS * b, PROPS), PROPS), 2:3]
        slot = iota((WINDOW, PROPS), 0) + (base - start)
        selector = jnp.where(slot == iota((WINDOW, PROPS), 1), 1.0, 0.0).astype(bf16)
        raw = joined[b, :, WIDTH:].astype(f32)
        rows = jnp.dot(selector, (inv * raw).astype(bf16), preferred_element_type=f32)
        slot = iota((WINDOW, WIDTH), 0) + (base - start)
        return (slot >= 0) & (slot < PROPS), rows

    for t in range(8):
        moves[t][0].wait()

        @pl.loop(3 * t, 3 * t + 3)
        def _(b):
            start, base, hit = place(b)

            @pl.when(hit)
            def _():
                inside, rows = patched(b, start, base)
                window = pl.ds(base, WINDOW)
                held = near[b, window, :].astype(f32)
                near[b, window, :] = jnp.where(inside, rows[:, WIDTH:], held).astype(bf16)
                copy_in(b, base).wait()
                held = buf[b].astype(f32)
                buf[b] = jnp.where(inside, rows[:, 0:WIDTH], held).astype(bf16)
                copy_out(b, base).start()

        moves[t][1].start()
    for move in moves:
        move[1].wait()

    @pl.loop(0, SEQS)
    def _(b):
        start, base, hit = place(b)

        @pl.when(hit)
        def _():
            copy_out(b, base).wait()


def shards(
    tokens,
    norm_gain,
    w_query,
    w_key,
    w_value,
    w_gate,
    gate_bias,
    w_out,
    keys_cache,
    values_cache,
    cum_gates,
    prior_len,
    accepted,
    parents,
):
    cache = jax.ShapeDtypeStruct(keys_cache.shape, bf16)

    def near(*arrays):
        return [pltpu.with_memory_space_constraint(a, pltpu.VMEM) for a in arrays]

    def far(*arrays):
        return [pltpu.with_memory_space_constraint(a, pltpu.HBM) for a in arrays]

    def limit(mib):
        return pltpu.CompilerParams(vmem_limit_bytes=mib << 20)

    parts, biases = pl.pallas_call(
        project_kernel,
        out_shape=(
            jax.ShapeDtypeStruct((N_KV, PROPS, ROWS), bf16),
            pltpu.VMEM(cum_gates.shape, f32),
        ),
        in_specs=[SM, SM, VM, VM, VM, VM, VM, ANY, VM],
        out_specs=(VM, VM),
        scratch_shapes=[
            pltpu.VMEM((16, WIDTH), bf16),
            pltpu.VMEM((16, ROWS), f32),
            pltpu.SemaphoreType.DMA,
        ],
        name="project",
    )(
        prior_len,
        accepted,
        tokens.T,
        norm_gain[None],
        w_query,
        w_key,
        w_value,
        w_gate.T,
        cum_gates,
    )
    arrived = lax.all_to_all(parts, KV, 0, 0, tiled=True)

    keys_copy, ancestors = pl.pallas_call(
        copy_kernel,
        out_shape=(
            cache,
            pltpu.VMEM((PROPS, WIDTH), f32),
        ),
        in_specs=[ANY, SM, ANY],
        out_specs=(ANY, VM),
        scratch_shapes=[
            pltpu.VMEM(keys_cache.shape, bf16),
            pltpu.SemaphoreType.DMA((2, 8)),
        ],
        compiler_params=limit(8),
        cost_estimate=pl.CostEstimate(
            flops=2_000_000_000, bytes_accessed=12_600_000, transcendentals=0
        ),
        name="copy",
    )(*far(parts), parents.T, *far(keys_cache))

    tp_count = lax.axis_size("tp")

    def gathered(name, *pieces):
        return pl.pallas_call(
            join_kernel,
            out_shape=pltpu.VMEM((sum(len(p) for p in pieces), *pieces[0].shape[1:]), bf16),
            in_specs=[VM, VM],
            out_specs=VM,
            compiler_params=limit(2),
            name=name,
        )(*near(*pieces))

    def across(x, bit):
        return lax.ppermute(x, "tp", [(i, i ^ bit) for i in range(tp_count)])

    w_0 = w_out.T
    w_1 = across(w_0, 1)
    w_pair = gathered("pair", w_0[None], w_1[None])
    w_2 = across(w_pair, 2)
    w_4 = across(gathered("four", w_pair, w_2), 4)

    block = pl.pallas_call(
        share_kernel,
        out_shape=pltpu.VMEM((N_KV, PROPS, ROWS), bf16),
        in_specs=[SM, VM, VM, VM],
        out_specs=VM,
        compiler_params=limit(8),
        name="share",
    )(gate_bias, *near(arrived, ancestors, w_2))
    joined = lax.all_to_all(block, KV, 0, 0, tiled=True)

    sent = pl.pallas_call(
        attention_kernel,
        out_shape=jax.ShapeDtypeStruct((512, WIDTH), bf16),
        in_specs=[VM, VM, VM, ANY, ANY],
        out_specs=VM,
        scratch_shapes=[
            pltpu.VMEM((ROWS, 8), f32),
            pltpu.VMEM((SEQS, 2 * PROPS, LEN), f32),
            pltpu.VMEM((SEQS, 2 * PROPS, LEN), bf16),
            pltpu.VMEM(keys_cache.shape, bf16),
            pltpu.VMEM(keys_cache.shape, bf16),
            pltpu.VMEM((SEQS, 2 * PROPS, WIDTH), f32),
            pltpu.VMEM((SEQS, 2 * PROPS, WIDTH), f32),
            pltpu.VMEM((512, WIDTH), f32),
            pltpu.SemaphoreType.DMA((2, N_TP)),
        ],
        compiler_params=limit(20),
        name="attention",
    )(*near(ancestors, joined, biases), *far(keys_cache, values_cache))
    pieces = lax.all_to_all(sent.reshape(256, 2, WIDTH), (*KV, "tp"), 0, 0, tiled=True)

    keys_out, values_out = pl.pallas_call(
        write_kernel,
        out_shape=(cache, cache),
        in_specs=[SM, SM, VM, ANY, ANY, ANY],
        out_specs=(ANY, ANY),
        input_output_aliases={4: 0},
        scratch_shapes=[
            pltpu.VMEM((SEQS, WINDOW, WIDTH), bf16),
            pltpu.VMEM(keys_cache.shape, bf16),
            pltpu.VMEM((ROWS, 8), f32),
            pltpu.SemaphoreType.DMA((SEQS,)),
            pltpu.SemaphoreType.DMA((SEQS,)),
            pltpu.SemaphoreType.DMA((2, 8)),
        ],
        compiler_params=limit(8),
        cost_estimate=pl.CostEstimate(
            flops=2_000_000_000, bytes_accessed=100_000, transcendentals=0
        ),
        name="write",
    )(
        *far(prior_len, accepted),
        *near(joined),
        *far(sent, keys_copy, values_cache),
    )

    combined = pl.pallas_call(
        combine_kernel,
        out_shape=pltpu.VMEM((N_KV, PROPS, WIDTH), bf16),
        in_specs=[VM, VM, ANY],
        out_specs=VM,
        scratch_shapes=[pltpu.VMEM((64, 8, WIDTH), f32), pltpu.VMEM((64, 8, WIDTH), f32)],
        compiler_params=limit(8),
        name="combine",
    )(*near(pieces.reshape(512, WIDTH), w_4), *far(keys_out))
    shared = lax.all_to_all(combined, KV, 0, 0, tiled=True)

    mixed_rows = pl.pallas_call(
        output_kernel,
        out_shape=jax.ShapeDtypeStruct((48, 64), bf16),
        in_specs=[VM] * 5,
        out_specs=VM,
        scratch_shapes=[pltpu.VMEM((512, WIDTH), f32)],
        compiler_params=limit(8),
        name="output",
    )(*near(shared.reshape(512, WIDTH), w_0, w_1, w_2, w_4))
    return (mixed_rows, keys_out, values_out)


def solution(mesh):
    torus = Mesh(mesh.devices.reshape(8, 4, mesh.shape["tp"]), ("kv_0", "kv_1", "tp"))
    in_specs = (
        P(None, KV),
        P(KV),
        P(KV, "tp"),
        P(KV, "tp"),
        P(KV, "tp"),
        P(),
        P(),
        P("tp", KV),
        P(None, KV, "tp"),
        P(None, KV, "tp"),
        P(None, "tp", KV),
        P(),
        P(),
        P(),
    )
    out_specs = (P("tp", KV), P(None, KV, "tp"), P(None, KV, "tp"))
    return jax.shard_map(
        shards, mesh=torus, in_specs=in_specs, out_specs=out_specs, check_vma=False
    )
```

```python
import jax
import jax.numpy as jnp
from jax import lax
from jax.experimental import pallas as pl
from jax.experimental.pallas import tpu as pltpu
from jax.sharding import Mesh
from jax.sharding import PartitionSpec as P

D = 2048
HEAD = 64
PROPS = 16
ROWS = 384
SEQS = 24
LEN = 512
WIDTH = 128
N_KV = 32
N_TP = 8
STATS = 24
WINDOW = 32
KV = ("kv_0", "kv_1")

masked_score = -1e30
lowest_max = -1e20
norm_eps = 1e-06

VM = pl.BlockSpec(memory_space=pltpu.VMEM)
SM = pl.BlockSpec(memory_space=pltpu.SMEM)
ANY = pl.BlockSpec(memory_space=pl.ANY)
bf16 = jnp.bfloat16
f32 = jnp.float32


def iota(shape, dim):
    return lax.broadcasted_iota(jnp.int32, shape, dim)


def high_low(x):
    high = x.astype(bf16).astype(f32)
    return high, (x - high).astype(bf16).astype(f32)


def dot_t(a, b):
    return lax.dot_general(a, b, (((1,), (1,)), ((), ())), preferred_element_type=f32)


def project_kernel(
    prior, accepted, tokens, gain, w_q, w_k, w_v, w_gate, cum, out, bias, gates
):
    kv, tp = lax.axis_index(KV), lax.axis_index("tp")
    columns = pl.ds(pl.multiple_of(lax.div(kv, 2) * WIDTH, WIDTH), WIDTH)
    floats = tokens[...].astype(f32)
    same = iota((64, 64), 0) == iota((64, 64), 1)
    gain_column = jnp.sum(jnp.where(same, gain[...], 0.0), axis=1, keepdims=True)
    scaled = floats * gain_column
    rows = jnp.transpose(scaled).astype(bf16)
    scaled = scaled.astype(bf16)
    for n, w in enumerate((w_q, w_k, w_v)):
        part = jnp.dot(rows, w[...], preferred_element_type=f32).astype(bf16)
        out[0:SEQS, :, n * WIDTH : (n + 1) * WIDTH] = part.reshape(SEQS, PROPS, WIDTH)
    sq_high, sq_low = high_low(floats * floats)
    ones = jnp.ones((8, 64), bf16)
    square_sum = jnp.dot(ones, sq_high.astype(bf16), preferred_element_type=f32) + jnp.dot(
        ones, sq_low.astype(bf16), preferred_element_type=f32
    )
    lane = iota((2, WIDTH), 1)
    position = iota((2, LEN), 1)
    last = jnp.zeros((2, WIDTH), f32)
    for b in range(SEQS):
        at = prior[b] + accepted[b] - 1 - kv * LEN
        here = cum[b]
        bias[b] = jnp.where(position <= at, -here, masked_score)
        found = jnp.sum(jnp.where(position == at, here, 0.0), axis=1, keepdims=True)
        last = jnp.where(lane == b, found, last)
    last_high, last_low = high_low(last)
    rest = last - last_high - last_low
    odd = lax.rem(kv, 2)
    zero = jnp.zeros_like(scaled)
    both = jnp.concatenate(
        [jnp.where(odd == 0, scaled, zero), jnp.where(odd == 1, scaled, zero)], axis=0
    )
    gates[...] = jnp.dot(w_gate[:, columns], both, preferred_element_type=f32)
    row = iota((8, ROWS), 0)
    gate_0 = gates[pl.ds(2 * tp, 1), :]
    gate_1 = gates[pl.ds(2 * tp + 1, 1), :]
    stats = jnp.where(row == 0, gate_0, jnp.where(row == 1, gate_1, 0.0))
    stats = jnp.where(row == 2, square_sum, stats)
    wide = jnp.zeros((2, ROWS - WIDTH), f32)
    last = jnp.concatenate([last, wide], axis=1)
    rest = jnp.concatenate([rest, wide], axis=1)
    stats = jnp.where(row == 3, last[0:1], jnp.where(row == 4, last[1:2], stats))
    stats = jnp.where(row == 5, rest[0:1], jnp.where(row == 6, rest[1:2], stats))
    out[STATS] = jnp.concatenate(high_low(stats), axis=0).astype(bf16)
    out[STATS + 1 :] = jnp.zeros((N_KV - STATS - 1, PROPS, ROWS), bf16)


def share_kernel(bias, parts, after, after_w, out):
    kv, tp = lax.axis_index(KV), lax.axis_index("tp")
    total = jnp.zeros((PROPS, ROWS), f32)
    for k in range(N_KV):
        total = total + parts[k].astype(f32)
    stats = total[0:8] + total[8:16]
    row = iota((8, ROWS), 0)
    inv_rms = lax.rsqrt(stats[2:3] / D + norm_eps)
    logits = inv_rms * stats + jnp.where(row == 0, bias[2 * tp], bias[2 * tp + 1])
    log_gates = jnp.minimum(logits, 0.0) - jnp.log1p(jnp.exp(-jnp.abs(logits)))
    stats = jnp.where(row < 2, log_gates, jnp.where(row == 2, inv_rms, stats))
    stats = jnp.concatenate(high_low(stats), axis=0)
    block = jnp.where(kv == STATS, stats, total).astype(bf16)
    for k in range(N_KV):
        out[k] = block


def attention_kernel(
    ancestors,
    joined,
    biases,
    keys_far,
    values_far,
    out,
    columns,
    scores_buf,
    weights_buf,
    keys,
    values,
    v_buf,
    stat_buf,
    mixed,
    sems,
):
    kv = lax.axis_index(KV)
    moves = []
    for n, (source, target) in enumerate(((keys_far, keys), (values_far, values))):
        for t in range(N_TP):
            three = pl.ds(3 * t, 3)
            moves.append(
                pltpu.make_async_copy(source.at[three], target.at[three], sems.at[n, t])
            )
    for move in moves:
        move.start()
    coded = joined[STATS].astype(f32)
    stats = coded[0:8] + coded[8:16]
    columns[...] = jnp.transpose(stats)
    lane = iota((PROPS, WIDTH), 1)
    first_head = lane < HEAD
    lane_out = iota((2 * PROPS, WIDTH), 1)
    first_row = iota((2 * PROPS, WIDTH), 0) < PROPS
    scale = HEAD**-0.5

    def both_heads(b_rows, b_block):
        inv = columns[b_rows, 2:3]
        q = (inv * joined[b_block, :, 0:WIDTH].astype(f32)).astype(bf16).astype(f32) * scale
        zero = jnp.zeros_like(q)
        return jnp.concatenate(
            [jnp.where(first_head, q, zero), jnp.where(first_head, zero, q)], axis=0
        ).astype(bf16)

    def coded_stats(s, top, total):
        place = lane_out - (HEAD + 4 * s)
        top_high, top_low = high_low(top)
        sum_high, sum_low = high_low(total)
        stats = jnp.where(place == 0, top_high, jnp.where(place == 1, top_low, 0.0))
        return jnp.where(place == 2, sum_high, jnp.where(place == 3, sum_low, stats))

    def sendable(top):
        high, low = high_low(jnp.maximum(top, lowest_max))
        return high + low

    own = jnp.minimum(kv, SEQS - 1)
    low = lane_out < HEAD

    def score(b):
        q = both_heads(pl.ds(PROPS * b, PROPS), b)
        bias = biases[b]
        bias = jnp.concatenate(
            [
                jnp.broadcast_to(bias[0:1], (PROPS, LEN)),
                jnp.broadcast_to(bias[1:2], (PROPS, LEN)),
            ],
            axis=0,
        )
        scores_buf[b] = dot_t(q, keys[b]) + bias

    def weigh(b):
        scores = scores_buf[b]
        top = sendable(jnp.max(scores, axis=1, keepdims=True))
        weights = jnp.exp(scores - top)
        total = jnp.sum(weights, axis=1, keepdims=True)
        weights_buf[b] = weights.astype(bf16)
        stat_buf[b] = coded_stats(b % 3, top, total)

    def gather(b):
        v_buf[b] = jnp.dot(weights_buf[b], values[b], preferred_element_type=f32)

    def pack(t):
        v = [v_buf[3 * t + s] for s in range(3)]
        turned = [pltpu.roll(x, HEAD, 1) for x in v]
        first = jnp.where(first_row, v[0], turned[0])
        second = jnp.where(first_row, turned[1], v[1])
        third = jnp.where(first_row, v[2], turned[2])
        stats = stat_buf[3 * t] + stat_buf[3 * t + 1] + stat_buf[3 * t + 2]
        mixed[pl.ds(2 * t, N_KV, stride=16), :] = jnp.where(low, first, second)
        mixed[pl.ds(2 * t + 1, N_KV, stride=16), :] = jnp.where(low, third, stats)

    def tree():
        mine = pl.ds(pl.multiple_of(PROPS * own, PROPS), PROPS)
        pad = jnp.zeros((WIDTH - PROPS, WIDTH), f32)
        picks = (iota((ROWS, WIDTH), 0) == iota((ROWS, WIDTH), 1) + PROPS * own) & (
            iota((ROWS, WIDTH), 1) < PROPS
        )
        own_gates = jnp.dot(
            joined[STATS], jnp.where(picks, 1.0, 0.0).astype(bf16), preferred_element_type=f32
        ).astype(bf16)
        reached = ancestors[...]
        tree = dot_t(own_gates, jnp.concatenate([reached, pad], axis=0).astype(bf16))
        tree = tree[0:8] + tree[8:16]
        last = jnp.sum(
            jnp.where(iota((8, WIDTH), 1) == own, stats[:, 0:WIDTH], 0.0), axis=1, keepdims=True
        )
        tree_bias = jnp.concatenate(
            [
                jnp.broadcast_to(-(last[3:4] + last[5:6] + tree[0:1]), (PROPS, WIDTH)),
                jnp.broadcast_to(-(last[4:5] + last[6:7] + tree[1:2]), (PROPS, WIDTH)),
            ],
            axis=0,
        )
        own_inv = columns[mine, 2:3]
        new_keys = own_inv * joined[own, :, WIDTH : 2 * WIDTH].astype(f32)
        new_values = own_inv * joined[own, :, 2 * WIDTH : 3 * WIDTH].astype(f32)
        new_keys = jnp.concatenate([new_keys, pad], axis=0).astype(bf16)
        new_values = jnp.concatenate([new_values, pad], axis=0).astype(bf16)
        needed = jnp.where(kv < SEQS, 0.5, 2.0)
        live = jnp.concatenate([reached, reached], axis=0) > needed
        tree_scores = jnp.where(live, dot_t(both_heads(mine, own), new_keys) + tree_bias, masked_score)
        tree_top = jnp.max(tree_scores, axis=1, keepdims=True)
        return tree_scores, tree_top, new_values

    for step in range(N_TP + 2):
        if step < N_TP:
            moves[step].wait()
        if step >= 2:
            moves[N_TP + step - 2].wait()
        for s in range(3):
            if step < N_TP:
                score(3 * step + s)
            if 1 <= step <= N_TP:
                weigh(3 * step - 3 + s)
            if step >= 2:
                gather(3 * step - 6 + s)
        if step == 3:
            tree_scores, tree_top, new_values = tree()
        if step == N_TP:
            scores = scores_buf[own]
            top = jnp.maximum(jnp.max(scores, axis=1, keepdims=True), tree_top)
            top = sendable(top)
            own_weights = jnp.exp(scores - top)
            tree_weights = jnp.exp(tree_scores - top)
            own_total = jnp.sum(own_weights, axis=1, keepdims=True) + jnp.sum(
                tree_weights, axis=1, keepdims=True
            )
            own_stats = coded_stats(lax.rem(own, 3), top, own_total)
    own_v = jnp.dot(
        own_weights.astype(bf16), values[own], preferred_element_type=f32
    ) + jnp.dot(tree_weights.astype(bf16), new_values, preferred_element_type=f32)
    stat_buf[own] = own_stats
    v_buf[own] = own_v
    for t in range(N_TP):
        pack(t)
    out[...] = mixed[...].astype(bf16)


def combine_kernel(parts, out, tops, sums):
    row = iota((WIDTH, 4 * WIDTH), 0) - HEAD
    column = iota((WIDTH, 4 * WIDTH), 1)
    unit = jnp.where(column < 2 * WIDTH, lax.rem(lax.div(column, HEAD), 2), 2)
    kind = lax.rem(lax.div(column, WIDTH), 2)
    row = row - 4 * unit - 2 * kind
    spread = jnp.where((row == 0) | (row == 1), 1.0, 0.0).astype(bf16)
    even = lax.rem(iota((8, WIDTH), 0), 2) == 0
    for n in range(4):
        stats = jnp.dot(parts[128 * n : 128 * n + 128], spread, preferred_element_type=f32)
        for v in range(16):
            rows = stats[8 * v : 8 * v + 8]
            near = pltpu.roll(rows[:, 0 : 2 * WIDTH], 7, 0)
            tops[16 * n + v] = jnp.where(even, near[:, 0:WIDTH], rows[:, 2 * WIDTH : 3 * WIDTH])
            sums[16 * n + v] = jnp.where(even, near[:, WIDTH:], rows[:, 3 * WIDTH :])
    results = []
    for half in range(2):
        top = tops[half]
        for k in range(1, N_KV):
            top = jnp.maximum(top, tops[2 * k + half])
        above = jnp.zeros((8, WIDTH), f32)
        below = jnp.zeros((8, WIDTH), f32)
        for k in range(N_KV):
            v = 2 * k + half
            factor = jnp.exp(tops[v] - top)
            above = above + factor * parts[8 * v : 8 * v + 8, :].astype(f32)
            below = below + factor * sums[v]
        results.append(above / below)
    block = jnp.concatenate(results, axis=0).astype(bf16)
    for k in range(N_KV):
        out[k] = block


def output_kernel(shared, w_0, w_1, w_2, w_4, out, rows):
    tp = lax.axis_index("tp")
    rows[...] = shared[...].astype(f32)
    near = (w_0[...], w_1[...], w_2[0], w_2[1], w_4[0], w_4[1], w_4[2], w_4[3])
    near = [w.astype(f32) for w in near]
    for bit in (1, 2, 4):
        swap = (tp & bit) != 0
        near = [jnp.where(swap, near[g ^ bit], near[g]) for g in range(N_TP)]
    low = iota((PROPS, WIDTH), 1) < HEAD
    total = jnp.zeros((48, 64), f32)
    for g in range(N_TP):
        pair_0 = rows[pl.ds(2 * g, PROPS, stride=16), :]
        pair_1 = rows[pl.ds(256 + 2 * g, PROPS, stride=16), :]
        last_0 = rows[pl.ds(2 * g + 1, PROPS, stride=16), :]
        last_1 = rows[pl.ds(257 + 2 * g, PROPS, stride=16), :]
        block = jnp.concatenate(
            [
                jnp.where(low, pair_0, pltpu.roll(pair_1, HEAD, 1)),
                jnp.where(low, pltpu.roll(pair_0, HEAD, 1), pair_1),
                jnp.where(low, last_0, pltpu.roll(last_1, HEAD, 1)),
            ],
            axis=0,
        )
        total = total + dot_t(block.astype(bf16), near[g].astype(bf16))
    out[...] = total.astype(bf16)


def join_kernel(first, second, out):
    count = first.shape[0]
    out[0:count] = first[...]
    out[count:] = second[...]


def copy_kernel(after, parents, keys, keys_out, ancestors, keys_near, sems):
    moves = []
    for t in range(8):
        three = pl.ds(3 * t, 3)
        moves.append(
            (
                pltpu.make_async_copy(keys.at[three], keys_near.at[three], sems.at[0, t]),
                pltpu.make_async_copy(keys_near.at[three], keys_out.at[three], sems.at[1, t]),
            )
        )
    for move in moves:
        move[0].start()
    own = jnp.minimum(lax.axis_index(KV), SEQS - 1)
    row = iota((PROPS, WIDTH), 0)
    lane = iota((PROPS, WIDTH), 1)
    reached = jnp.where(lane == row, 1.0, 0.0)
    for i in range(PROPS):
        reached = jnp.where((row == i) & (lane == parents[i, own]), 1.0, reached)
    pad = jnp.zeros((WIDTH - PROPS, WIDTH), f32)
    for _ in range(4):
        other = jnp.concatenate([reached, pad], axis=0).astype(bf16)
        reached = jnp.minimum(jnp.dot(reached.astype(bf16), other, preferred_element_type=f32), 1.0)
    ancestors[...] = reached
    for move in moves:
        move[0].wait()
        move[1].start()
    for move in moves:
        move[1].wait()


def write_kernel(
    prior,
    accepted,
    joined,
    after,
    keys_in,
    values_in,
    keys,
    values,
    buf,
    near,
    columns,
    in_sem,
    out_sem,
    near_sem,
):
    moves = []
    for t in range(8):
        three = pl.ds(3 * t, 3)
        moves.append(
            (
                pltpu.make_async_copy(values_in.at[three], near.at[three], near_sem.at[0, t]),
                pltpu.make_async_copy(near.at[three], values.at[three], near_sem.at[1, t]),
            )
        )
    offset = lax.axis_index(KV) * LEN

    def place(b):
        start = prior[b] + accepted[b] - offset
        base = jnp.clip(lax.div(jnp.maximum(start, 0), 16) * 16, 0, LEN - WINDOW)
        hit = (start > -PROPS) & (start < LEN)
        return start, pl.multiple_of(base, 16), hit

    def copy_in(b, base):
        return pltpu.make_async_copy(
            keys.at[b, pl.ds(base, WINDOW), :], buf.at[b], in_sem.at[b]
        )

    def copy_out(b, base):
        return pltpu.make_async_copy(
            buf.at[b], keys.at[b, pl.ds(base, WINDOW), :], out_sem.at[b]
        )

    @pl.loop(0, SEQS)
    def _(b):
        start, base, hit = place(b)

        @pl.when(hit)
        def _():
            copy_in(b, base).start()

    for move in moves:
        move[0].start()
    coded = joined[STATS].astype(f32)
    columns[...] = jnp.transpose(coded[0:8] + coded[8:16])

    def patched(b, start, base):
        inv = columns[pl.ds(pl.multiple_of(PROPS * b, PROPS), PROPS), 2:3]
        slot = iota((WINDOW, PROPS), 0) + (base - start)
        selector = jnp.where(slot == iota((WINDOW, PROPS), 1), 1.0, 0.0).astype(bf16)
        raw = joined[b, :, WIDTH:].astype(f32)
        rows = jnp.dot(selector, (inv * raw).astype(bf16), preferred_element_type=f32)
        slot = iota((WINDOW, WIDTH), 0) + (base - start)
        return (slot >= 0) & (slot < PROPS), rows

    for t in range(8):
        moves[t][0].wait()

        @pl.loop(3 * t, 3 * t + 3)
        def _(b):
            start, base, hit = place(b)

            @pl.when(hit)
            def _():
                inside, rows = patched(b, start, base)
                window = pl.ds(base, WINDOW)
                held = near[b, window, :].astype(f32)
                near[b, window, :] = jnp.where(inside, rows[:, WIDTH:], held).astype(bf16)
                copy_in(b, base).wait()
                held = buf[b].astype(f32)
                buf[b] = jnp.where(inside, rows[:, 0:WIDTH], held).astype(bf16)
                copy_out(b, base).start()

        moves[t][1].start()
    for move in moves:
        move[1].wait()

    @pl.loop(0, SEQS)
    def _(b):
        start, base, hit = place(b)

        @pl.when(hit)
        def _():
            copy_out(b, base).wait()


def shards(
    tokens,
    norm_gain,
    w_query,
    w_key,
    w_value,
    w_gate,
    gate_bias,
    w_out,
    keys_cache,
    values_cache,
    cum_gates,
    prior_len,
    accepted,
    parents,
):
    cache = jax.ShapeDtypeStruct(keys_cache.shape, bf16)

    def near(*arrays):
        return [pltpu.with_memory_space_constraint(a, pltpu.VMEM) for a in arrays]

    def far(*arrays):
        return [pltpu.with_memory_space_constraint(a, pltpu.HBM) for a in arrays]

    def limit(mib):
        return pltpu.CompilerParams(vmem_limit_bytes=mib << 20)

    parts, biases = pl.pallas_call(
        project_kernel,
        out_shape=(
            jax.ShapeDtypeStruct((N_KV, PROPS, ROWS), bf16),
            pltpu.VMEM(cum_gates.shape, f32),
        ),
        in_specs=[SM, SM, VM, VM, VM, VM, VM, VM, VM],
        out_specs=(VM, VM),
        scratch_shapes=[pltpu.VMEM((16, ROWS), f32)],
        name="project",
    )(
        prior_len,
        accepted,
        tokens.T,
        norm_gain[None],
        w_query,
        w_key,
        w_value,
        w_gate.T,
        cum_gates,
    )
    arrived = lax.all_to_all(parts, KV, 0, 0, tiled=True)

    keys_copy, ancestors = pl.pallas_call(
        copy_kernel,
        out_shape=(
            cache,
            pltpu.VMEM((PROPS, WIDTH), f32),
        ),
        in_specs=[ANY, SM, ANY],
        out_specs=(ANY, VM),
        scratch_shapes=[
            pltpu.VMEM(keys_cache.shape, bf16),
            pltpu.SemaphoreType.DMA((2, 8)),
        ],
        compiler_params=limit(8),
        cost_estimate=pl.CostEstimate(
            flops=2_000_000_000, bytes_accessed=12_600_000, transcendentals=0
        ),
        name="copy",
    )(*far(parts, parents.T, keys_cache))

    tp_count = lax.axis_size("tp")

    def gathered(name, *pieces):
        return pl.pallas_call(
            join_kernel,
            out_shape=pltpu.VMEM((sum(len(p) for p in pieces), *pieces[0].shape[1:]), bf16),
            in_specs=[VM, VM],
            out_specs=VM,
            compiler_params=limit(2),
            name=name,
        )(*pieces)

    def across(x, bit):
        return lax.ppermute(x, "tp", [(i, i ^ bit) for i in range(tp_count)])

    w_0 = w_out.T
    w_1 = across(w_0, 1)
    w_pair = gathered("pair", *far(w_0[None]), *near(w_1[None]))
    w_2 = across(w_pair, 2)
    w_4 = across(gathered("four", *near(w_pair, w_2)), 4)

    block = pl.pallas_call(
        share_kernel,
        out_shape=pltpu.VMEM((N_KV, PROPS, ROWS), bf16),
        in_specs=[SM, VM, VM, VM],
        out_specs=VM,
        compiler_params=limit(8),
        name="share",
    )(gate_bias, *near(arrived, ancestors, w_4))
    joined = lax.all_to_all(block, KV, 0, 0, tiled=True)

    sent = pl.pallas_call(
        attention_kernel,
        out_shape=pltpu.VMEM((512, WIDTH), bf16),
        in_specs=[VM, VM, VM, ANY, ANY],
        out_specs=VM,
        scratch_shapes=[
            pltpu.VMEM((ROWS, 8), f32),
            pltpu.VMEM((SEQS, 2 * PROPS, LEN), f32),
            pltpu.VMEM((SEQS, 2 * PROPS, LEN), bf16),
            pltpu.VMEM(keys_cache.shape, bf16),
            pltpu.VMEM(keys_cache.shape, bf16),
            pltpu.VMEM((SEQS, 2 * PROPS, WIDTH), f32),
            pltpu.VMEM((SEQS, 2 * PROPS, WIDTH), f32),
            pltpu.VMEM((512, WIDTH), f32),
            pltpu.SemaphoreType.DMA((2, N_TP)),
        ],
        compiler_params=limit(20),
        name="attention",
    )(*near(ancestors, joined, biases), *far(keys_cache, values_cache))
    pieces = lax.all_to_all(sent.reshape(256, 2, WIDTH), (*KV, "tp"), 0, 0, tiled=True)

    combined = pl.pallas_call(
        combine_kernel,
        out_shape=jax.ShapeDtypeStruct((N_KV, PROPS, WIDTH), bf16),
        in_specs=[VM],
        out_specs=VM,
        scratch_shapes=[pltpu.VMEM((64, 8, WIDTH), f32), pltpu.VMEM((64, 8, WIDTH), f32)],
        compiler_params=limit(8),
        name="combine",
    )(*near(pieces.reshape(512, WIDTH)))
    shared = lax.all_to_all(combined, KV, 0, 0, tiled=True)

    keys_out, values_out = pl.pallas_call(
        write_kernel,
        out_shape=(cache, cache),
        in_specs=[SM, SM, VM, ANY, ANY, ANY],
        out_specs=(ANY, ANY),
        input_output_aliases={4: 0},
        scratch_shapes=[
            pltpu.VMEM((SEQS, WINDOW, WIDTH), bf16),
            pltpu.VMEM(keys_cache.shape, bf16),
            pltpu.VMEM((ROWS, 8), f32),
            pltpu.SemaphoreType.DMA((SEQS,)),
            pltpu.SemaphoreType.DMA((SEQS,)),
            pltpu.SemaphoreType.DMA((2, 8)),
        ],
        compiler_params=limit(8),
        cost_estimate=pl.CostEstimate(
            flops=2_000_000_000, bytes_accessed=100_000, transcendentals=0
        ),
        name="write",
    )(
        *far(prior_len, accepted),
        *near(joined),
        *far(combined, keys_copy, values_cache),
    )

    mixed_rows = pl.pallas_call(
        output_kernel,
        out_shape=jax.ShapeDtypeStruct((48, 64), bf16),
        in_specs=[VM] * 5,
        out_specs=VM,
        scratch_shapes=[pltpu.VMEM((512, WIDTH), f32)],
        compiler_params=limit(8),
        name="output",
    )(*near(shared.reshape(512, WIDTH), w_0, w_1, w_2, w_4))
    return (mixed_rows, keys_out, values_out)


def solution(mesh):
    torus = Mesh(mesh.devices.reshape(8, 4, mesh.shape["tp"]), ("kv_0", "kv_1", "tp"))
    in_specs = (
        P(None, KV),
        P(KV),
        P(KV, "tp"),
        P(KV, "tp"),
        P(KV, "tp"),
        P(),
        P(),
        P("tp", KV),
        P(None, KV, "tp"),
        P(None, KV, "tp"),
        P(None, "tp", KV),
        P(),
        P(),
        P(),
    )
    out_specs = (P("tp", KV), P(None, KV, "tp"), P(None, KV, "tp"))
    return jax.shard_map(
        shards, mesh=torus, in_specs=in_specs, out_specs=out_specs, check_vma=False
    )
```

```python
import jax
import jax.numpy as jnp
from jax import lax
from jax.experimental import pallas as pl
from jax.experimental.pallas import tpu as pltpu
from jax.sharding import Mesh
from jax.sharding import PartitionSpec as P

D = 2048
HEAD = 64
PROPS = 16
ROWS = 384
SEQS = 24
LEN = 512
WIDTH = 128
N_KV = 32
N_TP = 8
STATS = 24
WINDOW = 32
KV = ("kv_0", "kv_1")

masked_score = -1e30
lowest_max = -1e20
norm_eps = 1e-06

VM = pl.BlockSpec(memory_space=pltpu.VMEM)
SM = pl.BlockSpec(memory_space=pltpu.SMEM)
ANY = pl.BlockSpec(memory_space=pl.ANY)
bf16 = jnp.bfloat16
f32 = jnp.float32


def iota(shape, dim):
    return lax.broadcasted_iota(jnp.int32, shape, dim)


def high_low(x):
    high = x.astype(bf16).astype(f32)
    return high, (x - high).astype(bf16).astype(f32)


def dot_t(a, b):
    return lax.dot_general(a, b, (((1,), (1,)), ((), ())), preferred_element_type=f32)


def project_kernel(
    prior, accepted, tokens, gain, w_q, w_k, w_v, w_gate, cum, out, bias, gates
):
    kv, tp = lax.axis_index(KV), lax.axis_index("tp")
    columns = pl.ds(pl.multiple_of(lax.div(kv, 2) * WIDTH, WIDTH), WIDTH)
    floats = tokens[...].astype(f32)
    same = iota((64, 64), 0) == iota((64, 64), 1)
    gain_column = jnp.sum(jnp.where(same, gain[...], 0.0), axis=1, keepdims=True)
    scaled = floats * gain_column
    rows = jnp.transpose(scaled).astype(bf16)
    scaled = scaled.astype(bf16)
    for n, w in enumerate((w_q, w_k, w_v)):
        part = jnp.dot(rows, w[...], preferred_element_type=f32).astype(bf16)
        out[0:SEQS, :, n * WIDTH : (n + 1) * WIDTH] = part.reshape(SEQS, PROPS, WIDTH)
    sq_high, sq_low = high_low(floats * floats)
    ones = jnp.ones((8, 64), bf16)
    square_sum = jnp.dot(ones, sq_high.astype(bf16), preferred_element_type=f32) + jnp.dot(
        ones, sq_low.astype(bf16), preferred_element_type=f32
    )
    lane = iota((2, WIDTH), 1)
    position = iota((2, LEN), 1)
    last = jnp.zeros((2, WIDTH), f32)
    for b in range(SEQS):
        at = prior[b] + accepted[b] - 1 - kv * LEN
        here = cum[b]
        bias[b] = jnp.where(position <= at, -here, masked_score)
        found = jnp.sum(jnp.where(position == at, here, 0.0), axis=1, keepdims=True)
        last = jnp.where(lane == b, found, last)
    last_high, last_low = high_low(last)
    rest = last - last_high - last_low
    odd = lax.rem(kv, 2)
    zero = jnp.zeros_like(scaled)
    both = jnp.concatenate(
        [jnp.where(odd == 0, scaled, zero), jnp.where(odd == 1, scaled, zero)], axis=0
    )
    gates[...] = jnp.dot(w_gate[:, columns], both, preferred_element_type=f32)
    row = iota((8, ROWS), 0)
    gate_0 = gates[pl.ds(2 * tp, 1), :]
    gate_1 = gates[pl.ds(2 * tp + 1, 1), :]
    stats = jnp.where(row == 0, gate_0, jnp.where(row == 1, gate_1, 0.0))
    stats = jnp.where(row == 2, square_sum, stats)
    wide = jnp.zeros((2, ROWS - WIDTH), f32)
    last = jnp.concatenate([last, wide], axis=1)
    rest = jnp.concatenate([rest, wide], axis=1)
    stats = jnp.where(row == 3, last[0:1], jnp.where(row == 4, last[1:2], stats))
    stats = jnp.where(row == 5, rest[0:1], jnp.where(row == 6, rest[1:2], stats))
    out[STATS] = jnp.concatenate(high_low(stats), axis=0).astype(bf16)
    out[STATS + 1 :] = jnp.zeros((N_KV - STATS - 1, PROPS, ROWS), bf16)


def share_kernel(bias, parts, out):
    kv, tp = lax.axis_index(KV), lax.axis_index("tp")
    total = jnp.zeros((PROPS, ROWS), f32)
    for k in range(N_KV):
        total = total + parts[k].astype(f32)
    stats = total[0:8] + total[8:16]
    row = iota((8, ROWS), 0)
    inv_rms = lax.rsqrt(stats[2:3] / D + norm_eps)
    logits = inv_rms * stats + jnp.where(row == 0, bias[2 * tp], bias[2 * tp + 1])
    log_gates = jnp.minimum(logits, 0.0) - jnp.log1p(jnp.exp(-jnp.abs(logits)))
    stats = jnp.where(row < 2, log_gates, jnp.where(row == 2, inv_rms, stats))
    stats = jnp.concatenate(high_low(stats), axis=0)
    block = jnp.where(kv == STATS, stats, total).astype(bf16)
    for k in range(N_KV):
        out[k] = block


def attention_kernel(
    parents,
    joined,
    biases,
    keys,
    values,
    out,
    keys_out,
    values_out,
    columns,
    scores_buf,
    weights_buf,
    v_buf,
    stat_buf,
    mixed,
    sems,
):
    kv = lax.axis_index(KV)
    moves = []
    for n, (source, target) in enumerate(((keys, keys_out), (values, values_out))):
        for t in range(4):
            six = pl.ds(6 * t, 6)
            moves.append(pltpu.make_async_copy(source.at[six], target.at[six], sems.at[n, t]))
    for move in moves:
        move.start()
    coded = joined[STATS].astype(f32)
    stats = coded[0:8] + coded[8:16]
    columns[...] = jnp.transpose(stats)
    lane = iota((PROPS, WIDTH), 1)
    first_head = lane < HEAD
    lane_out = iota((2 * PROPS, WIDTH), 1)
    first_row = iota((2 * PROPS, WIDTH), 0) < PROPS
    scale = HEAD**-0.5

    def both_heads(b_rows, b_block):
        inv = columns[b_rows, 2:3]
        q = (inv * joined[b_block, :, 0:WIDTH].astype(f32)).astype(bf16).astype(f32) * scale
        zero = jnp.zeros_like(q)
        return jnp.concatenate(
            [jnp.where(first_head, q, zero), jnp.where(first_head, zero, q)], axis=0
        ).astype(bf16)

    def coded_stats(s, top, total):
        place = lane_out - (HEAD + 4 * s)
        top_high, top_low = high_low(top)
        sum_high, sum_low = high_low(total)
        stats = jnp.where(place == 0, top_high, jnp.where(place == 1, top_low, 0.0))
        return jnp.where(place == 2, sum_high, jnp.where(place == 3, sum_low, stats))

    def sendable(top):
        high, low = high_low(jnp.maximum(top, lowest_max))
        return high + low

    own = jnp.minimum(kv, SEQS - 1)
    low = lane_out < HEAD

    def score(b):
        q = both_heads(pl.ds(PROPS * b, PROPS), b)
        bias = biases[b]
        bias = jnp.concatenate(
            [
                jnp.broadcast_to(bias[0:1], (PROPS, LEN)),
                jnp.broadcast_to(bias[1:2], (PROPS, LEN)),
            ],
            axis=0,
        )
        scores_buf[b] = dot_t(q, keys[b]) + bias

    def weigh(b):
        scores = scores_buf[b]
        top = sendable(jnp.max(scores, axis=1, keepdims=True))
        weights = jnp.exp(scores - top)
        total = jnp.sum(weights, axis=1, keepdims=True)
        weights_buf[b] = weights.astype(bf16)
        stat_buf[b] = coded_stats(b % 3, top, total)

    def gather(b):
        v_buf[b] = jnp.dot(weights_buf[b], values[b], preferred_element_type=f32)

    def pack(t):
        v = [v_buf[3 * t + s] for s in range(3)]
        turned = [pltpu.roll(x, HEAD, 1) for x in v]
        first = jnp.where(first_row, v[0], turned[0])
        second = jnp.where(first_row, turned[1], v[1])
        third = jnp.where(first_row, v[2], turned[2])
        stats = stat_buf[3 * t] + stat_buf[3 * t + 1] + stat_buf[3 * t + 2]
        mixed[pl.ds(2 * t, N_KV, stride=16), :] = jnp.where(low, first, second)
        mixed[pl.ds(2 * t + 1, N_KV, stride=16), :] = jnp.where(low, third, stats)

    def lineage():
        row = iota((PROPS, WIDTH), 0)
        linked = jnp.where(lane == row, 1.0, 0.0)
        for i in range(PROPS):
            linked = jnp.where((row == i) & (lane == parents[i, own]), 1.0, linked)
        return linked

    def squared(linked):
        other = jnp.concatenate([linked, jnp.zeros((WIDTH - PROPS, WIDTH), f32)], axis=0)
        product = jnp.dot(linked.astype(bf16), other.astype(bf16), preferred_element_type=f32)
        return jnp.minimum(product, 1.0)

    def tree(reached):
        mine = pl.ds(pl.multiple_of(PROPS * own, PROPS), PROPS)
        pad = jnp.zeros((WIDTH - PROPS, WIDTH), f32)
        picks = (iota((ROWS, WIDTH), 0) == iota((ROWS, WIDTH), 1) + PROPS * own) & (
            iota((ROWS, WIDTH), 1) < PROPS
        )
        own_gates = jnp.dot(
            joined[STATS], jnp.where(picks, 1.0, 0.0).astype(bf16), preferred_element_type=f32
        ).astype(bf16)
        tree = dot_t(own_gates, jnp.concatenate([reached, pad], axis=0).astype(bf16))
        tree = tree[0:8] + tree[8:16]
        last = jnp.sum(
            jnp.where(iota((8, WIDTH), 1) == own, stats[:, 0:WIDTH], 0.0), axis=1, keepdims=True
        )
        tree_bias = jnp.concatenate(
            [
                jnp.broadcast_to(-(last[3:4] + last[5:6] + tree[0:1]), (PROPS, WIDTH)),
                jnp.broadcast_to(-(last[4:5] + last[6:7] + tree[1:2]), (PROPS, WIDTH)),
            ],
            axis=0,
        )
        own_inv = columns[mine, 2:3]
        new_keys = own_inv * joined[own, :, WIDTH : 2 * WIDTH].astype(f32)
        new_values = own_inv * joined[own, :, 2 * WIDTH : 3 * WIDTH].astype(f32)
        new_keys = jnp.concatenate([new_keys, pad], axis=0).astype(bf16)
        new_values = jnp.concatenate([new_values, pad], axis=0).astype(bf16)
        needed = jnp.where(kv < SEQS, 0.5, 2.0)
        live = jnp.concatenate([reached, reached], axis=0) > needed
        tree_scores = jnp.where(live, dot_t(both_heads(mine, own), new_keys) + tree_bias, masked_score)
        tree_top = jnp.max(tree_scores, axis=1, keepdims=True)
        return tree_scores, tree_top, new_values

    for step in range(N_TP + 2):
        for s in range(3):
            if step < N_TP:
                score(3 * step + s)
            if 1 <= step <= N_TP:
                weigh(3 * step - 3 + s)
            if step >= 2:
                gather(3 * step - 6 + s)
        if step == 0:
            reached = lineage()
        if 1 <= step <= 4:
            reached = squared(reached)
        if step == 5:
            tree_scores, tree_top, new_values = tree(reached)
        if step == N_TP:
            scores = scores_buf[own]
            top = jnp.maximum(jnp.max(scores, axis=1, keepdims=True), tree_top)
            top = sendable(top)
            own_weights = jnp.exp(scores - top)
            tree_weights = jnp.exp(tree_scores - top)
            own_total = jnp.sum(own_weights, axis=1, keepdims=True) + jnp.sum(
                tree_weights, axis=1, keepdims=True
            )
            own_stats = coded_stats(lax.rem(own, 3), top, own_total)
    own_v = jnp.dot(
        own_weights.astype(bf16), values[own], preferred_element_type=f32
    ) + jnp.dot(tree_weights.astype(bf16), new_values, preferred_element_type=f32)
    stat_buf[own] = own_stats
    v_buf[own] = own_v
    for t in range(N_TP):
        pack(t)
    out[...] = mixed[...].astype(bf16)
    for move in moves:
        move.wait()


def combine_kernel(parts, after_w, out, tops, sums):
    row = iota((WIDTH, 4 * WIDTH), 0) - HEAD
    column = iota((WIDTH, 4 * WIDTH), 1)
    unit = jnp.where(column < 2 * WIDTH, lax.rem(lax.div(column, HEAD), 2), 2)
    kind = lax.rem(lax.div(column, WIDTH), 2)
    row = row - 4 * unit - 2 * kind
    spread = jnp.where((row == 0) | (row == 1), 1.0, 0.0).astype(bf16)
    even = lax.rem(iota((8, WIDTH), 0), 2) == 0
    for n in range(4):
        stats = jnp.dot(parts[128 * n : 128 * n + 128], spread, preferred_element_type=f32)
        for v in range(16):
            rows = stats[8 * v : 8 * v + 8]
            near = pltpu.roll(rows[:, 0 : 2 * WIDTH], 7, 0)
            tops[16 * n + v] = jnp.where(even, near[:, 0:WIDTH], rows[:, 2 * WIDTH : 3 * WIDTH])
            sums[16 * n + v] = jnp.where(even, near[:, WIDTH:], rows[:, 3 * WIDTH :])
    results = []
    for half in range(2):
        top = tops[half]
        for k in range(1, N_KV):
            top = jnp.maximum(top, tops[2 * k + half])
        above = jnp.zeros((8, WIDTH), f32)
        below = jnp.zeros((8, WIDTH), f32)
        for k in range(N_KV):
            v = 2 * k + half
            factor = jnp.exp(tops[v] - top)
            above = above + factor * parts[8 * v : 8 * v + 8, :].astype(f32)
            below = below + factor * sums[v]
        results.append(above / below)
    block = jnp.concatenate(results, axis=0).astype(bf16)
    for k in range(N_KV):
        out[k] = block


def output_kernel(shared, w_0, w_1, w_2, w_4, out, rows):
    tp = lax.axis_index("tp")
    rows[...] = shared[...].astype(f32)
    near = (w_0[...], w_1[...], w_2[0], w_2[1], w_4[0], w_4[1], w_4[2], w_4[3])
    near = [w.astype(f32) for w in near]
    for bit in (1, 2, 4):
        swap = (tp & bit) != 0
        near = [jnp.where(swap, near[g ^ bit], near[g]) for g in range(N_TP)]
    low = iota((PROPS, WIDTH), 1) < HEAD
    total = jnp.zeros((48, 64), f32)
    for g in range(N_TP):
        pair_0 = rows[pl.ds(2 * g, PROPS, stride=16), :]
        pair_1 = rows[pl.ds(256 + 2 * g, PROPS, stride=16), :]
        last_0 = rows[pl.ds(2 * g + 1, PROPS, stride=16), :]
        last_1 = rows[pl.ds(257 + 2 * g, PROPS, stride=16), :]
        block = jnp.concatenate(
            [
                jnp.where(low, pair_0, pltpu.roll(pair_1, HEAD, 1)),
                jnp.where(low, pltpu.roll(pair_0, HEAD, 1), pair_1),
                jnp.where(low, last_0, pltpu.roll(last_1, HEAD, 1)),
            ],
            axis=0,
        )
        total = total + dot_t(block.astype(bf16), near[g].astype(bf16))
    out[...] = total.astype(bf16)


def join_kernel(first, second, out):
    count = first.shape[0]
    out[0:count] = first[...]
    out[count:] = second[...]


def write_kernel(
    prior, accepted, joined, after, keys_in, values_in, keys, values, buf, columns, in_sem, out_sem
):
    offset = lax.axis_index(KV) * LEN
    coded = joined[STATS].astype(f32)
    columns[...] = jnp.transpose(coded[0:8] + coded[8:16])

    def place(b):
        start = prior[b] + accepted[b] - offset
        base = jnp.clip(lax.div(jnp.maximum(start, 0), 16) * 16, 0, LEN - WINDOW)
        hit = (start > -PROPS) & (start < LEN)
        return start, pl.multiple_of(base, 16), hit

    def copy_in(n, b, base):
        source = (keys, values)[n].at[b, pl.ds(base, WINDOW), :]
        return pltpu.make_async_copy(source, buf.at[n, b], in_sem.at[n, b])

    def copy_out(n, b, base):
        target = (keys, values)[n].at[b, pl.ds(base, WINDOW), :]
        return pltpu.make_async_copy(buf.at[n, b], target, out_sem.at[n, b])

    @pl.loop(0, SEQS)
    def _(b):
        start, base, hit = place(b)

        @pl.when(hit)
        def _():
            for n in range(2):
                copy_in(n, b, base).start()

    @pl.loop(0, SEQS)
    def _(b):
        start, base, hit = place(b)

        @pl.when(hit)
        def _():
            inv = columns[pl.ds(pl.multiple_of(PROPS * b, PROPS), PROPS), 2:3]
            slot = iota((WINDOW, PROPS), 0) + (base - start)
            selector = jnp.where(slot == iota((WINDOW, PROPS), 1), 1.0, 0.0).astype(bf16)
            slot = iota((WINDOW, WIDTH), 0) + (base - start)
            inside = (slot >= 0) & (slot < PROPS)
            for n in range(2):
                raw = joined[b, :, (n + 1) * WIDTH : (n + 2) * WIDTH].astype(f32)
                rows = jnp.dot(selector, (inv * raw).astype(bf16), preferred_element_type=f32)
                copy_in(n, b, base).wait()
                held = buf[n, b].astype(f32)
                buf[n, b] = jnp.where(inside, rows, held).astype(bf16)
                copy_out(n, b, base).start()

    @pl.loop(0, SEQS)
    def _(b):
        start, base, hit = place(b)

        @pl.when(hit)
        def _():
            for n in range(2):
                copy_out(n, b, base).wait()


def shards(
    tokens,
    norm_gain,
    w_query,
    w_key,
    w_value,
    w_gate,
    gate_bias,
    w_out,
    keys_cache,
    values_cache,
    cum_gates,
    prior_len,
    accepted,
    parents,
):
    cache = jax.ShapeDtypeStruct(keys_cache.shape, bf16)

    def near(*arrays):
        return [pltpu.with_memory_space_constraint(a, pltpu.VMEM) for a in arrays]

    def far(*arrays):
        return [pltpu.with_memory_space_constraint(a, pltpu.HBM) for a in arrays]

    def limit(mib):
        return pltpu.CompilerParams(vmem_limit_bytes=mib << 20)

    parts, biases = pl.pallas_call(
        project_kernel,
        out_shape=(
            pltpu.VMEM((N_KV, PROPS, ROWS), bf16),
            pltpu.VMEM(cum_gates.shape, f32),
        ),
        in_specs=[SM, SM, VM, VM, VM, VM, VM, VM, VM],
        out_specs=(VM, VM),
        scratch_shapes=[pltpu.VMEM((16, ROWS), f32)],
        name="project",
    )(
        prior_len,
        accepted,
        tokens.T,
        norm_gain[None],
        w_query,
        w_key,
        w_value,
        w_gate.T,
        cum_gates,
    )
    arrived = lax.all_to_all(parts, KV, 0, 0, tiled=True)

    tp_count = lax.axis_size("tp")

    def gathered(name, *pieces):
        return pl.pallas_call(
            join_kernel,
            out_shape=pltpu.VMEM((sum(len(p) for p in pieces), *pieces[0].shape[1:]), bf16),
            in_specs=[VM, VM],
            out_specs=VM,
            compiler_params=limit(2),
            name=name,
        )(*pieces)

    def across(x, bit):
        return lax.ppermute(x, "tp", [(i, i ^ bit) for i in range(tp_count)])

    w_0 = w_out.T
    w_1 = across(w_0, 1)
    w_pair = gathered("pair", *far(w_0[None]), *near(w_1[None]))
    w_2 = across(w_pair, 2)
    w_4 = across(gathered("four", *near(w_pair, w_2)), 4)

    block = pl.pallas_call(
        share_kernel,
        out_shape=pltpu.VMEM((N_KV, PROPS, ROWS), bf16),
        in_specs=[SM, VM],
        out_specs=VM,
        compiler_params=limit(8),
        cost_estimate=pl.CostEstimate(
            flops=10_000_000_000, bytes_accessed=800_000, transcendentals=0
        ),
        name="share",
    )(*far(gate_bias), *near(arrived))
    joined = lax.all_to_all(block, KV, 0, 0, tiled=True)

    sent, keys_copy, values_copy = pl.pallas_call(
        attention_kernel,
        out_shape=(jax.ShapeDtypeStruct((512, WIDTH), bf16), cache, cache),
        in_specs=[SM, VM, VM, VM, VM],
        out_specs=(VM, ANY, ANY),
        scratch_shapes=[
            pltpu.VMEM((ROWS, 8), f32),
            pltpu.VMEM((SEQS, 2 * PROPS, LEN), f32),
            pltpu.VMEM((SEQS, 2 * PROPS, LEN), bf16),
            pltpu.VMEM((SEQS, 2 * PROPS, WIDTH), f32),
            pltpu.VMEM((SEQS, 2 * PROPS, WIDTH), f32),
            pltpu.VMEM((512, WIDTH), f32),
            pltpu.SemaphoreType.DMA((2, 4)),
        ],
        compiler_params=limit(12),
        name="attention",
    )(*far(parents.T), *near(joined, biases, keys_cache, values_cache))
    pieces = lax.all_to_all(sent.reshape(256, 2, WIDTH), (*KV, "tp"), 0, 0, tiled=True)

    combined = pl.pallas_call(
        combine_kernel,
        out_shape=jax.ShapeDtypeStruct((N_KV, PROPS, WIDTH), bf16),
        in_specs=[VM, VM],
        out_specs=VM,
        scratch_shapes=[pltpu.VMEM((64, 8, WIDTH), f32), pltpu.VMEM((64, 8, WIDTH), f32)],
        compiler_params=limit(8),
        name="combine",
    )(*near(pieces.reshape(512, WIDTH), w_4))
    shared = lax.all_to_all(combined, KV, 0, 0, tiled=True)

    keys_out, values_out = pl.pallas_call(
        write_kernel,
        out_shape=(cache, cache),
        in_specs=[SM, SM, VM, ANY, ANY, ANY],
        out_specs=(ANY, ANY),
        input_output_aliases={4: 0, 5: 1},
        scratch_shapes=[
            pltpu.VMEM((2, SEQS, WINDOW, WIDTH), bf16),
            pltpu.VMEM((ROWS, 8), f32),
            pltpu.SemaphoreType.DMA((2, SEQS)),
            pltpu.SemaphoreType.DMA((2, SEQS)),
        ],
        compiler_params=limit(8),
        cost_estimate=pl.CostEstimate(
            flops=2_000_000_000, bytes_accessed=100_000, transcendentals=0
        ),
        name="write",
    )(
        *far(prior_len, accepted),
        *near(joined),
        *far(combined, keys_copy, values_copy),
    )

    mixed_rows = pl.pallas_call(
        output_kernel,
        out_shape=jax.ShapeDtypeStruct((48, 64), bf16),
        in_specs=[VM] * 5,
        out_specs=VM,
        scratch_shapes=[pltpu.VMEM((512, WIDTH), f32)],
        compiler_params=limit(8),
        name="output",
    )(*near(shared.reshape(512, WIDTH), w_0, w_1, w_2, w_4))
    return (mixed_rows, keys_out, values_out)


def solution(mesh):
    torus = Mesh(mesh.devices.reshape(8, 4, mesh.shape["tp"]), ("kv_0", "kv_1", "tp"))
    in_specs = (
        P(None, KV),
        P(KV),
        P(KV, "tp"),
        P(KV, "tp"),
        P(KV, "tp"),
        P(),
        P(),
        P("tp", KV),
        P(None, KV, "tp"),
        P(None, KV, "tp"),
        P(None, "tp", KV),
        P(),
        P(),
        P(),
    )
    out_specs = (P("tp", KV), P(None, KV, "tp"), P(None, KV, "tp"))
    return jax.shard_map(
        shards, mesh=torus, in_specs=in_specs, out_specs=out_specs, check_vma=False
    )
```

```python
import jax
import jax.numpy as jnp
from jax import lax
from jax.experimental import pallas as pl
from jax.experimental.pallas import tpu as pltpu
from jax.sharding import Mesh
from jax.sharding import PartitionSpec as P

D = 2048
HEAD = 64
PROPS = 16
ROWS = 384
SEQS = 24
LEN = 512
WIDTH = 128
N_KV = 32
N_TP = 8
STATS = 24
WINDOW = 32
KV = ("kv_0", "kv_1")

masked_score = -1e30
lowest_max = -1e20
norm_eps = 1e-06

VM = pl.BlockSpec(memory_space=pltpu.VMEM)
SM = pl.BlockSpec(memory_space=pltpu.SMEM)
ANY = pl.BlockSpec(memory_space=pl.ANY)
bf16 = jnp.bfloat16
f32 = jnp.float32


def iota(shape, dim):
    return lax.broadcasted_iota(jnp.int32, shape, dim)


def high_low(x):
    high = x.astype(bf16).astype(f32)
    return high, (x - high).astype(bf16).astype(f32)


def dot_t(a, b):
    return lax.dot_general(a, b, (((1,), (1,)), ((), ())), preferred_element_type=f32)


def project_kernel(
    prior, accepted, tokens, gain, w_q, w_k, w_v, w_gate, cum, out, bias, gates
):
    kv, tp = lax.axis_index(KV), lax.axis_index("tp")
    columns = pl.ds(pl.multiple_of(lax.div(kv, 2) * WIDTH, WIDTH), WIDTH)
    floats = tokens[...].astype(f32)
    same = iota((64, 64), 0) == iota((64, 64), 1)
    gain_column = jnp.sum(jnp.where(same, gain[...], 0.0), axis=1, keepdims=True)
    scaled = floats * gain_column
    rows = jnp.transpose(scaled).astype(bf16)
    scaled = scaled.astype(bf16)
    for n, w in enumerate((w_q, w_k, w_v)):
        part = jnp.dot(rows, w[...], preferred_element_type=f32).astype(bf16)
        out[0:SEQS, :, n * WIDTH : (n + 1) * WIDTH] = part.reshape(SEQS, PROPS, WIDTH)
    sq_high, sq_low = high_low(floats * floats)
    ones = jnp.ones((8, 64), bf16)
    square_sum = jnp.dot(ones, sq_high.astype(bf16), preferred_element_type=f32) + jnp.dot(
        ones, sq_low.astype(bf16), preferred_element_type=f32
    )
    lane = iota((2, WIDTH), 1)
    position = iota((2, LEN), 1)
    last = jnp.zeros((2, WIDTH), f32)
    for b in range(SEQS):
        at = prior[b] + accepted[b] - 1 - kv * LEN
        here = cum[b]
        bias[b] = jnp.where(position <= at, -here, masked_score)
        found = jnp.sum(jnp.where(position == at, here, 0.0), axis=1, keepdims=True)
        last = jnp.where(lane == b, found, last)
    last_high, last_low = high_low(last)
    rest = last - last_high - last_low
    odd = lax.rem(kv, 2)
    zero = jnp.zeros_like(scaled)
    both = jnp.concatenate(
        [jnp.where(odd == 0, scaled, zero), jnp.where(odd == 1, scaled, zero)], axis=0
    )
    gates[...] = jnp.dot(w_gate[:, columns], both, preferred_element_type=f32)
    row = iota((8, ROWS), 0)
    gate_0 = gates[pl.ds(2 * tp, 1), :]
    gate_1 = gates[pl.ds(2 * tp + 1, 1), :]
    stats = jnp.where(row == 0, gate_0, jnp.where(row == 1, gate_1, 0.0))
    stats = jnp.where(row == 2, square_sum, stats)
    wide = jnp.zeros((2, ROWS - WIDTH), f32)
    last = jnp.concatenate([last, wide], axis=1)
    rest = jnp.concatenate([rest, wide], axis=1)
    stats = jnp.where(row == 3, last[0:1], jnp.where(row == 4, last[1:2], stats))
    stats = jnp.where(row == 5, rest[0:1], jnp.where(row == 6, rest[1:2], stats))
    out[STATS] = jnp.concatenate(high_low(stats), axis=0).astype(bf16)
    out[STATS + 1 :] = jnp.zeros((N_KV - STATS - 1, PROPS, ROWS), bf16)


def share_kernel(bias, parts, after_w, out):
    kv, tp = lax.axis_index(KV), lax.axis_index("tp")
    total = jnp.zeros((PROPS, ROWS), f32)
    for k in range(N_KV):
        total = total + parts[k].astype(f32)
    stats = total[0:8] + total[8:16]
    row = iota((8, ROWS), 0)
    inv_rms = lax.rsqrt(stats[2:3] / D + norm_eps)
    logits = inv_rms * stats + jnp.where(row == 0, bias[2 * tp], bias[2 * tp + 1])
    log_gates = jnp.minimum(logits, 0.0) - jnp.log1p(jnp.exp(-jnp.abs(logits)))
    stats = jnp.where(row < 2, log_gates, jnp.where(row == 2, inv_rms, stats))
    stats = jnp.concatenate(high_low(stats), axis=0)
    block = jnp.where(kv == STATS, stats, total).astype(bf16)
    for k in range(N_KV):
        out[k] = block


def attention_kernel(
    parents,
    joined,
    biases,
    keys,
    values,
    out,
    keys_out,
    columns,
    scores_buf,
    weights_buf,
    v_buf,
    stat_buf,
    mixed,
    sems,
):
    kv = lax.axis_index(KV)
    moves = []
    for t in range(4):
        six = pl.ds(6 * t, 6)
        moves.append(pltpu.make_async_copy(keys.at[six], keys_out.at[six], sems.at[t]))
    for move in moves:
        move.start()
    coded = joined[STATS].astype(f32)
    stats = coded[0:8] + coded[8:16]
    columns[...] = jnp.transpose(stats)
    lane = iota((PROPS, WIDTH), 1)
    first_head = lane < HEAD
    lane_out = iota((2 * PROPS, WIDTH), 1)
    first_row = iota((2 * PROPS, WIDTH), 0) < PROPS
    scale = HEAD**-0.5

    def both_heads(b_rows, b_block):
        inv = columns[b_rows, 2:3]
        q = (inv * joined[b_block, :, 0:WIDTH].astype(f32)).astype(bf16).astype(f32) * scale
        zero = jnp.zeros_like(q)
        return jnp.concatenate(
            [jnp.where(first_head, q, zero), jnp.where(first_head, zero, q)], axis=0
        ).astype(bf16)

    def coded_stats(s, top, total):
        place = lane_out - (HEAD + 4 * s)
        top_high, top_low = high_low(top)
        sum_high, sum_low = high_low(total)
        stats = jnp.where(place == 0, top_high, jnp.where(place == 1, top_low, 0.0))
        return jnp.where(place == 2, sum_high, jnp.where(place == 3, sum_low, stats))

    def sendable(top):
        high, low = high_low(jnp.maximum(top, lowest_max))
        return high + low

    own = jnp.minimum(kv, SEQS - 1)
    low = lane_out < HEAD

    def score(b):
        q = both_heads(pl.ds(PROPS * b, PROPS), b)
        bias = biases[b]
        bias = jnp.concatenate(
            [
                jnp.broadcast_to(bias[0:1], (PROPS, LEN)),
                jnp.broadcast_to(bias[1:2], (PROPS, LEN)),
            ],
            axis=0,
        )
        scores_buf[b] = dot_t(q, keys[b]) + bias

    def weigh(b):
        scores = scores_buf[b]
        top = sendable(jnp.max(scores, axis=1, keepdims=True))
        weights = jnp.exp(scores - top)
        total = jnp.sum(weights, axis=1, keepdims=True)
        weights_buf[b] = weights.astype(bf16)
        stat_buf[b] = coded_stats(b % 3, top, total)

    def gather(b):
        v_buf[b] = jnp.dot(weights_buf[b], values[b], preferred_element_type=f32)

    def pack(t):
        v = [v_buf[3 * t + s] for s in range(3)]
        turned = [pltpu.roll(x, HEAD, 1) for x in v]
        first = jnp.where(first_row, v[0], turned[0])
        second = jnp.where(first_row, turned[1], v[1])
        third = jnp.where(first_row, v[2], turned[2])
        stats = stat_buf[3 * t] + stat_buf[3 * t + 1] + stat_buf[3 * t + 2]
        mixed[pl.ds(2 * t, N_KV, stride=16), :] = jnp.where(low, first, second)
        mixed[pl.ds(2 * t + 1, N_KV, stride=16), :] = jnp.where(low, third, stats)

    def lineage():
        row = iota((PROPS, WIDTH), 0)
        linked = jnp.where(lane == row, 1.0, 0.0)
        for i in range(PROPS):
            linked = jnp.where((row == i) & (lane == parents[i, own]), 1.0, linked)
        return linked

    def squared(linked):
        other = jnp.concatenate([linked, jnp.zeros((WIDTH - PROPS, WIDTH), f32)], axis=0)
        product = jnp.dot(linked.astype(bf16), other.astype(bf16), preferred_element_type=f32)
        return jnp.minimum(product, 1.0)

    def tree(reached):
        mine = pl.ds(pl.multiple_of(PROPS * own, PROPS), PROPS)
        pad = jnp.zeros((WIDTH - PROPS, WIDTH), f32)
        picks = (iota((ROWS, WIDTH), 0) == iota((ROWS, WIDTH), 1) + PROPS * own) & (
            iota((ROWS, WIDTH), 1) < PROPS
        )
        own_gates = jnp.dot(
            joined[STATS], jnp.where(picks, 1.0, 0.0).astype(bf16), preferred_element_type=f32
        ).astype(bf16)
        tree = dot_t(own_gates, jnp.concatenate([reached, pad], axis=0).astype(bf16))
        tree = tree[0:8] + tree[8:16]
        last = jnp.sum(
            jnp.where(iota((8, WIDTH), 1) == own, stats[:, 0:WIDTH], 0.0), axis=1, keepdims=True
        )
        tree_bias = jnp.concatenate(
            [
                jnp.broadcast_to(-(last[3:4] + last[5:6] + tree[0:1]), (PROPS, WIDTH)),
                jnp.broadcast_to(-(last[4:5] + last[6:7] + tree[1:2]), (PROPS, WIDTH)),
            ],
            axis=0,
        )
        own_inv = columns[mine, 2:3]
        new_keys = own_inv * joined[own, :, WIDTH : 2 * WIDTH].astype(f32)
        new_values = own_inv * joined[own, :, 2 * WIDTH : 3 * WIDTH].astype(f32)
        new_keys = jnp.concatenate([new_keys, pad], axis=0).astype(bf16)
        new_values = jnp.concatenate([new_values, pad], axis=0).astype(bf16)
        needed = jnp.where(kv < SEQS, 0.5, 2.0)
        live = jnp.concatenate([reached, reached], axis=0) > needed
        tree_scores = jnp.where(live, dot_t(both_heads(mine, own), new_keys) + tree_bias, masked_score)
        tree_top = jnp.max(tree_scores, axis=1, keepdims=True)
        return tree_scores, tree_top, new_values

    for step in range(N_TP + 2):
        for s in range(3):
            if step < N_TP:
                score(3 * step + s)
            if 1 <= step <= N_TP:
                weigh(3 * step - 3 + s)
            if step >= 2:
                gather(3 * step - 6 + s)
        if step == 0:
            reached = lineage()
        if 1 <= step <= 4:
            reached = squared(reached)
        if step == 5:
            tree_scores, tree_top, new_values = tree(reached)
        if step == N_TP:
            scores = scores_buf[own]
            top = jnp.maximum(jnp.max(scores, axis=1, keepdims=True), tree_top)
            top = sendable(top)
            own_weights = jnp.exp(scores - top)
            tree_weights = jnp.exp(tree_scores - top)
            own_total = jnp.sum(own_weights, axis=1, keepdims=True) + jnp.sum(
                tree_weights, axis=1, keepdims=True
            )
            own_stats = coded_stats(lax.rem(own, 3), top, own_total)
    own_v = jnp.dot(
        own_weights.astype(bf16), values[own], preferred_element_type=f32
    ) + jnp.dot(tree_weights.astype(bf16), new_values, preferred_element_type=f32)
    stat_buf[own] = own_stats
    v_buf[own] = own_v
    for t in range(N_TP):
        pack(t)
    out[...] = mixed[...].astype(bf16)
    for move in moves:
        move.wait()


def combine_kernel(parts, out, tops, sums):
    row = iota((WIDTH, 4 * WIDTH), 0) - HEAD
    column = iota((WIDTH, 4 * WIDTH), 1)
    unit = jnp.where(column < 2 * WIDTH, lax.rem(lax.div(column, HEAD), 2), 2)
    kind = lax.rem(lax.div(column, WIDTH), 2)
    row = row - 4 * unit - 2 * kind
    spread = jnp.where((row == 0) | (row == 1), 1.0, 0.0).astype(bf16)
    even = lax.rem(iota((8, WIDTH), 0), 2) == 0
    for n in range(4):
        stats = jnp.dot(parts[128 * n : 128 * n + 128], spread, preferred_element_type=f32)
        for v in range(16):
            rows = stats[8 * v : 8 * v + 8]
            near = pltpu.roll(rows[:, 0 : 2 * WIDTH], 7, 0)
            tops[16 * n + v] = jnp.where(even, near[:, 0:WIDTH], rows[:, 2 * WIDTH : 3 * WIDTH])
            sums[16 * n + v] = jnp.where(even, near[:, WIDTH:], rows[:, 3 * WIDTH :])
    results = []
    for half in range(2):
        top = tops[half]
        for k in range(1, N_KV):
            top = jnp.maximum(top, tops[2 * k + half])
        above = jnp.zeros((8, WIDTH), f32)
        below = jnp.zeros((8, WIDTH), f32)
        for k in range(N_KV):
            v = 2 * k + half
            factor = jnp.exp(tops[v] - top)
            above = above + factor * parts[8 * v : 8 * v + 8, :].astype(f32)
            below = below + factor * sums[v]
        results.append(above / below)
    block = jnp.concatenate(results, axis=0).astype(bf16)
    for k in range(N_KV):
        out[k] = block


def output_kernel(shared, w_0, w_1, w_2, w_4, out, rows):
    tp = lax.axis_index("tp")
    rows[...] = shared[...].astype(f32)
    near = (w_0[...], w_1[...], w_2[0], w_2[1], w_4[0], w_4[1], w_4[2], w_4[3])
    near = [w.astype(f32) for w in near]
    for bit in (1, 2, 4):
        swap = (tp & bit) != 0
        near = [jnp.where(swap, near[g ^ bit], near[g]) for g in range(N_TP)]
    low = iota((PROPS, WIDTH), 1) < HEAD
    total = jnp.zeros((48, 64), f32)
    for g in range(N_TP):
        pair_0 = rows[pl.ds(2 * g, PROPS, stride=16), :]
        pair_1 = rows[pl.ds(256 + 2 * g, PROPS, stride=16), :]
        last_0 = rows[pl.ds(2 * g + 1, PROPS, stride=16), :]
        last_1 = rows[pl.ds(257 + 2 * g, PROPS, stride=16), :]
        block = jnp.concatenate(
            [
                jnp.where(low, pair_0, pltpu.roll(pair_1, HEAD, 1)),
                jnp.where(low, pltpu.roll(pair_0, HEAD, 1), pair_1),
                jnp.where(low, last_0, pltpu.roll(last_1, HEAD, 1)),
            ],
            axis=0,
        )
        total = total + dot_t(block.astype(bf16), near[g].astype(bf16))
    out[...] = total.astype(bf16)


def join_kernel(first, second, out):
    count = first.shape[0]
    out[0:count] = first[...]
    out[count:] = second[...]


def write_kernel(
    prior,
    accepted,
    joined,
    after,
    keys_in,
    values_in,
    keys,
    values,
    buf,
    near,
    columns,
    in_sem,
    out_sem,
    near_sem,
):
    moves = []
    for t in range(8):
        three = pl.ds(3 * t, 3)
        moves.append(
            (
                pltpu.make_async_copy(values_in.at[three], near.at[three], near_sem.at[0, t]),
                pltpu.make_async_copy(near.at[three], values.at[three], near_sem.at[1, t]),
            )
        )
    offset = lax.axis_index(KV) * LEN

    def place(b):
        start = prior[b] + accepted[b] - offset
        base = jnp.clip(lax.div(jnp.maximum(start, 0), 16) * 16, 0, LEN - WINDOW)
        hit = (start > -PROPS) & (start < LEN)
        return start, pl.multiple_of(base, 16), hit

    def copy_in(b, base):
        return pltpu.make_async_copy(
            keys.at[b, pl.ds(base, WINDOW), :], buf.at[b], in_sem.at[b]
        )

    def copy_out(b, base):
        return pltpu.make_async_copy(
            buf.at[b], keys.at[b, pl.ds(base, WINDOW), :], out_sem.at[b]
        )

    @pl.loop(0, SEQS)
    def _(b):
        start, base, hit = place(b)

        @pl.when(hit)
        def _():
            copy_in(b, base).start()

    for move in moves:
        move[0].start()
    coded = joined[STATS].astype(f32)
    columns[...] = jnp.transpose(coded[0:8] + coded[8:16])

    def patched(b, start, base):
        inv = columns[pl.ds(pl.multiple_of(PROPS * b, PROPS), PROPS), 2:3]
        slot = iota((WINDOW, PROPS), 0) + (base - start)
        selector = jnp.where(slot == iota((WINDOW, PROPS), 1), 1.0, 0.0).astype(bf16)
        raw = joined[b, :, WIDTH:].astype(f32)
        rows = jnp.dot(selector, (inv * raw).astype(bf16), preferred_element_type=f32)
        slot = iota((WINDOW, WIDTH), 0) + (base - start)
        return (slot >= 0) & (slot < PROPS), rows

    for t in range(8):
        moves[t][0].wait()

        @pl.loop(3 * t, 3 * t + 3)
        def _(b):
            start, base, hit = place(b)

            @pl.when(hit)
            def _():
                inside, rows = patched(b, start, base)
                window = pl.ds(base, WINDOW)
                held = near[b, window, :].astype(f32)
                near[b, window, :] = jnp.where(inside, rows[:, WIDTH:], held).astype(bf16)
                copy_in(b, base).wait()
                held = buf[b].astype(f32)
                buf[b] = jnp.where(inside, rows[:, 0:WIDTH], held).astype(bf16)
                copy_out(b, base).start()

        moves[t][1].start()
    for move in moves:
        move[1].wait()

    @pl.loop(0, SEQS)
    def _(b):
        start, base, hit = place(b)

        @pl.when(hit)
        def _():
            copy_out(b, base).wait()


def shards(
    tokens,
    norm_gain,
    w_query,
    w_key,
    w_value,
    w_gate,
    gate_bias,
    w_out,
    keys_cache,
    values_cache,
    cum_gates,
    prior_len,
    accepted,
    parents,
):
    cache = jax.ShapeDtypeStruct(keys_cache.shape, bf16)

    def near(*arrays):
        return [pltpu.with_memory_space_constraint(a, pltpu.VMEM) for a in arrays]

    def far(*arrays):
        return [pltpu.with_memory_space_constraint(a, pltpu.HBM) for a in arrays]

    def limit(mib):
        return pltpu.CompilerParams(vmem_limit_bytes=mib << 20)

    parts, biases = pl.pallas_call(
        project_kernel,
        out_shape=(
            jax.ShapeDtypeStruct((N_KV, PROPS, ROWS), bf16),
            pltpu.VMEM(cum_gates.shape, f32),
        ),
        in_specs=[SM, SM, VM, VM, VM, VM, VM, VM, VM],
        out_specs=(VM, VM),
        scratch_shapes=[pltpu.VMEM((16, ROWS), f32)],
        name="project",
    )(
        prior_len,
        accepted,
        tokens.T,
        norm_gain[None],
        w_query,
        w_key,
        w_value,
        w_gate.T,
        cum_gates,
    )
    arrived = lax.all_to_all(parts, KV, 0, 0, tiled=True)

    tp_count = lax.axis_size("tp")

    def gathered(name, *pieces):
        return pl.pallas_call(
            join_kernel,
            out_shape=pltpu.VMEM((sum(len(p) for p in pieces), *pieces[0].shape[1:]), bf16),
            in_specs=[VM, VM],
            out_specs=VM,
            compiler_params=limit(2),
            name=name,
        )(*pieces)

    def across(x, bit):
        return lax.ppermute(x, "tp", [(i, i ^ bit) for i in range(tp_count)])

    w_0 = w_out.T
    w_1 = across(w_0, 1)
    w_pair = gathered("pair", *far(w_0[None]), *near(w_1[None]))
    w_2 = across(w_pair, 2)
    w_4 = across(gathered("four", *near(w_pair, w_2)), 4)

    block = pl.pallas_call(
        share_kernel,
        out_shape=pltpu.VMEM((N_KV, PROPS, ROWS), bf16),
        in_specs=[SM, VM, ANY],
        out_specs=VM,
        compiler_params=limit(8),
        cost_estimate=pl.CostEstimate(
            flops=10_000_000_000, bytes_accessed=800_000, transcendentals=0
        ),
        name="share",
    )(*far(gate_bias), *near(arrived), *far(w_4))
    joined = lax.all_to_all(block, KV, 0, 0, tiled=True)

    sent, keys_copy = pl.pallas_call(
        attention_kernel,
        out_shape=(pltpu.VMEM((512, WIDTH), bf16), cache),
        in_specs=[SM, VM, VM, VM, VM],
        out_specs=(VM, ANY),
        scratch_shapes=[
            pltpu.VMEM((ROWS, 8), f32),
            pltpu.VMEM((SEQS, 2 * PROPS, LEN), f32),
            pltpu.VMEM((SEQS, 2 * PROPS, LEN), bf16),
            pltpu.VMEM((SEQS, 2 * PROPS, WIDTH), f32),
            pltpu.VMEM((SEQS, 2 * PROPS, WIDTH), f32),
            pltpu.VMEM((512, WIDTH), f32),
            pltpu.SemaphoreType.DMA((4,)),
        ],
        compiler_params=limit(12),
        name="attention",
    )(*far(parents.T), *near(joined, biases, keys_cache, values_cache))
    pieces = lax.all_to_all(sent.reshape(256, 2, WIDTH), (*KV, "tp"), 0, 0, tiled=True)

    combined = pl.pallas_call(
        combine_kernel,
        out_shape=jax.ShapeDtypeStruct((N_KV, PROPS, WIDTH), bf16),
        in_specs=[VM],
        out_specs=VM,
        scratch_shapes=[pltpu.VMEM((64, 8, WIDTH), f32), pltpu.VMEM((64, 8, WIDTH), f32)],
        compiler_params=limit(8),
        name="combine",
    )(*near(pieces.reshape(512, WIDTH)))
    shared = lax.all_to_all(combined, KV, 0, 0, tiled=True)

    keys_out, values_out = pl.pallas_call(
        write_kernel,
        out_shape=(cache, cache),
        in_specs=[SM, SM, VM, ANY, ANY, ANY],
        out_specs=(ANY, ANY),
        input_output_aliases={4: 0},
        scratch_shapes=[
            pltpu.VMEM((SEQS, WINDOW, WIDTH), bf16),
            pltpu.VMEM(keys_cache.shape, bf16),
            pltpu.VMEM((ROWS, 8), f32),
            pltpu.SemaphoreType.DMA((SEQS,)),
            pltpu.SemaphoreType.DMA((SEQS,)),
            pltpu.SemaphoreType.DMA((2, 8)),
        ],
        compiler_params=limit(8),
        cost_estimate=pl.CostEstimate(
            flops=2_000_000_000, bytes_accessed=100_000, transcendentals=0
        ),
        name="write",
    )(
        *far(prior_len, accepted),
        *near(joined),
        *far(combined, keys_copy, values_cache),
    )

    mixed_rows = pl.pallas_call(
        output_kernel,
        out_shape=jax.ShapeDtypeStruct((48, 64), bf16),
        in_specs=[VM] * 5,
        out_specs=VM,
        scratch_shapes=[pltpu.VMEM((512, WIDTH), f32)],
        compiler_params=limit(8),
        name="output",
    )(*near(shared.reshape(512, WIDTH), w_0, w_1, w_2, w_4))
    return (mixed_rows, keys_out, values_out)


def solution(mesh):
    torus = Mesh(mesh.devices.reshape(8, 4, mesh.shape["tp"]), ("kv_0", "kv_1", "tp"))
    in_specs = (
        P(None, KV),
        P(KV),
        P(KV, "tp"),
        P(KV, "tp"),
        P(KV, "tp"),
        P(),
        P(),
        P("tp", KV),
        P(None, KV, "tp"),
        P(None, KV, "tp"),
        P(None, "tp", KV),
        P(),
        P(),
        P(),
    )
    out_specs = (P("tp", KV), P(None, KV, "tp"), P(None, KV, "tp"))
    return jax.shard_map(
        shards, mesh=torus, in_specs=in_specs, out_specs=out_specs, check_vma=False
    )
```

```python
import jax
import jax.numpy as jnp
from jax import lax
from jax.experimental import pallas as pl
from jax.experimental.pallas import tpu as pltpu
from jax.sharding import Mesh
from jax.sharding import PartitionSpec as P

D = 2048
HEAD = 64
PROPS = 16
ROWS = 384
SEQS = 24
LEN = 512
WIDTH = 128
N_KV = 32
N_TP = 8
STATS = 24
WINDOW = 32
KV = ("kv_0", "kv_1")

masked_score = -1e30
lowest_max = -1e20
norm_eps = 1e-06

VM = pl.BlockSpec(memory_space=pltpu.VMEM)
SM = pl.BlockSpec(memory_space=pltpu.SMEM)
ANY = pl.BlockSpec(memory_space=pl.ANY)
bf16 = jnp.bfloat16
f32 = jnp.float32


def iota(shape, dim):
    return lax.broadcasted_iota(jnp.int32, shape, dim)


def high_low(x):
    high = x.astype(bf16).astype(f32)
    return high, (x - high).astype(bf16).astype(f32)


def dot_t(a, b):
    return lax.dot_general(a, b, (((1,), (1,)), ((), ())), preferred_element_type=f32)


def project_kernel(
    prior, accepted, tokens, gain, w_q, w_k, w_v, w_gate, cum, out, bias, gates
):
    kv, tp = lax.axis_index(KV), lax.axis_index("tp")
    columns = pl.ds(pl.multiple_of(lax.div(kv, 2) * WIDTH, WIDTH), WIDTH)
    floats = tokens[...].astype(f32)
    same = iota((64, 64), 0) == iota((64, 64), 1)
    gain_column = jnp.sum(jnp.where(same, gain[...], 0.0), axis=1, keepdims=True)
    scaled = floats * gain_column
    rows = jnp.transpose(scaled).astype(bf16)
    scaled = scaled.astype(bf16)
    for n, w in enumerate((w_q, w_k, w_v)):
        part = jnp.dot(rows, w[...], preferred_element_type=f32).astype(bf16)
        out[0:SEQS, :, n * WIDTH : (n + 1) * WIDTH] = part.reshape(SEQS, PROPS, WIDTH)
    sq_high, sq_low = high_low(floats * floats)
    ones = jnp.ones((8, 64), bf16)
    square_sum = jnp.dot(ones, sq_high.astype(bf16), preferred_element_type=f32) + jnp.dot(
        ones, sq_low.astype(bf16), preferred_element_type=f32
    )
    lane = iota((2, WIDTH), 1)
    position = iota((2, LEN), 1)
    last = jnp.zeros((2, WIDTH), f32)
    for b in range(SEQS):
        at = prior[b] + accepted[b] - 1 - kv * LEN
        here = cum[b]
        bias[b] = jnp.where(position <= at, -here, masked_score)
        found = jnp.sum(jnp.where(position == at, here, 0.0), axis=1, keepdims=True)
        last = jnp.where(lane == b, found, last)
    last_high, last_low = high_low(last)
    rest = last - last_high - last_low
    odd = lax.rem(kv, 2)
    zero = jnp.zeros_like(scaled)
    both = jnp.concatenate(
        [jnp.where(odd == 0, scaled, zero), jnp.where(odd == 1, scaled, zero)], axis=0
    )
    gates[...] = jnp.dot(w_gate[:, columns], both, preferred_element_type=f32)
    row = iota((8, ROWS), 0)
    gate_0 = gates[pl.ds(2 * tp, 1), :]
    gate_1 = gates[pl.ds(2 * tp + 1, 1), :]
    stats = jnp.where(row == 0, gate_0, jnp.where(row == 1, gate_1, 0.0))
    stats = jnp.where(row == 2, square_sum, stats)
    wide = jnp.zeros((2, ROWS - WIDTH), f32)
    last = jnp.concatenate([last, wide], axis=1)
    rest = jnp.concatenate([rest, wide], axis=1)
    stats = jnp.where(row == 3, last[0:1], jnp.where(row == 4, last[1:2], stats))
    stats = jnp.where(row == 5, rest[0:1], jnp.where(row == 6, rest[1:2], stats))
    out[STATS] = jnp.concatenate(high_low(stats), axis=0).astype(bf16)
    out[STATS + 1 :] = jnp.zeros((N_KV - STATS - 1, PROPS, ROWS), bf16)


def share_kernel(bias, parts, after_1, after_3, after_5, after_7, out):
    kv, tp = lax.axis_index(KV), lax.axis_index("tp")
    total = jnp.zeros((PROPS, ROWS), f32)
    for k in range(N_KV):
        total = total + parts[k].astype(f32)
    stats = total[0:8] + total[8:16]
    row = iota((8, ROWS), 0)
    inv_rms = lax.rsqrt(stats[2:3] / D + norm_eps)
    logits = inv_rms * stats + jnp.where(row == 0, bias[2 * tp], bias[2 * tp + 1])
    log_gates = jnp.minimum(logits, 0.0) - jnp.log1p(jnp.exp(-jnp.abs(logits)))
    stats = jnp.where(row < 2, log_gates, jnp.where(row == 2, inv_rms, stats))
    stats = jnp.concatenate(high_low(stats), axis=0)
    block = jnp.where(kv == STATS, stats, total).astype(bf16)
    for k in range(N_KV):
        out[k] = block


def attention_kernel(
    parents,
    joined,
    biases,
    keys,
    values,
    out,
    keys_out,
    columns,
    scores_buf,
    weights_buf,
    v_buf,
    stat_buf,
    mixed,
    sems,
):
    kv = lax.axis_index(KV)
    moves = []
    for t in range(4):
        six = pl.ds(6 * t, 6)
        moves.append(pltpu.make_async_copy(keys.at[six], keys_out.at[six], sems.at[t]))
    for move in moves:
        move.start()
    coded = joined[STATS].astype(f32)
    stats = coded[0:8] + coded[8:16]
    columns[...] = jnp.transpose(stats)
    lane = iota((PROPS, WIDTH), 1)
    first_head = lane < HEAD
    lane_out = iota((2 * PROPS, WIDTH), 1)
    first_row = iota((2 * PROPS, WIDTH), 0) < PROPS
    scale = HEAD**-0.5

    def both_heads(b_rows, b_block):
        inv = columns[b_rows, 2:3]
        q = (inv * joined[b_block, :, 0:WIDTH].astype(f32)).astype(bf16).astype(f32) * scale
        zero = jnp.zeros_like(q)
        return jnp.concatenate(
            [jnp.where(first_head, q, zero), jnp.where(first_head, zero, q)], axis=0
        ).astype(bf16)

    def coded_stats(s, top, total):
        place = lane_out - (HEAD + 4 * s)
        top_high, top_low = high_low(top)
        sum_high, sum_low = high_low(total)
        stats = jnp.where(place == 0, top_high, jnp.where(place == 1, top_low, 0.0))
        return jnp.where(place == 2, sum_high, jnp.where(place == 3, sum_low, stats))

    def sendable(top):
        high, low = high_low(jnp.maximum(top, lowest_max))
        return high + low

    own = jnp.minimum(kv, SEQS - 1)
    low = lane_out < HEAD

    def score(b):
        q = both_heads(pl.ds(PROPS * b, PROPS), b)
        bias = biases[b]
        bias = jnp.concatenate(
            [
                jnp.broadcast_to(bias[0:1], (PROPS, LEN)),
                jnp.broadcast_to(bias[1:2], (PROPS, LEN)),
            ],
            axis=0,
        )
        scores_buf[b] = dot_t(q, keys[b]) + bias

    def weigh(b):
        scores = scores_buf[b]
        top = sendable(jnp.max(scores, axis=1, keepdims=True))
        weights = jnp.exp(scores - top)
        total = jnp.sum(weights, axis=1, keepdims=True)
        weights_buf[b] = weights.astype(bf16)
        stat_buf[b] = coded_stats(b % 3, top, total)

    def gather(b):
        v_buf[b] = jnp.dot(weights_buf[b], values[b], preferred_element_type=f32)

    def pack(t):
        v = [v_buf[3 * t + s] for s in range(3)]
        turned = [pltpu.roll(x, HEAD, 1) for x in v]
        first = jnp.where(first_row, v[0], turned[0])
        second = jnp.where(first_row, turned[1], v[1])
        third = jnp.where(first_row, v[2], turned[2])
        stats = stat_buf[3 * t] + stat_buf[3 * t + 1] + stat_buf[3 * t + 2]
        mixed[pl.ds(2 * t, N_KV, stride=16), :] = jnp.where(low, first, second)
        mixed[pl.ds(2 * t + 1, N_KV, stride=16), :] = jnp.where(low, third, stats)

    def lineage():
        row = iota((PROPS, WIDTH), 0)
        linked = jnp.where(lane == row, 1.0, 0.0)
        for i in range(PROPS):
            linked = jnp.where((row == i) & (lane == parents[i, own]), 1.0, linked)
        return linked

    def squared(linked):
        other = jnp.concatenate([linked, jnp.zeros((WIDTH - PROPS, WIDTH), f32)], axis=0)
        product = jnp.dot(linked.astype(bf16), other.astype(bf16), preferred_element_type=f32)
        return jnp.minimum(product, 1.0)

    def tree(reached):
        mine = pl.ds(pl.multiple_of(PROPS * own, PROPS), PROPS)
        pad = jnp.zeros((WIDTH - PROPS, WIDTH), f32)
        picks = (iota((ROWS, WIDTH), 0) == iota((ROWS, WIDTH), 1) + PROPS * own) & (
            iota((ROWS, WIDTH), 1) < PROPS
        )
        own_gates = jnp.dot(
            joined[STATS], jnp.where(picks, 1.0, 0.0).astype(bf16), preferred_element_type=f32
        ).astype(bf16)
        tree = dot_t(own_gates, jnp.concatenate([reached, pad], axis=0).astype(bf16))
        tree = tree[0:8] + tree[8:16]
        last = jnp.sum(
            jnp.where(iota((8, WIDTH), 1) == own, stats[:, 0:WIDTH], 0.0), axis=1, keepdims=True
        )
        tree_bias = jnp.concatenate(
            [
                jnp.broadcast_to(-(last[3:4] + last[5:6] + tree[0:1]), (PROPS, WIDTH)),
                jnp.broadcast_to(-(last[4:5] + last[6:7] + tree[1:2]), (PROPS, WIDTH)),
            ],
            axis=0,
        )
        own_inv = columns[mine, 2:3]
        new_keys = own_inv * joined[own, :, WIDTH : 2 * WIDTH].astype(f32)
        new_values = own_inv * joined[own, :, 2 * WIDTH : 3 * WIDTH].astype(f32)
        new_keys = jnp.concatenate([new_keys, pad], axis=0).astype(bf16)
        new_values = jnp.concatenate([new_values, pad], axis=0).astype(bf16)
        needed = jnp.where(kv < SEQS, 0.5, 2.0)
        live = jnp.concatenate([reached, reached], axis=0) > needed
        tree_scores = jnp.where(live, dot_t(both_heads(mine, own), new_keys) + tree_bias, masked_score)
        tree_top = jnp.max(tree_scores, axis=1, keepdims=True)
        return tree_scores, tree_top, new_values

    for step in range(N_TP + 2):
        for s in range(3):
            if step < N_TP:
                score(3 * step + s)
            if 1 <= step <= N_TP:
                weigh(3 * step - 3 + s)
            if step >= 2:
                gather(3 * step - 6 + s)
        if step == 0:
            reached = lineage()
        if 1 <= step <= 4:
            reached = squared(reached)
        if step == 5:
            tree_scores, tree_top, new_values = tree(reached)
        if step == N_TP:
            scores = scores_buf[own]
            top = jnp.maximum(jnp.max(scores, axis=1, keepdims=True), tree_top)
            top = sendable(top)
            own_weights = jnp.exp(scores - top)
            tree_weights = jnp.exp(tree_scores - top)
            own_total = jnp.sum(own_weights, axis=1, keepdims=True) + jnp.sum(
                tree_weights, axis=1, keepdims=True
            )
            own_stats = coded_stats(lax.rem(own, 3), top, own_total)
    own_v = jnp.dot(
        own_weights.astype(bf16), values[own], preferred_element_type=f32
    ) + jnp.dot(tree_weights.astype(bf16), new_values, preferred_element_type=f32)
    stat_buf[own] = own_stats
    v_buf[own] = own_v
    for t in range(N_TP):
        pack(t)
    out[...] = mixed[...].astype(bf16)
    for move in moves:
        move.wait()


def combine_kernel(parts, out, tops, sums):
    row = iota((WIDTH, 4 * WIDTH), 0) - HEAD
    column = iota((WIDTH, 4 * WIDTH), 1)
    unit = jnp.where(column < 2 * WIDTH, lax.rem(lax.div(column, HEAD), 2), 2)
    kind = lax.rem(lax.div(column, WIDTH), 2)
    row = row - 4 * unit - 2 * kind
    spread = jnp.where((row == 0) | (row == 1), 1.0, 0.0).astype(bf16)
    even = lax.rem(iota((8, WIDTH), 0), 2) == 0
    for n in range(4):
        stats = jnp.dot(parts[128 * n : 128 * n + 128], spread, preferred_element_type=f32)
        for v in range(16):
            rows = stats[8 * v : 8 * v + 8]
            near = pltpu.roll(rows[:, 0 : 2 * WIDTH], 7, 0)
            tops[16 * n + v] = jnp.where(even, near[:, 0:WIDTH], rows[:, 2 * WIDTH : 3 * WIDTH])
            sums[16 * n + v] = jnp.where(even, near[:, WIDTH:], rows[:, 3 * WIDTH :])
    results = []
    for half in range(2):
        top = tops[half]
        for k in range(1, N_KV):
            top = jnp.maximum(top, tops[2 * k + half])
        above = jnp.zeros((8, WIDTH), f32)
        below = jnp.zeros((8, WIDTH), f32)
        for k in range(N_KV):
            v = 2 * k + half
            factor = jnp.exp(tops[v] - top)
            above = above + factor * parts[8 * v : 8 * v + 8, :].astype(f32)
            below = below + factor * sums[v]
        results.append(above / below)
    block = jnp.concatenate(results, axis=0).astype(bf16)
    for k in range(N_KV):
        out[k] = block


def output_kernel(shared, w_all, out, rows):
    rows[...] = shared[...].astype(f32)
    low = iota((PROPS, WIDTH), 1) < HEAD
    total = jnp.zeros((48, 64), f32)
    for g in range(N_TP):
        pair_0 = rows[pl.ds(2 * g, PROPS, stride=16), :]
        pair_1 = rows[pl.ds(256 + 2 * g, PROPS, stride=16), :]
        last_0 = rows[pl.ds(2 * g + 1, PROPS, stride=16), :]
        last_1 = rows[pl.ds(257 + 2 * g, PROPS, stride=16), :]
        block = jnp.concatenate(
            [
                jnp.where(low, pair_0, pltpu.roll(pair_1, HEAD, 1)),
                jnp.where(low, pltpu.roll(pair_0, HEAD, 1), pair_1),
                jnp.where(low, last_0, pltpu.roll(last_1, HEAD, 1)),
            ],
            axis=0,
        )
        total = total + dot_t(block.astype(bf16), w_all[g])
    out[...] = total.astype(bf16)


def write_kernel(
    prior,
    accepted,
    joined,
    w_0,
    w_1,
    w_2,
    w_3,
    w_4,
    w_5,
    w_6,
    w_7,
    after,
    keys_in,
    values_in,
    keys,
    values,
    w_all,
    buf,
    near,
    columns,
    in_sem,
    out_sem,
    near_sem,
):
    moves = []
    for t in range(8):
        three = pl.ds(3 * t, 3)
        moves.append(
            (
                pltpu.make_async_copy(values_in.at[three], near.at[three], near_sem.at[0, t]),
                pltpu.make_async_copy(near.at[three], values.at[three], near_sem.at[1, t]),
            )
        )
    offset = lax.axis_index(KV) * LEN

    def place(b):
        start = prior[b] + accepted[b] - offset
        base = jnp.clip(lax.div(jnp.maximum(start, 0), 16) * 16, 0, LEN - WINDOW)
        hit = (start > -PROPS) & (start < LEN)
        return start, pl.multiple_of(base, 16), hit

    def copy_in(b, base):
        return pltpu.make_async_copy(
            keys.at[b, pl.ds(base, WINDOW), :], buf.at[b], in_sem.at[b]
        )

    def copy_out(b, base):
        return pltpu.make_async_copy(
            buf.at[b], keys.at[b, pl.ds(base, WINDOW), :], out_sem.at[b]
        )

    @pl.loop(0, SEQS)
    def _(b):
        start, base, hit = place(b)

        @pl.when(hit)
        def _():
            copy_in(b, base).start()

    for move in moves:
        move[0].start()
    tp = lax.axis_index("tp")
    for distance, w in enumerate((w_0, w_1, w_2, w_3, w_4, w_5, w_6, w_7)):
        w_all[tp ^ distance] = w[...]
    coded = joined[STATS].astype(f32)
    columns[...] = jnp.transpose(coded[0:8] + coded[8:16])

    def patched(b, start, base):
        inv = columns[pl.ds(pl.multiple_of(PROPS * b, PROPS), PROPS), 2:3]
        slot = iota((WINDOW, PROPS), 0) + (base - start)
        selector = jnp.where(slot == iota((WINDOW, PROPS), 1), 1.0, 0.0).astype(bf16)
        raw = joined[b, :, WIDTH:].astype(f32)
        rows = jnp.dot(selector, (inv * raw).astype(bf16), preferred_element_type=f32)
        slot = iota((WINDOW, WIDTH), 0) + (base - start)
        return (slot >= 0) & (slot < PROPS), rows

    for t in range(8):
        moves[t][0].wait()

        @pl.loop(3 * t, 3 * t + 3)
        def _(b):
            start, base, hit = place(b)

            @pl.when(hit)
            def _():
                inside, rows = patched(b, start, base)
                window = pl.ds(base, WINDOW)
                held = near[b, window, :].astype(f32)
                near[b, window, :] = jnp.where(inside, rows[:, WIDTH:], held).astype(bf16)
                copy_in(b, base).wait()
                held = buf[b].astype(f32)
                buf[b] = jnp.where(inside, rows[:, 0:WIDTH], held).astype(bf16)
                copy_out(b, base).start()

        moves[t][1].start()
    for move in moves:
        move[1].wait()

    @pl.loop(0, SEQS)
    def _(b):
        start, base, hit = place(b)

        @pl.when(hit)
        def _():
            copy_out(b, base).wait()


def shards(
    tokens,
    norm_gain,
    w_query,
    w_key,
    w_value,
    w_gate,
    gate_bias,
    w_out,
    keys_cache,
    values_cache,
    cum_gates,
    prior_len,
    accepted,
    parents,
):
    cache = jax.ShapeDtypeStruct(keys_cache.shape, bf16)

    def near(*arrays):
        return [pltpu.with_memory_space_constraint(a, pltpu.VMEM) for a in arrays]

    def far(*arrays):
        return [pltpu.with_memory_space_constraint(a, pltpu.HBM) for a in arrays]

    def limit(mib):
        return pltpu.CompilerParams(vmem_limit_bytes=mib << 20)

    parts, biases = pl.pallas_call(
        project_kernel,
        out_shape=(
            jax.ShapeDtypeStruct((N_KV, PROPS, ROWS), bf16),
            pltpu.VMEM(cum_gates.shape, f32),
        ),
        in_specs=[SM, SM, VM, VM, VM, VM, VM, VM, VM],
        out_specs=(VM, VM),
        scratch_shapes=[pltpu.VMEM((16, ROWS), f32)],
        name="project",
    )(
        prior_len,
        accepted,
        tokens.T,
        norm_gain[None],
        w_query,
        w_key,
        w_value,
        w_gate.T,
        cum_gates,
    )
    arrived = lax.all_to_all(parts, KV, 0, 0, tiled=True)

    tp_count = lax.axis_size("tp")

    def across(x, bit):
        return lax.ppermute(x, "tp", [(i, i ^ bit) for i in range(tp_count)])

    all_w = [w_out.T]
    for bit in (4, 2, 1):
        all_w = all_w + [across(w, bit) for w in all_w]
    order = {distance: n for n, distance in enumerate((0, 4, 2, 6, 1, 5, 3, 7))}
    all_w = [all_w[order[distance]] for distance in range(tp_count)]
    block = pl.pallas_call(
        share_kernel,
        out_shape=pltpu.VMEM((N_KV, PROPS, ROWS), bf16),
        in_specs=[SM, VM] + [ANY] * 4,
        out_specs=VM,
        compiler_params=limit(8),
        cost_estimate=pl.CostEstimate(
            flops=10_000_000_000, bytes_accessed=800_000, transcendentals=0
        ),
        name="share",
    )(*far(gate_bias), *near(arrived), *far(*all_w[1::2]))
    joined = lax.all_to_all(block, KV, 0, 0, tiled=True)

    sent, keys_copy = pl.pallas_call(
        attention_kernel,
        out_shape=(pltpu.VMEM((512, WIDTH), bf16), cache),
        in_specs=[SM, VM, VM, VM, VM],
        out_specs=(VM, ANY),
        scratch_shapes=[
            pltpu.VMEM((ROWS, 8), f32),
            pltpu.VMEM((SEQS, 2 * PROPS, LEN), f32),
            pltpu.VMEM((SEQS, 2 * PROPS, LEN), bf16),
            pltpu.VMEM((SEQS, 2 * PROPS, WIDTH), f32),
            pltpu.VMEM((SEQS, 2 * PROPS, WIDTH), f32),
            pltpu.VMEM((512, WIDTH), f32),
            pltpu.SemaphoreType.DMA((4,)),
        ],
        compiler_params=limit(12),
        name="attention",
    )(*far(parents.T), *near(joined, biases, keys_cache, values_cache))
    pieces = lax.all_to_all(sent.reshape(256, 2, WIDTH), (*KV, "tp"), 0, 0, tiled=True)

    combined = pl.pallas_call(
        combine_kernel,
        out_shape=jax.ShapeDtypeStruct((N_KV, PROPS, WIDTH), bf16),
        in_specs=[VM],
        out_specs=VM,
        scratch_shapes=[pltpu.VMEM((64, 8, WIDTH), f32), pltpu.VMEM((64, 8, WIDTH), f32)],
        compiler_params=limit(8),
        name="combine",
    )(*near(pieces.reshape(512, WIDTH)))
    shared = lax.all_to_all(combined, KV, 0, 0, tiled=True)

    keys_out, values_out, w_all = pl.pallas_call(
        write_kernel,
        out_shape=(cache, cache, pltpu.VMEM((N_TP, 64, WIDTH), bf16)),
        in_specs=[SM, SM] + [VM] * 9 + [ANY] * 3,
        out_specs=(ANY, ANY, VM),
        input_output_aliases={12: 0},
        scratch_shapes=[
            pltpu.VMEM((SEQS, WINDOW, WIDTH), bf16),
            pltpu.VMEM(keys_cache.shape, bf16),
            pltpu.VMEM((ROWS, 8), f32),
            pltpu.SemaphoreType.DMA((SEQS,)),
            pltpu.SemaphoreType.DMA((SEQS,)),
            pltpu.SemaphoreType.DMA((2, 8)),
        ],
        compiler_params=limit(8),
        cost_estimate=pl.CostEstimate(
            flops=2_000_000_000, bytes_accessed=100_000, transcendentals=0
        ),
        name="write",
    )(
        *far(prior_len, accepted),
        *near(joined),
        *far(*all_w),
        *far(combined, keys_copy, values_cache),
    )

    mixed_rows = pl.pallas_call(
        output_kernel,
        out_shape=jax.ShapeDtypeStruct((48, 64), bf16),
        in_specs=[VM, VM],
        out_specs=VM,
        scratch_shapes=[pltpu.VMEM((512, WIDTH), f32)],
        compiler_params=limit(8),
        name="output",
    )(*near(shared.reshape(512, WIDTH), w_all))
    return (mixed_rows, keys_out, values_out)


def solution(mesh):
    torus = Mesh(mesh.devices.reshape(8, 4, mesh.shape["tp"]), ("kv_0", "kv_1", "tp"))
    in_specs = (
        P(None, KV),
        P(KV),
        P(KV, "tp"),
        P(KV, "tp"),
        P(KV, "tp"),
        P(),
        P(),
        P("tp", KV),
        P(None, KV, "tp"),
        P(None, KV, "tp"),
        P(None, "tp", KV),
        P(),
        P(),
        P(),
    )
    out_specs = (P("tp", KV), P(None, KV, "tp"), P(None, KV, "tp"))
    return jax.shard_map(
        shards, mesh=torus, in_specs=in_specs, out_specs=out_specs, check_vma=False
    )
```

```python
import jax
import jax.numpy as jnp
from jax import lax
from jax.experimental import pallas as pl
from jax.experimental.pallas import tpu as pltpu
from jax.sharding import Mesh
from jax.sharding import PartitionSpec as P

D = 2048
HEAD = 64
PROPS = 16
ROWS = 384
SEQS = 24
LEN = 512
WIDTH = 128
N_KV = 32
N_TP = 8
STATS = 24
WINDOW = 32
KV = ("kv_0", "kv_1")

masked_score = -1e30
lowest_max = -1e20
norm_eps = 1e-06

VM = pl.BlockSpec(memory_space=pltpu.VMEM)
SM = pl.BlockSpec(memory_space=pltpu.SMEM)
ANY = pl.BlockSpec(memory_space=pl.ANY)
bf16 = jnp.bfloat16
f32 = jnp.float32


def iota(shape, dim):
    return lax.broadcasted_iota(jnp.int32, shape, dim)


def high_low(x):
    high = x.astype(bf16).astype(f32)
    return high, (x - high).astype(bf16).astype(f32)


def dot_t(a, b):
    return lax.dot_general(a, b, (((1,), (1,)), ((), ())), preferred_element_type=f32)


def project_kernel(
    prior, accepted, tokens, gain, w_q, w_k, w_v, w_gate, cum, out, bias, gates
):
    kv, tp = lax.axis_index(KV), lax.axis_index("tp")
    columns = pl.ds(pl.multiple_of(lax.div(kv, 2) * WIDTH, WIDTH), WIDTH)
    floats = tokens[...].astype(f32)
    same = iota((64, 64), 0) == iota((64, 64), 1)
    gain_column = jnp.sum(jnp.where(same, gain[...], 0.0), axis=1, keepdims=True)
    scaled = floats * gain_column
    rows = jnp.transpose(scaled).astype(bf16)
    scaled = scaled.astype(bf16)
    for n, w in enumerate((w_q, w_k, w_v)):
        part = jnp.dot(rows, w[...], preferred_element_type=f32).astype(bf16)
        out[0:SEQS, :, n * WIDTH : (n + 1) * WIDTH] = part.reshape(SEQS, PROPS, WIDTH)
    sq_high, sq_low = high_low(floats * floats)
    ones = jnp.ones((8, 64), bf16)
    square_sum = jnp.dot(ones, sq_high.astype(bf16), preferred_element_type=f32) + jnp.dot(
        ones, sq_low.astype(bf16), preferred_element_type=f32
    )
    lane = iota((2, WIDTH), 1)
    position = iota((2, LEN), 1)
    last = jnp.zeros((2, WIDTH), f32)
    for b in range(SEQS):
        at = prior[b] + accepted[b] - 1 - kv * LEN
        here = cum[b]
        bias[b] = jnp.where(position <= at, -here, masked_score)
        found = jnp.sum(jnp.where(position == at, here, 0.0), axis=1, keepdims=True)
        last = jnp.where(lane == b, found, last)
    last_high, last_low = high_low(last)
    rest = last - last_high - last_low
    odd = lax.rem(kv, 2)
    zero = jnp.zeros_like(scaled)
    both = jnp.concatenate(
        [jnp.where(odd == 0, scaled, zero), jnp.where(odd == 1, scaled, zero)], axis=0
    )
    gates[...] = jnp.dot(w_gate[:, columns], both, preferred_element_type=f32)
    row = iota((8, ROWS), 0)
    gate_0 = gates[pl.ds(2 * tp, 1), :]
    gate_1 = gates[pl.ds(2 * tp + 1, 1), :]
    stats = jnp.where(row == 0, gate_0, jnp.where(row == 1, gate_1, 0.0))
    stats = jnp.where(row == 2, square_sum, stats)
    wide = jnp.zeros((2, ROWS - WIDTH), f32)
    last = jnp.concatenate([last, wide], axis=1)
    rest = jnp.concatenate([rest, wide], axis=1)
    stats = jnp.where(row == 3, last[0:1], jnp.where(row == 4, last[1:2], stats))
    stats = jnp.where(row == 5, rest[0:1], jnp.where(row == 6, rest[1:2], stats))
    out[STATS] = jnp.concatenate(high_low(stats), axis=0).astype(bf16)
    out[STATS + 1 :] = jnp.zeros((N_KV - STATS - 1, PROPS, ROWS), bf16)


def share_kernel(bias, parts, after_w, out):
    kv, tp = lax.axis_index(KV), lax.axis_index("tp")
    total = jnp.zeros((PROPS, ROWS), f32)
    for k in range(N_KV):
        total = total + parts[k].astype(f32)
    stats = total[0:8] + total[8:16]
    row = iota((8, ROWS), 0)
    inv_rms = lax.rsqrt(stats[2:3] / D + norm_eps)
    logits = inv_rms * stats + jnp.where(row == 0, bias[2 * tp], bias[2 * tp + 1])
    log_gates = jnp.minimum(logits, 0.0) - jnp.log1p(jnp.exp(-jnp.abs(logits)))
    stats = jnp.where(row < 2, log_gates, jnp.where(row == 2, inv_rms, stats))
    stats = jnp.concatenate(high_low(stats), axis=0)
    block = jnp.where(kv == STATS, stats, total).astype(bf16)
    for k in range(N_KV):
        out[k] = block


def attention_kernel(
    parents,
    joined,
    biases,
    keys,
    values,
    out,
    keys_out,
    columns,
    scores_buf,
    weights_buf,
    v_buf,
    stat_buf,
    mixed,
    sems,
):
    kv = lax.axis_index(KV)
    moves = []
    for t in range(4):
        six = pl.ds(6 * t, 6)
        moves.append(pltpu.make_async_copy(keys.at[six], keys_out.at[six], sems.at[t]))
    for move in moves:
        move.start()
    coded = joined[STATS].astype(f32)
    stats = coded[0:8] + coded[8:16]
    columns[...] = jnp.transpose(stats)
    lane = iota((PROPS, WIDTH), 1)
    first_head = lane < HEAD
    lane_out = iota((2 * PROPS, WIDTH), 1)
    first_row = iota((2 * PROPS, WIDTH), 0) < PROPS
    scale = HEAD**-0.5

    def both_heads(b_rows, b_block):
        inv = columns[b_rows, 2:3]
        q = (inv * joined[b_block, :, 0:WIDTH].astype(f32)).astype(bf16).astype(f32) * scale
        zero = jnp.zeros_like(q)
        return jnp.concatenate(
            [jnp.where(first_head, q, zero), jnp.where(first_head, zero, q)], axis=0
        ).astype(bf16)

    def coded_stats(s, top, total):
        place = lane_out - (HEAD + 4 * s)
        top_high, top_low = high_low(top)
        sum_high, sum_low = high_low(total)
        stats = jnp.where(place == 0, top_high, jnp.where(place == 1, top_low, 0.0))
        return jnp.where(place == 2, sum_high, jnp.where(place == 3, sum_low, stats))

    def sendable(top):
        high, low = high_low(jnp.maximum(top, lowest_max))
        return high + low

    own = jnp.minimum(kv, SEQS - 1)
    low = lane_out < HEAD

    def score(b):
        q = both_heads(pl.ds(PROPS * b, PROPS), b)
        bias = biases[b]
        bias = jnp.concatenate(
            [
                jnp.broadcast_to(bias[0:1], (PROPS, LEN)),
                jnp.broadcast_to(bias[1:2], (PROPS, LEN)),
            ],
            axis=0,
        )
        scores_buf[b] = dot_t(q, keys[b]) + bias

    def weigh(b):
        scores = scores_buf[b]
        top = sendable(jnp.max(scores, axis=1, keepdims=True))
        weights = jnp.exp(scores - top)
        total = jnp.sum(weights, axis=1, keepdims=True)
        weights_buf[b] = weights.astype(bf16)
        stat_buf[b] = coded_stats(b % 3, top, total)

    def gather(b):
        v_buf[b] = jnp.dot(weights_buf[b], values[b], preferred_element_type=f32)

    def pack(t):
        v = [v_buf[3 * t + s] for s in range(3)]
        turned = [pltpu.roll(x, HEAD, 1) for x in v]
        first = jnp.where(first_row, v[0], turned[0])
        second = jnp.where(first_row, turned[1], v[1])
        third = jnp.where(first_row, v[2], turned[2])
        stats = stat_buf[3 * t] + stat_buf[3 * t + 1] + stat_buf[3 * t + 2]
        mixed[pl.ds(2 * t, N_KV, stride=16), :] = jnp.where(low, first, second)
        mixed[pl.ds(2 * t + 1, N_KV, stride=16), :] = jnp.where(low, third, stats)

    def lineage():
        row = iota((PROPS, WIDTH), 0)
        linked = jnp.where(lane == row, 1.0, 0.0)
        for i in range(PROPS):
            linked = jnp.where((row == i) & (lane == parents[i, own]), 1.0, linked)
        return linked

    def squared(linked):
        other = jnp.concatenate([linked, jnp.zeros((WIDTH - PROPS, WIDTH), f32)], axis=0)
        product = jnp.dot(linked.astype(bf16), other.astype(bf16), preferred_element_type=f32)
        return jnp.minimum(product, 1.0)

    def tree(reached):
        mine = pl.ds(pl.multiple_of(PROPS * own, PROPS), PROPS)
        pad = jnp.zeros((WIDTH - PROPS, WIDTH), f32)
        picks = (iota((ROWS, WIDTH), 0) == iota((ROWS, WIDTH), 1) + PROPS * own) & (
            iota((ROWS, WIDTH), 1) < PROPS
        )
        own_gates = jnp.dot(
            joined[STATS], jnp.where(picks, 1.0, 0.0).astype(bf16), preferred_element_type=f32
        ).astype(bf16)
        tree = dot_t(own_gates, jnp.concatenate([reached, pad], axis=0).astype(bf16))
        tree = tree[0:8] + tree[8:16]
        last = jnp.sum(
            jnp.where(iota((8, WIDTH), 1) == own, stats[:, 0:WIDTH], 0.0), axis=1, keepdims=True
        )
        tree_bias = jnp.concatenate(
            [
                jnp.broadcast_to(-(last[3:4] + last[5:6] + tree[0:1]), (PROPS, WIDTH)),
                jnp.broadcast_to(-(last[4:5] + last[6:7] + tree[1:2]), (PROPS, WIDTH)),
            ],
            axis=0,
        )
        own_inv = columns[mine, 2:3]
        new_keys = own_inv * joined[own, :, WIDTH : 2 * WIDTH].astype(f32)
        new_values = own_inv * joined[own, :, 2 * WIDTH : 3 * WIDTH].astype(f32)
        new_keys = jnp.concatenate([new_keys, pad], axis=0).astype(bf16)
        new_values = jnp.concatenate([new_values, pad], axis=0).astype(bf16)
        needed = jnp.where(kv < SEQS, 0.5, 2.0)
        live = jnp.concatenate([reached, reached], axis=0) > needed
        tree_scores = jnp.where(live, dot_t(both_heads(mine, own), new_keys) + tree_bias, masked_score)
        tree_top = jnp.max(tree_scores, axis=1, keepdims=True)
        return tree_scores, tree_top, new_values

    for step in range(N_TP + 2):
        for s in range(3):
            if step < N_TP:
                score(3 * step + s)
            if 1 <= step <= N_TP:
                weigh(3 * step - 3 + s)
            if step >= 2:
                gather(3 * step - 6 + s)
        if step == 0:
            reached = lineage()
        if 1 <= step <= 4:
            reached = squared(reached)
        if step == 5:
            tree_scores, tree_top, new_values = tree(reached)
        if step == N_TP:
            scores = scores_buf[own]
            top = jnp.maximum(jnp.max(scores, axis=1, keepdims=True), tree_top)
            top = sendable(top)
            own_weights = jnp.exp(scores - top)
            tree_weights = jnp.exp(tree_scores - top)
            own_total = jnp.sum(own_weights, axis=1, keepdims=True) + jnp.sum(
                tree_weights, axis=1, keepdims=True
            )
            own_stats = coded_stats(lax.rem(own, 3), top, own_total)
    own_v = jnp.dot(
        own_weights.astype(bf16), values[own], preferred_element_type=f32
    ) + jnp.dot(tree_weights.astype(bf16), new_values, preferred_element_type=f32)
    stat_buf[own] = own_stats
    v_buf[own] = own_v
    for t in range(N_TP):
        pack(t)
    out[...] = mixed[...].astype(bf16)
    for move in moves:
        move.wait()


def combine_kernel(parts, out, tops, sums):
    row = iota((WIDTH, 4 * WIDTH), 0) - HEAD
    column = iota((WIDTH, 4 * WIDTH), 1)
    unit = jnp.where(column < 2 * WIDTH, lax.rem(lax.div(column, HEAD), 2), 2)
    kind = lax.rem(lax.div(column, WIDTH), 2)
    row = row - 4 * unit - 2 * kind
    spread = jnp.where((row == 0) | (row == 1), 1.0, 0.0).astype(bf16)
    even = lax.rem(iota((8, WIDTH), 0), 2) == 0
    for n in range(4):
        stats = jnp.dot(parts[128 * n : 128 * n + 128], spread, preferred_element_type=f32)
        for v in range(16):
            rows = stats[8 * v : 8 * v + 8]
            near = pltpu.roll(rows[:, 0 : 2 * WIDTH], 7, 0)
            tops[16 * n + v] = jnp.where(even, near[:, 0:WIDTH], rows[:, 2 * WIDTH : 3 * WIDTH])
            sums[16 * n + v] = jnp.where(even, near[:, WIDTH:], rows[:, 3 * WIDTH :])
    results = []
    for half in range(2):
        top = tops[half]
        for k in range(1, N_KV):
            top = jnp.maximum(top, tops[2 * k + half])
        above = jnp.zeros((8, WIDTH), f32)
        below = jnp.zeros((8, WIDTH), f32)
        for k in range(N_KV):
            v = 2 * k + half
            factor = jnp.exp(tops[v] - top)
            above = above + factor * parts[8 * v : 8 * v + 8, :].astype(f32)
            below = below + factor * sums[v]
        results.append(above / below)
    block = jnp.concatenate(results, axis=0).astype(bf16)
    for k in range(N_KV):
        out[k] = block


def output_kernel(shared, w_even, w_odd, out, rows):
    tp = lax.axis_index("tp")
    rows[...] = shared[...].astype(f32)
    near = (w_even[0], w_odd[0], w_even[2], w_odd[2], w_even[1], w_odd[1], w_even[3], w_odd[3])
    near = [w.astype(f32) for w in near]
    for bit in (1, 2, 4):
        swap = (tp & bit) != 0
        near = [jnp.where(swap, near[g ^ bit], near[g]) for g in range(N_TP)]
    low = iota((PROPS, WIDTH), 1) < HEAD
    total = jnp.zeros((48, 64), f32)
    for g in range(N_TP):
        pair_0 = rows[pl.ds(2 * g, PROPS, stride=16), :]
        pair_1 = rows[pl.ds(256 + 2 * g, PROPS, stride=16), :]
        last_0 = rows[pl.ds(2 * g + 1, PROPS, stride=16), :]
        last_1 = rows[pl.ds(257 + 2 * g, PROPS, stride=16), :]
        block = jnp.concatenate(
            [
                jnp.where(low, pair_0, pltpu.roll(pair_1, HEAD, 1)),
                jnp.where(low, pltpu.roll(pair_0, HEAD, 1), pair_1),
                jnp.where(low, last_0, pltpu.roll(last_1, HEAD, 1)),
            ],
            axis=0,
        )
        total = total + dot_t(block.astype(bf16), near[g].astype(bf16))
    out[...] = total.astype(bf16)


def join_kernel(first, second, after, out):
    count = first.shape[0]
    out[0:count] = first[...]
    out[count:] = second[...]


def write_kernel(
    prior,
    accepted,
    joined,
    after,
    keys_in,
    values_in,
    keys,
    values,
    buf,
    near,
    columns,
    in_sem,
    out_sem,
    near_sem,
):
    moves = []
    for t in range(8):
        three = pl.ds(3 * t, 3)
        moves.append(
            (
                pltpu.make_async_copy(values_in.at[three], near.at[three], near_sem.at[0, t]),
                pltpu.make_async_copy(near.at[three], values.at[three], near_sem.at[1, t]),
            )
        )
    offset = lax.axis_index(KV) * LEN

    def place(b):
        start = prior[b] + accepted[b] - offset
        base = jnp.clip(lax.div(jnp.maximum(start, 0), 16) * 16, 0, LEN - WINDOW)
        hit = (start > -PROPS) & (start < LEN)
        return start, pl.multiple_of(base, 16), hit

    def copy_in(b, base):
        return pltpu.make_async_copy(
            keys.at[b, pl.ds(base, WINDOW), :], buf.at[b], in_sem.at[b]
        )

    def copy_out(b, base):
        return pltpu.make_async_copy(
            buf.at[b], keys.at[b, pl.ds(base, WINDOW), :], out_sem.at[b]
        )

    @pl.loop(0, SEQS)
    def _(b):
        start, base, hit = place(b)

        @pl.when(hit)
        def _():
            copy_in(b, base).start()

    for move in moves:
        move[0].start()
    coded = joined[STATS].astype(f32)
    columns[...] = jnp.transpose(coded[0:8] + coded[8:16])

    def patched(b, start, base):
        inv = columns[pl.ds(pl.multiple_of(PROPS * b, PROPS), PROPS), 2:3]
        slot = iota((WINDOW, PROPS), 0) + (base - start)
        selector = jnp.where(slot == iota((WINDOW, PROPS), 1), 1.0, 0.0).astype(bf16)
        raw = joined[b, :, WIDTH:].astype(f32)
        rows = jnp.dot(selector, (inv * raw).astype(bf16), preferred_element_type=f32)
        slot = iota((WINDOW, WIDTH), 0) + (base - start)
        return (slot >= 0) & (slot < PROPS), rows

    for t in range(8):
        moves[t][0].wait()

        @pl.loop(3 * t, 3 * t + 3)
        def _(b):
            start, base, hit = place(b)

            @pl.when(hit)
            def _():
                inside, rows = patched(b, start, base)
                window = pl.ds(base, WINDOW)
                held = near[b, window, :].astype(f32)
                near[b, window, :] = jnp.where(inside, rows[:, WIDTH:], held).astype(bf16)
                copy_in(b, base).wait()
                held = buf[b].astype(f32)
                buf[b] = jnp.where(inside, rows[:, 0:WIDTH], held).astype(bf16)
                copy_out(b, base).start()

        moves[t][1].start()
    for move in moves:
        move[1].wait()

    @pl.loop(0, SEQS)
    def _(b):
        start, base, hit = place(b)

        @pl.when(hit)
        def _():
            copy_out(b, base).wait()


def shards(
    tokens,
    norm_gain,
    w_query,
    w_key,
    w_value,
    w_gate,
    gate_bias,
    w_out,
    keys_cache,
    values_cache,
    cum_gates,
    prior_len,
    accepted,
    parents,
):
    cache = jax.ShapeDtypeStruct(keys_cache.shape, bf16)

    def near(*arrays):
        return [pltpu.with_memory_space_constraint(a, pltpu.VMEM) for a in arrays]

    def far(*arrays):
        return [pltpu.with_memory_space_constraint(a, pltpu.HBM) for a in arrays]

    def limit(mib):
        return pltpu.CompilerParams(vmem_limit_bytes=mib << 20)

    parts, biases = pl.pallas_call(
        project_kernel,
        out_shape=(
            jax.ShapeDtypeStruct((N_KV, PROPS, ROWS), bf16),
            pltpu.VMEM(cum_gates.shape, f32),
        ),
        in_specs=[SM, SM, VM, VM, VM, VM, VM, VM, VM],
        out_specs=(VM, VM),
        scratch_shapes=[pltpu.VMEM((16, ROWS), f32)],
        name="project",
    )(
        prior_len,
        accepted,
        tokens.T,
        norm_gain[None],
        w_query,
        w_key,
        w_value,
        w_gate.T,
        cum_gates,
    )
    arrived = lax.all_to_all(parts, KV, 0, 0, tiled=True)

    tp_count = lax.axis_size("tp")

    def gathered(name, first, second, after, out_shape):
        return pl.pallas_call(
            join_kernel,
            out_shape=out_shape((2 * len(first), *first.shape[1:]), bf16),
            in_specs=[VM, VM, ANY],
            out_specs=VM,
            compiler_params=limit(2),
            name=name,
        )(*far(first, second, after))

    def across(x, bit):
        return lax.ppermute(x, "tp", [(i, i ^ bit) for i in range(tp_count)])

    w_0 = w_out.T
    w_4 = across(w_0, 4)
    w_pair = gathered("pair", w_0[None], w_4[None], parts, jax.ShapeDtypeStruct)
    w_2 = across(w_pair, 2)

    block = pl.pallas_call(
        share_kernel,
        out_shape=pltpu.VMEM((N_KV, PROPS, ROWS), bf16),
        in_specs=[SM, VM, ANY],
        out_specs=VM,
        compiler_params=limit(8),
        cost_estimate=pl.CostEstimate(
            flops=10_000_000_000, bytes_accessed=800_000, transcendentals=0
        ),
        name="share",
    )(*far(gate_bias), *near(arrived), *far(w_2))
    joined = lax.all_to_all(block, KV, 0, 0, tiled=True)

    sent, keys_copy = pl.pallas_call(
        attention_kernel,
        out_shape=(pltpu.VMEM((512, WIDTH), bf16), cache),
        in_specs=[SM, VM, VM, VM, VM],
        out_specs=(VM, ANY),
        scratch_shapes=[
            pltpu.VMEM((ROWS, 8), f32),
            pltpu.VMEM((SEQS, 2 * PROPS, LEN), f32),
            pltpu.VMEM((SEQS, 2 * PROPS, LEN), bf16),
            pltpu.VMEM((SEQS, 2 * PROPS, WIDTH), f32),
            pltpu.VMEM((SEQS, 2 * PROPS, WIDTH), f32),
            pltpu.VMEM((512, WIDTH), f32),
            pltpu.SemaphoreType.DMA((4,)),
        ],
        compiler_params=limit(12),
        name="attention",
    )(*far(parents.T), *near(joined, biases, keys_cache, values_cache))
    pieces = lax.all_to_all(sent.reshape(256, 2, WIDTH), (*KV, "tp"), 0, 0, tiled=True)

    combined = pl.pallas_call(
        combine_kernel,
        out_shape=jax.ShapeDtypeStruct((N_KV, PROPS, WIDTH), bf16),
        in_specs=[VM],
        out_specs=VM,
        scratch_shapes=[pltpu.VMEM((64, 8, WIDTH), f32), pltpu.VMEM((64, 8, WIDTH), f32)],
        compiler_params=limit(8),
        name="combine",
    )(*near(pieces.reshape(512, WIDTH)))
    shared = lax.all_to_all(combined, KV, 0, 0, tiled=True)
    w_even = gathered("four", w_pair, w_2, combined, pltpu.VMEM)
    w_odd = across(w_even, 1)

    keys_out, values_out = pl.pallas_call(
        write_kernel,
        out_shape=(cache, cache),
        in_specs=[SM, SM, VM, ANY, ANY, ANY],
        out_specs=(ANY, ANY),
        input_output_aliases={4: 0},
        scratch_shapes=[
            pltpu.VMEM((SEQS, WINDOW, WIDTH), bf16),
            pltpu.VMEM(keys_cache.shape, bf16),
            pltpu.VMEM((ROWS, 8), f32),
            pltpu.SemaphoreType.DMA((SEQS,)),
            pltpu.SemaphoreType.DMA((SEQS,)),
            pltpu.SemaphoreType.DMA((2, 8)),
        ],
        compiler_params=limit(8),
        cost_estimate=pl.CostEstimate(
            flops=2_000_000_000, bytes_accessed=100_000, transcendentals=0
        ),
        name="write",
    )(
        *far(prior_len, accepted),
        *near(joined),
        *far(combined, keys_copy, values_cache),
    )

    mixed_rows = pl.pallas_call(
        output_kernel,
        out_shape=jax.ShapeDtypeStruct((48, 64), bf16),
        in_specs=[VM] * 3,
        out_specs=VM,
        scratch_shapes=[pltpu.VMEM((512, WIDTH), f32)],
        compiler_params=limit(8),
        name="output",
    )(*near(shared.reshape(512, WIDTH), w_even, w_odd))
    return (mixed_rows, keys_out, values_out)


def solution(mesh):
    torus = Mesh(mesh.devices.reshape(8, 4, mesh.shape["tp"]), ("kv_0", "kv_1", "tp"))
    in_specs = (
        P(None, KV),
        P(KV),
        P(KV, "tp"),
        P(KV, "tp"),
        P(KV, "tp"),
        P(),
        P(),
        P("tp", KV),
        P(None, KV, "tp"),
        P(None, KV, "tp"),
        P(None, "tp", KV),
        P(),
        P(),
        P(),
    )
    out_specs = (P("tp", KV), P(None, KV, "tp"), P(None, KV, "tp"))
    return jax.shard_map(
        shards, mesh=torus, in_specs=in_specs, out_specs=out_specs, check_vma=False
    )
```

```python
import jax
import jax.numpy as jnp
from jax import lax
from jax.experimental import pallas as pl
from jax.experimental.pallas import tpu as pltpu
from jax.sharding import Mesh
from jax.sharding import PartitionSpec as P

D = 2048
HEAD = 64
PROPS = 16
ROWS = 384
SEQS = 24
LEN = 512
WIDTH = 128
N_KV = 32
N_TP = 8
STATS = 24
WINDOW = 32
KV = ("kv_0", "kv_1")

masked_score = -1e30
lowest_max = -1e20
norm_eps = 1e-06

VM = pl.BlockSpec(memory_space=pltpu.VMEM)
SM = pl.BlockSpec(memory_space=pltpu.SMEM)
ANY = pl.BlockSpec(memory_space=pl.ANY)
bf16 = jnp.bfloat16
f32 = jnp.float32


def iota(shape, dim):
    return lax.broadcasted_iota(jnp.int32, shape, dim)


def high_low(x):
    high = x.astype(bf16).astype(f32)
    return high, (x - high).astype(bf16).astype(f32)


def dot_t(a, b):
    return lax.dot_general(a, b, (((1,), (1,)), ((), ())), preferred_element_type=f32)


def project_kernel(
    prior, accepted, tokens, gain, w_q, w_k, w_v, w_gate, cum, out, bias, gates
):
    kv, tp = lax.axis_index(KV), lax.axis_index("tp")
    columns = pl.ds(pl.multiple_of(lax.div(kv, 2) * WIDTH, WIDTH), WIDTH)
    floats = tokens[...].astype(f32)
    same = iota((64, 64), 0) == iota((64, 64), 1)
    gain_column = jnp.sum(jnp.where(same, gain[...], 0.0), axis=1, keepdims=True)
    scaled = floats * gain_column
    rows = jnp.transpose(scaled).astype(bf16)
    scaled = scaled.astype(bf16)
    for n, w in enumerate((w_q, w_k, w_v)):
        part = jnp.dot(rows, w[...], preferred_element_type=f32).astype(bf16)
        out[0:SEQS, :, n * WIDTH : (n + 1) * WIDTH] = part.reshape(SEQS, PROPS, WIDTH)
    sq_high, sq_low = high_low(floats * floats)
    ones = jnp.ones((8, 64), bf16)
    square_sum = jnp.dot(ones, sq_high.astype(bf16), preferred_element_type=f32) + jnp.dot(
        ones, sq_low.astype(bf16), preferred_element_type=f32
    )
    lane = iota((2, WIDTH), 1)
    position = iota((2, LEN), 1)
    last = jnp.zeros((2, WIDTH), f32)
    for b in range(SEQS):
        at = prior[b] + accepted[b] - 1 - kv * LEN
        here = cum[b]
        bias[b] = jnp.where(position <= at, -here, masked_score)
        found = jnp.sum(jnp.where(position == at, here, 0.0), axis=1, keepdims=True)
        last = jnp.where(lane == b, found, last)
    last_high, last_low = high_low(last)
    rest = last - last_high - last_low
    odd = lax.rem(kv, 2)
    zero = jnp.zeros_like(scaled)
    both = jnp.concatenate(
        [jnp.where(odd == 0, scaled, zero), jnp.where(odd == 1, scaled, zero)], axis=0
    )
    gates[...] = jnp.dot(w_gate[:, columns], both, preferred_element_type=f32)
    row = iota((8, ROWS), 0)
    gate_0 = gates[pl.ds(2 * tp, 1), :]
    gate_1 = gates[pl.ds(2 * tp + 1, 1), :]
    stats = jnp.where(row == 0, gate_0, jnp.where(row == 1, gate_1, 0.0))
    stats = jnp.where(row == 2, square_sum, stats)
    wide = jnp.zeros((2, ROWS - WIDTH), f32)
    last = jnp.concatenate([last, wide], axis=1)
    rest = jnp.concatenate([rest, wide], axis=1)
    stats = jnp.where(row == 3, last[0:1], jnp.where(row == 4, last[1:2], stats))
    stats = jnp.where(row == 5, rest[0:1], jnp.where(row == 6, rest[1:2], stats))
    out[STATS] = jnp.concatenate(high_low(stats), axis=0).astype(bf16)
    out[STATS + 1 :] = jnp.zeros((N_KV - STATS - 1, PROPS, ROWS), bf16)


def share_kernel(bias, parts, after_2, after_6, out):
    kv, tp = lax.axis_index(KV), lax.axis_index("tp")
    total = jnp.zeros((PROPS, ROWS), f32)
    for k in range(N_KV):
        total = total + parts[k].astype(f32)
    stats = total[0:8] + total[8:16]
    row = iota((8, ROWS), 0)
    inv_rms = lax.rsqrt(stats[2:3] / D + norm_eps)
    logits = inv_rms * stats + jnp.where(row == 0, bias[2 * tp], bias[2 * tp + 1])
    log_gates = jnp.minimum(logits, 0.0) - jnp.log1p(jnp.exp(-jnp.abs(logits)))
    stats = jnp.where(row < 2, log_gates, jnp.where(row == 2, inv_rms, stats))
    stats = jnp.concatenate(high_low(stats), axis=0)
    block = jnp.where(kv == STATS, stats, total).astype(bf16)
    for k in range(N_KV):
        out[k] = block


def attention_kernel(
    parents,
    joined,
    biases,
    keys,
    values,
    out,
    keys_out,
    columns,
    scores_buf,
    weights_buf,
    v_buf,
    stat_buf,
    mixed,
    sems,
):
    kv = lax.axis_index(KV)
    moves = []
    for t in range(4):
        six = pl.ds(6 * t, 6)
        moves.append(pltpu.make_async_copy(keys.at[six], keys_out.at[six], sems.at[t]))
    for move in moves:
        move.start()
    coded = joined[STATS].astype(f32)
    stats = coded[0:8] + coded[8:16]
    columns[...] = jnp.transpose(stats)
    lane = iota((PROPS, WIDTH), 1)
    first_head = lane < HEAD
    lane_out = iota((2 * PROPS, WIDTH), 1)
    first_row = iota((2 * PROPS, WIDTH), 0) < PROPS
    scale = HEAD**-0.5

    def both_heads(b_rows, b_block):
        inv = columns[b_rows, 2:3]
        q = (inv * joined[b_block, :, 0:WIDTH].astype(f32)).astype(bf16).astype(f32) * scale
        zero = jnp.zeros_like(q)
        return jnp.concatenate(
            [jnp.where(first_head, q, zero), jnp.where(first_head, zero, q)], axis=0
        ).astype(bf16)

    def coded_stats(s, top, total):
        place = lane_out - (HEAD + 4 * s)
        top_high, top_low = high_low(top)
        sum_high, sum_low = high_low(total)
        stats = jnp.where(place == 0, top_high, jnp.where(place == 1, top_low, 0.0))
        return jnp.where(place == 2, sum_high, jnp.where(place == 3, sum_low, stats))

    def sendable(top):
        high, low = high_low(jnp.maximum(top, lowest_max))
        return high + low

    own = jnp.minimum(kv, SEQS - 1)
    low = lane_out < HEAD

    def score(b):
        q = both_heads(pl.ds(PROPS * b, PROPS), b)
        bias = biases[b]
        bias = jnp.concatenate(
            [
                jnp.broadcast_to(bias[0:1], (PROPS, LEN)),
                jnp.broadcast_to(bias[1:2], (PROPS, LEN)),
            ],
            axis=0,
        )
        scores_buf[b] = dot_t(q, keys[b]) + bias

    def weigh(b):
        scores = scores_buf[b]
        top = sendable(jnp.max(scores, axis=1, keepdims=True))
        weights = jnp.exp(scores - top)
        total = jnp.sum(weights, axis=1, keepdims=True)
        weights_buf[b] = weights.astype(bf16)
        stat_buf[b] = coded_stats(b % 3, top, total)

    def gather(b):
        v_buf[b] = jnp.dot(weights_buf[b], values[b], preferred_element_type=f32)

    def pack(t):
        v = [v_buf[3 * t + s] for s in range(3)]
        turned = [pltpu.roll(x, HEAD, 1) for x in v]
        first = jnp.where(first_row, v[0], turned[0])
        second = jnp.where(first_row, turned[1], v[1])
        third = jnp.where(first_row, v[2], turned[2])
        stats = stat_buf[3 * t] + stat_buf[3 * t + 1] + stat_buf[3 * t + 2]
        mixed[pl.ds(2 * t, N_KV, stride=16), :] = jnp.where(low, first, second)
        mixed[pl.ds(2 * t + 1, N_KV, stride=16), :] = jnp.where(low, third, stats)

    def lineage():
        row = iota((PROPS, WIDTH), 0)
        linked = jnp.where(lane == row, 1.0, 0.0)
        for i in range(PROPS):
            linked = jnp.where((row == i) & (lane == parents[i, own]), 1.0, linked)
        return linked

    def squared(linked):
        other = jnp.concatenate([linked, jnp.zeros((WIDTH - PROPS, WIDTH), f32)], axis=0)
        product = jnp.dot(linked.astype(bf16), other.astype(bf16), preferred_element_type=f32)
        return jnp.minimum(product, 1.0)

    def tree(reached):
        mine = pl.ds(pl.multiple_of(PROPS * own, PROPS), PROPS)
        pad = jnp.zeros((WIDTH - PROPS, WIDTH), f32)
        picks = (iota((ROWS, WIDTH), 0) == iota((ROWS, WIDTH), 1) + PROPS * own) & (
            iota((ROWS, WIDTH), 1) < PROPS
        )
        own_gates = jnp.dot(
            joined[STATS], jnp.where(picks, 1.0, 0.0).astype(bf16), preferred_element_type=f32
        ).astype(bf16)
        tree = dot_t(own_gates, jnp.concatenate([reached, pad], axis=0).astype(bf16))
        tree = tree[0:8] + tree[8:16]
        last = jnp.sum(
            jnp.where(iota((8, WIDTH), 1) == own, stats[:, 0:WIDTH], 0.0), axis=1, keepdims=True
        )
        tree_bias = jnp.concatenate(
            [
                jnp.broadcast_to(-(last[3:4] + last[5:6] + tree[0:1]), (PROPS, WIDTH)),
                jnp.broadcast_to(-(last[4:5] + last[6:7] + tree[1:2]), (PROPS, WIDTH)),
            ],
            axis=0,
        )
        own_inv = columns[mine, 2:3]
        new_keys = own_inv * joined[own, :, WIDTH : 2 * WIDTH].astype(f32)
        new_values = own_inv * joined[own, :, 2 * WIDTH : 3 * WIDTH].astype(f32)
        new_keys = jnp.concatenate([new_keys, pad], axis=0).astype(bf16)
        new_values = jnp.concatenate([new_values, pad], axis=0).astype(bf16)
        needed = jnp.where(kv < SEQS, 0.5, 2.0)
        live = jnp.concatenate([reached, reached], axis=0) > needed
        tree_scores = jnp.where(live, dot_t(both_heads(mine, own), new_keys) + tree_bias, masked_score)
        tree_top = jnp.max(tree_scores, axis=1, keepdims=True)
        return tree_scores, tree_top, new_values

    for step in range(N_TP + 2):
        for s in range(3):
            if step < N_TP:
                score(3 * step + s)
            if 1 <= step <= N_TP:
                weigh(3 * step - 3 + s)
            if step >= 2:
                gather(3 * step - 6 + s)
        if step == 0:
            reached = lineage()
        if 1 <= step <= 4:
            reached = squared(reached)
        if step == 5:
            tree_scores, tree_top, new_values = tree(reached)
        if step == N_TP:
            scores = scores_buf[own]
            top = jnp.maximum(jnp.max(scores, axis=1, keepdims=True), tree_top)
            top = sendable(top)
            own_weights = jnp.exp(scores - top)
            tree_weights = jnp.exp(tree_scores - top)
            own_total = jnp.sum(own_weights, axis=1, keepdims=True) + jnp.sum(
                tree_weights, axis=1, keepdims=True
            )
            own_stats = coded_stats(lax.rem(own, 3), top, own_total)
    own_v = jnp.dot(
        own_weights.astype(bf16), values[own], preferred_element_type=f32
    ) + jnp.dot(tree_weights.astype(bf16), new_values, preferred_element_type=f32)
    stat_buf[own] = own_stats
    v_buf[own] = own_v
    for t in range(N_TP):
        pack(t)
    out[...] = mixed[...].astype(bf16)
    for move in moves:
        move.wait()


def combine_kernel(parts, out, tops, sums):
    row = iota((WIDTH, 4 * WIDTH), 0) - HEAD
    column = iota((WIDTH, 4 * WIDTH), 1)
    unit = jnp.where(column < 2 * WIDTH, lax.rem(lax.div(column, HEAD), 2), 2)
    kind = lax.rem(lax.div(column, WIDTH), 2)
    row = row - 4 * unit - 2 * kind
    spread = jnp.where((row == 0) | (row == 1), 1.0, 0.0).astype(bf16)
    even = lax.rem(iota((8, WIDTH), 0), 2) == 0
    for n in range(4):
        stats = jnp.dot(parts[128 * n : 128 * n + 128], spread, preferred_element_type=f32)
        for v in range(16):
            rows = stats[8 * v : 8 * v + 8]
            near = pltpu.roll(rows[:, 0 : 2 * WIDTH], 7, 0)
            tops[16 * n + v] = jnp.where(even, near[:, 0:WIDTH], rows[:, 2 * WIDTH : 3 * WIDTH])
            sums[16 * n + v] = jnp.where(even, near[:, WIDTH:], rows[:, 3 * WIDTH :])
    results = []
    for half in range(2):
        top = tops[half]
        for k in range(1, N_KV):
            top = jnp.maximum(top, tops[2 * k + half])
        above = jnp.zeros((8, WIDTH), f32)
        below = jnp.zeros((8, WIDTH), f32)
        for k in range(N_KV):
            v = 2 * k + half
            factor = jnp.exp(tops[v] - top)
            above = above + factor * parts[8 * v : 8 * v + 8, :].astype(f32)
            below = below + factor * sums[v]
        results.append(above / below)
    block = jnp.concatenate(results, axis=0).astype(bf16)
    for k in range(N_KV):
        out[k] = block


def output_kernel(shared, w_even, w_odd, out, rows):
    tp = lax.axis_index("tp")
    rows[...] = shared[...].astype(f32)
    near = (w_even[0], w_odd[0], w_even[2], w_odd[2], w_even[1], w_odd[1], w_even[3], w_odd[3])
    near = [w.astype(f32) for w in near]
    for bit in (1, 2, 4):
        swap = (tp & bit) != 0
        near = [jnp.where(swap, near[g ^ bit], near[g]) for g in range(N_TP)]
    low = iota((PROPS, WIDTH), 1) < HEAD
    total = jnp.zeros((48, 64), f32)
    for g in range(N_TP):
        pair_0 = rows[pl.ds(2 * g, PROPS, stride=16), :]
        pair_1 = rows[pl.ds(256 + 2 * g, PROPS, stride=16), :]
        last_0 = rows[pl.ds(2 * g + 1, PROPS, stride=16), :]
        last_1 = rows[pl.ds(257 + 2 * g, PROPS, stride=16), :]
        block = jnp.concatenate(
            [
                jnp.where(low, pair_0, pltpu.roll(pair_1, HEAD, 1)),
                jnp.where(low, pltpu.roll(pair_0, HEAD, 1), pair_1),
                jnp.where(low, last_0, pltpu.roll(last_1, HEAD, 1)),
            ],
            axis=0,
        )
        total = total + dot_t(block.astype(bf16), near[g].astype(bf16))
    out[...] = total.astype(bf16)


def join_kernel(first, second, third, fourth, after, out):
    for n, w in enumerate((first, second, third, fourth)):
        out[n] = w[...]


def write_kernel(
    prior,
    accepted,
    joined,
    after,
    keys_in,
    values_in,
    keys,
    values,
    buf,
    near,
    columns,
    in_sem,
    out_sem,
    near_sem,
):
    moves = []
    for t in range(8):
        three = pl.ds(3 * t, 3)
        moves.append(
            (
                pltpu.make_async_copy(values_in.at[three], near.at[three], near_sem.at[0, t]),
                pltpu.make_async_copy(near.at[three], values.at[three], near_sem.at[1, t]),
            )
        )
    offset = lax.axis_index(KV) * LEN

    def place(b):
        start = prior[b] + accepted[b] - offset
        base = jnp.clip(lax.div(jnp.maximum(start, 0), 16) * 16, 0, LEN - WINDOW)
        hit = (start > -PROPS) & (start < LEN)
        return start, pl.multiple_of(base, 16), hit

    def copy_in(b, base):
        return pltpu.make_async_copy(
            keys.at[b, pl.ds(base, WINDOW), :], buf.at[b], in_sem.at[b]
        )

    def copy_out(b, base):
        return pltpu.make_async_copy(
            buf.at[b], keys.at[b, pl.ds(base, WINDOW), :], out_sem.at[b]
        )

    @pl.loop(0, SEQS)
    def _(b):
        start, base, hit = place(b)

        @pl.when(hit)
        def _():
            copy_in(b, base).start()

    for move in moves:
        move[0].start()
    coded = joined[STATS].astype(f32)
    columns[...] = jnp.transpose(coded[0:8] + coded[8:16])

    def patched(b, start, base):
        inv = columns[pl.ds(pl.multiple_of(PROPS * b, PROPS), PROPS), 2:3]
        slot = iota((WINDOW, PROPS), 0) + (base - start)
        selector = jnp.where(slot == iota((WINDOW, PROPS), 1), 1.0, 0.0).astype(bf16)
        raw = joined[b, :, WIDTH:].astype(f32)
        rows = jnp.dot(selector, (inv * raw).astype(bf16), preferred_element_type=f32)
        slot = iota((WINDOW, WIDTH), 0) + (base - start)
        return (slot >= 0) & (slot < PROPS), rows

    for t in range(8):
        moves[t][0].wait()

        @pl.loop(3 * t, 3 * t + 3)
        def _(b):
            start, base, hit = place(b)

            @pl.when(hit)
            def _():
                inside, rows = patched(b, start, base)
                window = pl.ds(base, WINDOW)
                held = near[b, window, :].astype(f32)
                near[b, window, :] = jnp.where(inside, rows[:, WIDTH:], held).astype(bf16)
                copy_in(b, base).wait()
                held = buf[b].astype(f32)
                buf[b] = jnp.where(inside, rows[:, 0:WIDTH], held).astype(bf16)
                copy_out(b, base).start()

        moves[t][1].start()
    for move in moves:
        move[1].wait()

    @pl.loop(0, SEQS)
    def _(b):
        start, base, hit = place(b)

        @pl.when(hit)
        def _():
            copy_out(b, base).wait()


def shards(
    tokens,
    norm_gain,
    w_query,
    w_key,
    w_value,
    w_gate,
    gate_bias,
    w_out,
    keys_cache,
    values_cache,
    cum_gates,
    prior_len,
    accepted,
    parents,
):
    cache = jax.ShapeDtypeStruct(keys_cache.shape, bf16)

    def near(*arrays):
        return [pltpu.with_memory_space_constraint(a, pltpu.VMEM) for a in arrays]

    def far(*arrays):
        return [pltpu.with_memory_space_constraint(a, pltpu.HBM) for a in arrays]

    def limit(mib):
        return pltpu.CompilerParams(vmem_limit_bytes=mib << 20)

    parts, biases = pl.pallas_call(
        project_kernel,
        out_shape=(
            jax.ShapeDtypeStruct((N_KV, PROPS, ROWS), bf16),
            pltpu.VMEM(cum_gates.shape, f32),
        ),
        in_specs=[SM, SM, VM, VM, VM, VM, VM, VM, VM],
        out_specs=(VM, VM),
        scratch_shapes=[pltpu.VMEM((16, ROWS), f32)],
        name="project",
    )(
        prior_len,
        accepted,
        tokens.T,
        norm_gain[None],
        w_query,
        w_key,
        w_value,
        w_gate.T,
        cum_gates,
    )
    arrived = lax.all_to_all(parts, KV, 0, 0, tiled=True)

    tp_count = lax.axis_size("tp")

    def across(x, bit):
        return lax.ppermute(x, "tp", [(i, i ^ bit) for i in range(tp_count)])

    w_0 = w_out.T
    w_4 = across(w_0, 4)
    w_2 = across(w_0, 2)
    w_6 = across(w_4, 2)

    block = pl.pallas_call(
        share_kernel,
        out_shape=pltpu.VMEM((N_KV, PROPS, ROWS), bf16),
        in_specs=[SM, VM, ANY, ANY],
        out_specs=VM,
        compiler_params=limit(8),
        cost_estimate=pl.CostEstimate(
            flops=10_000_000_000, bytes_accessed=800_000, transcendentals=0
        ),
        name="share",
    )(*far(gate_bias), *near(arrived), *far(w_2, w_6))
    joined = lax.all_to_all(block, KV, 0, 0, tiled=True)

    sent, keys_copy = pl.pallas_call(
        attention_kernel,
        out_shape=(pltpu.VMEM((512, WIDTH), bf16), cache),
        in_specs=[SM, VM, VM, VM, VM],
        out_specs=(VM, ANY),
        scratch_shapes=[
            pltpu.VMEM((ROWS, 8), f32),
            pltpu.VMEM((SEQS, 2 * PROPS, LEN), f32),
            pltpu.VMEM((SEQS, 2 * PROPS, LEN), bf16),
            pltpu.VMEM((SEQS, 2 * PROPS, WIDTH), f32),
            pltpu.VMEM((SEQS, 2 * PROPS, WIDTH), f32),
            pltpu.VMEM((512, WIDTH), f32),
            pltpu.SemaphoreType.DMA((4,)),
        ],
        compiler_params=limit(12),
        name="attention",
    )(*far(parents.T), *near(joined, biases, keys_cache, values_cache))
    pieces = lax.all_to_all(sent.reshape(256, 2, WIDTH), (*KV, "tp"), 0, 0, tiled=True)

    combined = pl.pallas_call(
        combine_kernel,
        out_shape=jax.ShapeDtypeStruct((N_KV, PROPS, WIDTH), bf16),
        in_specs=[VM],
        out_specs=VM,
        scratch_shapes=[pltpu.VMEM((64, 8, WIDTH), f32), pltpu.VMEM((64, 8, WIDTH), f32)],
        compiler_params=limit(8),
        name="combine",
    )(*near(pieces.reshape(512, WIDTH)))
    shared = lax.all_to_all(combined, KV, 0, 0, tiled=True)
    w_even = pl.pallas_call(
        join_kernel,
        out_shape=pltpu.VMEM((4, *w_0.shape), bf16),
        in_specs=[VM] * 4 + [ANY],
        out_specs=VM,
        compiler_params=limit(2),
        name="four",
    )(*far(w_0, w_4, w_2, w_6, combined))
    w_odd = across(w_even, 1)

    keys_out, values_out = pl.pallas_call(
        write_kernel,
        out_shape=(cache, cache),
        in_specs=[SM, SM, VM, ANY, ANY, ANY],
        out_specs=(ANY, ANY),
        input_output_aliases={4: 0},
        scratch_shapes=[
            pltpu.VMEM((SEQS, WINDOW, WIDTH), bf16),
            pltpu.VMEM(keys_cache.shape, bf16),
            pltpu.VMEM((ROWS, 8), f32),
            pltpu.SemaphoreType.DMA((SEQS,)),
            pltpu.SemaphoreType.DMA((SEQS,)),
            pltpu.SemaphoreType.DMA((2, 8)),
        ],
        compiler_params=limit(8),
        cost_estimate=pl.CostEstimate(
            flops=2_000_000_000, bytes_accessed=100_000, transcendentals=0
        ),
        name="write",
    )(
        *far(prior_len, accepted),
        *near(joined),
        *far(combined, keys_copy, values_cache),
    )

    mixed_rows = pl.pallas_call(
        output_kernel,
        out_shape=jax.ShapeDtypeStruct((48, 64), bf16),
        in_specs=[VM] * 3,
        out_specs=VM,
        scratch_shapes=[pltpu.VMEM((512, WIDTH), f32)],
        compiler_params=limit(8),
        name="output",
    )(*near(shared.reshape(512, WIDTH), w_even, w_odd))
    return (mixed_rows, keys_out, values_out)


def solution(mesh):
    torus = Mesh(mesh.devices.reshape(8, 4, mesh.shape["tp"]), ("kv_0", "kv_1", "tp"))
    in_specs = (
        P(None, KV),
        P(KV),
        P(KV, "tp"),
        P(KV, "tp"),
        P(KV, "tp"),
        P(),
        P(),
        P("tp", KV),
        P(None, KV, "tp"),
        P(None, KV, "tp"),
        P(None, "tp", KV),
        P(),
        P(),
        P(),
    )
    out_specs = (P("tp", KV), P(None, KV, "tp"), P(None, KV, "tp"))
    return jax.shard_map(
        shards, mesh=torus, in_specs=in_specs, out_specs=out_specs, check_vma=False
    )
```

```python
import jax
import jax.numpy as jnp
from jax import lax
from jax.experimental import pallas as pl
from jax.experimental.pallas import tpu as pltpu
from jax.sharding import Mesh
from jax.sharding import PartitionSpec as P

D = 2048
HEAD = 64
PROPS = 16
ROWS = 384
SEQS = 24
LEN = 512
WIDTH = 128
N_KV = 32
N_TP = 8
STATS = 24
WINDOW = 32
KV = ("kv_0", "kv_1")

masked_score = -1e30
lowest_max = -1e20
norm_eps = 1e-06

VM = pl.BlockSpec(memory_space=pltpu.VMEM)
SM = pl.BlockSpec(memory_space=pltpu.SMEM)
ANY = pl.BlockSpec(memory_space=pl.ANY)
bf16 = jnp.bfloat16
f32 = jnp.float32


def iota(shape, dim):
    return lax.broadcasted_iota(jnp.int32, shape, dim)


def high_low(x):
    high = x.astype(bf16).astype(f32)
    return high, (x - high).astype(bf16).astype(f32)


def dot_t(a, b):
    return lax.dot_general(a, b, (((1,), (1,)), ((), ())), preferred_element_type=f32)


def project_kernel(
    prior, accepted, tokens, gain, w_q, w_k, w_v, w_gate, cum, out, bias, gates
):
    kv, tp = lax.axis_index(KV), lax.axis_index("tp")
    columns = pl.ds(pl.multiple_of(lax.div(kv, 2) * WIDTH, WIDTH), WIDTH)
    floats = tokens[...].astype(f32)
    same = iota((64, 64), 0) == iota((64, 64), 1)
    gain_column = jnp.sum(jnp.where(same, gain[...], 0.0), axis=1, keepdims=True)
    scaled = floats * gain_column
    rows = jnp.transpose(scaled).astype(bf16)
    scaled = scaled.astype(bf16)
    for n, w in enumerate((w_q, w_k, w_v)):
        part = jnp.dot(rows, w[...], preferred_element_type=f32).astype(bf16)
        out[0:SEQS, :, n * WIDTH : (n + 1) * WIDTH] = part.reshape(SEQS, PROPS, WIDTH)
    sq_high, sq_low = high_low(floats * floats)
    ones = jnp.ones((8, 64), bf16)
    square_sum = jnp.dot(ones, sq_high.astype(bf16), preferred_element_type=f32) + jnp.dot(
        ones, sq_low.astype(bf16), preferred_element_type=f32
    )
    lane = iota((2, WIDTH), 1)
    position = iota((2, LEN), 1)
    last = jnp.zeros((2, WIDTH), f32)
    for b in range(SEQS):
        at = prior[b] + accepted[b] - 1 - kv * LEN
        here = cum[b]
        bias[b] = jnp.where(position <= at, -here, masked_score)
        found = jnp.sum(jnp.where(position == at, here, 0.0), axis=1, keepdims=True)
        last = jnp.where(lane == b, found, last)
    last_high, last_low = high_low(last)
    rest = last - last_high - last_low
    odd = lax.rem(kv, 2)
    zero = jnp.zeros_like(scaled)
    both = jnp.concatenate(
        [jnp.where(odd == 0, scaled, zero), jnp.where(odd == 1, scaled, zero)], axis=0
    )
    gates[...] = jnp.dot(w_gate[:, columns], both, preferred_element_type=f32)
    row = iota((8, ROWS), 0)
    gate_0 = gates[pl.ds(2 * tp, 1), :]
    gate_1 = gates[pl.ds(2 * tp + 1, 1), :]
    stats = jnp.where(row == 0, gate_0, jnp.where(row == 1, gate_1, 0.0))
    stats = jnp.where(row == 2, square_sum, stats)
    wide = jnp.zeros((2, ROWS - WIDTH), f32)
    last = jnp.concatenate([last, wide], axis=1)
    rest = jnp.concatenate([rest, wide], axis=1)
    stats = jnp.where(row == 3, last[0:1], jnp.where(row == 4, last[1:2], stats))
    stats = jnp.where(row == 5, rest[0:1], jnp.where(row == 6, rest[1:2], stats))
    out[STATS] = jnp.concatenate(high_low(stats), axis=0).astype(bf16)
    out[STATS + 1 :] = jnp.zeros((N_KV - STATS - 1, PROPS, ROWS), bf16)


def share_kernel(bias, parts, after, out):
    kv, tp = lax.axis_index(KV), lax.axis_index("tp")
    total = jnp.zeros((PROPS, ROWS), f32)
    for k in range(N_KV):
        total = total + parts[k].astype(f32)
    stats = total[0:8] + total[8:16]
    row = iota((8, ROWS), 0)
    inv_rms = lax.rsqrt(stats[2:3] / D + norm_eps)
    logits = inv_rms * stats + jnp.where(row == 0, bias[2 * tp], bias[2 * tp + 1])
    log_gates = jnp.minimum(logits, 0.0) - jnp.log1p(jnp.exp(-jnp.abs(logits)))
    stats = jnp.where(row < 2, log_gates, jnp.where(row == 2, inv_rms, stats))
    stats = jnp.concatenate(high_low(stats), axis=0)
    block = jnp.where(kv == STATS, stats, total).astype(bf16)
    for k in range(N_KV):
        out[k] = block


def attention_kernel(
    parents,
    joined,
    biases,
    keys,
    values,
    out,
    keys_out,
    columns,
    scores_buf,
    weights_buf,
    v_buf,
    stat_buf,
    mixed,
    sems,
):
    kv = lax.axis_index(KV)
    moves = []
    for t in range(4):
        six = pl.ds(6 * t, 6)
        moves.append(pltpu.make_async_copy(keys.at[six], keys_out.at[six], sems.at[t]))
    for move in moves:
        move.start()
    coded = joined[STATS].astype(f32)
    stats = coded[0:8] + coded[8:16]
    columns[...] = jnp.transpose(stats)
    lane = iota((PROPS, WIDTH), 1)
    first_head = lane < HEAD
    lane_out = iota((2 * PROPS, WIDTH), 1)
    first_row = iota((2 * PROPS, WIDTH), 0) < PROPS
    scale = HEAD**-0.5

    def both_heads(b_rows, b_block):
        inv = columns[b_rows, 2:3]
        q = (inv * joined[b_block, :, 0:WIDTH].astype(f32)).astype(bf16).astype(f32) * scale
        zero = jnp.zeros_like(q)
        return jnp.concatenate(
            [jnp.where(first_head, q, zero), jnp.where(first_head, zero, q)], axis=0
        ).astype(bf16)

    def coded_stats(s, top, total):
        place = lane_out - (HEAD + 4 * s)
        top_high, top_low = high_low(top)
        sum_high, sum_low = high_low(total)
        stats = jnp.where(place == 0, top_high, jnp.where(place == 1, top_low, 0.0))
        return jnp.where(place == 2, sum_high, jnp.where(place == 3, sum_low, stats))

    def sendable(top):
        high, low = high_low(jnp.maximum(top, lowest_max))
        return high + low

    own = jnp.minimum(kv, SEQS - 1)
    low = lane_out < HEAD

    def score(b):
        q = both_heads(pl.ds(PROPS * b, PROPS), b)
        bias = biases[b]
        bias = jnp.concatenate(
            [
                jnp.broadcast_to(bias[0:1], (PROPS, LEN)),
                jnp.broadcast_to(bias[1:2], (PROPS, LEN)),
            ],
            axis=0,
        )
        scores_buf[b] = dot_t(q, keys[b]) + bias

    def weigh(b):
        scores = scores_buf[b]
        top = sendable(jnp.max(scores, axis=1, keepdims=True))
        weights = jnp.exp(scores - top)
        total = jnp.sum(weights, axis=1, keepdims=True)
        weights_buf[b] = weights.astype(bf16)
        stat_buf[b] = coded_stats(b % 3, top, total)

    def gather(b):
        v_buf[b] = jnp.dot(weights_buf[b], values[b], preferred_element_type=f32)

    def pack(t):
        v = [v_buf[3 * t + s] for s in range(3)]
        turned = [pltpu.roll(x, HEAD, 1) for x in v]
        first = jnp.where(first_row, v[0], turned[0])
        second = jnp.where(first_row, turned[1], v[1])
        third = jnp.where(first_row, v[2], turned[2])
        stats = stat_buf[3 * t] + stat_buf[3 * t + 1] + stat_buf[3 * t + 2]
        mixed[pl.ds(2 * t, N_KV, stride=16), :] = jnp.where(low, first, second)
        mixed[pl.ds(2 * t + 1, N_KV, stride=16), :] = jnp.where(low, third, stats)

    def lineage():
        row = iota((PROPS, WIDTH), 0)
        linked = jnp.where(lane == row, 1.0, 0.0)
        for i in range(PROPS):
            linked = jnp.where((row == i) & (lane == parents[i, own]), 1.0, linked)
        return linked

    def squared(linked):
        other = jnp.concatenate([linked, jnp.zeros((WIDTH - PROPS, WIDTH), f32)], axis=0)
        product = jnp.dot(linked.astype(bf16), other.astype(bf16), preferred_element_type=f32)
        return jnp.minimum(product, 1.0)

    def tree(reached):
        mine = pl.ds(pl.multiple_of(PROPS * own, PROPS), PROPS)
        pad = jnp.zeros((WIDTH - PROPS, WIDTH), f32)
        picks = (iota((ROWS, WIDTH), 0) == iota((ROWS, WIDTH), 1) + PROPS * own) & (
            iota((ROWS, WIDTH), 1) < PROPS
        )
        own_gates = jnp.dot(
            joined[STATS], jnp.where(picks, 1.0, 0.0).astype(bf16), preferred_element_type=f32
        ).astype(bf16)
        tree = dot_t(own_gates, jnp.concatenate([reached, pad], axis=0).astype(bf16))
        tree = tree[0:8] + tree[8:16]
        last = jnp.sum(
            jnp.where(iota((8, WIDTH), 1) == own, stats[:, 0:WIDTH], 0.0), axis=1, keepdims=True
        )
        tree_bias = jnp.concatenate(
            [
                jnp.broadcast_to(-(last[3:4] + last[5:6] + tree[0:1]), (PROPS, WIDTH)),
                jnp.broadcast_to(-(last[4:5] + last[6:7] + tree[1:2]), (PROPS, WIDTH)),
            ],
            axis=0,
        )
        own_inv = columns[mine, 2:3]
        new_keys = own_inv * joined[own, :, WIDTH : 2 * WIDTH].astype(f32)
        new_values = own_inv * joined[own, :, 2 * WIDTH : 3 * WIDTH].astype(f32)
        new_keys = jnp.concatenate([new_keys, pad], axis=0).astype(bf16)
        new_values = jnp.concatenate([new_values, pad], axis=0).astype(bf16)
        needed = jnp.where(kv < SEQS, 0.5, 2.0)
        live = jnp.concatenate([reached, reached], axis=0) > needed
        tree_scores = jnp.where(live, dot_t(both_heads(mine, own), new_keys) + tree_bias, masked_score)
        tree_top = jnp.max(tree_scores, axis=1, keepdims=True)
        return tree_scores, tree_top, new_values

    for step in range(N_TP + 2):
        for s in range(3):
            if step < N_TP:
                score(3 * step + s)
            if 1 <= step <= N_TP:
                weigh(3 * step - 3 + s)
            if step >= 2:
                gather(3 * step - 6 + s)
        if step == 0:
            reached = lineage()
        if 1 <= step <= 4:
            reached = squared(reached)
        if step == 5:
            tree_scores, tree_top, new_values = tree(reached)
        if step == N_TP:
            scores = scores_buf[own]
            top = jnp.maximum(jnp.max(scores, axis=1, keepdims=True), tree_top)
            top = sendable(top)
            own_weights = jnp.exp(scores - top)
            tree_weights = jnp.exp(tree_scores - top)
            own_total = jnp.sum(own_weights, axis=1, keepdims=True) + jnp.sum(
                tree_weights, axis=1, keepdims=True
            )
            own_stats = coded_stats(lax.rem(own, 3), top, own_total)
    own_v = jnp.dot(
        own_weights.astype(bf16), values[own], preferred_element_type=f32
    ) + jnp.dot(tree_weights.astype(bf16), new_values, preferred_element_type=f32)
    stat_buf[own] = own_stats
    v_buf[own] = own_v
    for t in range(N_TP):
        pack(t)
    out[...] = mixed[...].astype(bf16)
    for move in moves:
        move.wait()


def combine_kernel(parts, out, tops, sums):
    row = iota((WIDTH, 4 * WIDTH), 0) - HEAD
    column = iota((WIDTH, 4 * WIDTH), 1)
    unit = jnp.where(column < 2 * WIDTH, lax.rem(lax.div(column, HEAD), 2), 2)
    kind = lax.rem(lax.div(column, WIDTH), 2)
    row = row - 4 * unit - 2 * kind
    spread = jnp.where((row == 0) | (row == 1), 1.0, 0.0).astype(bf16)
    even = lax.rem(iota((8, WIDTH), 0), 2) == 0
    for n in range(4):
        stats = jnp.dot(parts[128 * n : 128 * n + 128], spread, preferred_element_type=f32)
        for v in range(16):
            rows = stats[8 * v : 8 * v + 8]
            near = pltpu.roll(rows[:, 0 : 2 * WIDTH], 7, 0)
            tops[16 * n + v] = jnp.where(even, near[:, 0:WIDTH], rows[:, 2 * WIDTH : 3 * WIDTH])
            sums[16 * n + v] = jnp.where(even, near[:, WIDTH:], rows[:, 3 * WIDTH :])
    results = []
    for half in range(2):
        top = tops[half]
        for k in range(1, N_KV):
            top = jnp.maximum(top, tops[2 * k + half])
        above = jnp.zeros((8, WIDTH), f32)
        below = jnp.zeros((8, WIDTH), f32)
        for k in range(N_KV):
            v = 2 * k + half
            factor = jnp.exp(tops[v] - top)
            above = above + factor * parts[8 * v : 8 * v + 8, :].astype(f32)
            below = below + factor * sums[v]
        results.append(above / below)
    block = jnp.concatenate(results, axis=0).astype(bf16)
    for k in range(N_KV):
        out[k] = block


def output_kernel(shared, w_even, w_odd, out, rows):
    tp = lax.axis_index("tp")
    rows[...] = shared[...].astype(f32)
    near = (w_even[0], w_odd[0], w_even[2], w_odd[2], w_even[1], w_odd[1], w_even[3], w_odd[3])
    near = [w.astype(f32) for w in near]
    for bit in (1, 2, 4):
        swap = (tp & bit) != 0
        near = [jnp.where(swap, near[g ^ bit], near[g]) for g in range(N_TP)]
    low = iota((PROPS, WIDTH), 1) < HEAD
    total = jnp.zeros((48, 64), f32)
    for g in range(N_TP):
        pair_0 = rows[pl.ds(2 * g, PROPS, stride=16), :]
        pair_1 = rows[pl.ds(256 + 2 * g, PROPS, stride=16), :]
        last_0 = rows[pl.ds(2 * g + 1, PROPS, stride=16), :]
        last_1 = rows[pl.ds(257 + 2 * g, PROPS, stride=16), :]
        block = jnp.concatenate(
            [
                jnp.where(low, pair_0, pltpu.roll(pair_1, HEAD, 1)),
                jnp.where(low, pltpu.roll(pair_0, HEAD, 1), pair_1),
                jnp.where(low, last_0, pltpu.roll(last_1, HEAD, 1)),
            ],
            axis=0,
        )
        total = total + dot_t(block.astype(bf16), near[g].astype(bf16))
    out[...] = total.astype(bf16)


def join_kernel(first, second, third, fourth, after, out):
    for n, w in enumerate((first, second, third, fourth)):
        out[n] = w[...]


def write_kernel(
    prior,
    accepted,
    joined,
    after,
    keys_in,
    values_in,
    keys,
    values,
    buf,
    near,
    columns,
    in_sem,
    out_sem,
    near_sem,
):
    moves = []
    for t in range(8):
        three = pl.ds(3 * t, 3)
        moves.append(
            (
                pltpu.make_async_copy(values_in.at[three], near.at[three], near_sem.at[0, t]),
                pltpu.make_async_copy(near.at[three], values.at[three], near_sem.at[1, t]),
            )
        )
    offset = lax.axis_index(KV) * LEN

    def place(b):
        start = prior[b] + accepted[b] - offset
        base = jnp.clip(lax.div(jnp.maximum(start, 0), 16) * 16, 0, LEN - WINDOW)
        hit = (start > -PROPS) & (start < LEN)
        return start, pl.multiple_of(base, 16), hit

    def copy_in(b, base):
        return pltpu.make_async_copy(
            keys.at[b, pl.ds(base, WINDOW), :], buf.at[b], in_sem.at[b]
        )

    def copy_out(b, base):
        return pltpu.make_async_copy(
            buf.at[b], keys.at[b, pl.ds(base, WINDOW), :], out_sem.at[b]
        )

    @pl.loop(0, SEQS)
    def _(b):
        start, base, hit = place(b)

        @pl.when(hit)
        def _():
            copy_in(b, base).start()

    for move in moves:
        move[0].start()
    coded = joined[STATS].astype(f32)
    columns[...] = jnp.transpose(coded[0:8] + coded[8:16])

    def patched(b, start, base):
        inv = columns[pl.ds(pl.multiple_of(PROPS * b, PROPS), PROPS), 2:3]
        slot = iota((WINDOW, PROPS), 0) + (base - start)
        selector = jnp.where(slot == iota((WINDOW, PROPS), 1), 1.0, 0.0).astype(bf16)
        raw = joined[b, :, WIDTH:].astype(f32)
        rows = jnp.dot(selector, (inv * raw).astype(bf16), preferred_element_type=f32)
        slot = iota((WINDOW, WIDTH), 0) + (base - start)
        return (slot >= 0) & (slot < PROPS), rows

    for t in range(8):
        moves[t][0].wait()

        @pl.loop(3 * t, 3 * t + 3)
        def _(b):
            start, base, hit = place(b)

            @pl.when(hit)
            def _():
                inside, rows = patched(b, start, base)
                window = pl.ds(base, WINDOW)
                held = near[b, window, :].astype(f32)
                near[b, window, :] = jnp.where(inside, rows[:, WIDTH:], held).astype(bf16)
                copy_in(b, base).wait()
                held = buf[b].astype(f32)
                buf[b] = jnp.where(inside, rows[:, 0:WIDTH], held).astype(bf16)
                copy_out(b, base).start()

        moves[t][1].start()
    for move in moves:
        move[1].wait()

    @pl.loop(0, SEQS)
    def _(b):
        start, base, hit = place(b)

        @pl.when(hit)
        def _():
            copy_out(b, base).wait()


def shards(
    tokens,
    norm_gain,
    w_query,
    w_key,
    w_value,
    w_gate,
    gate_bias,
    w_out,
    keys_cache,
    values_cache,
    cum_gates,
    prior_len,
    accepted,
    parents,
):
    cache = jax.ShapeDtypeStruct(keys_cache.shape, bf16)

    def near(*arrays):
        return [pltpu.with_memory_space_constraint(a, pltpu.VMEM) for a in arrays]

    def far(*arrays):
        return [pltpu.with_memory_space_constraint(a, pltpu.HBM) for a in arrays]

    def limit(mib):
        return pltpu.CompilerParams(vmem_limit_bytes=mib << 20)

    parts, biases = pl.pallas_call(
        project_kernel,
        out_shape=(
            jax.ShapeDtypeStruct((N_KV, PROPS, ROWS), bf16),
            jax.ShapeDtypeStruct(cum_gates.shape, f32),
        ),
        in_specs=[SM, SM, VM, VM, VM, VM, VM, VM, VM],
        out_specs=(VM, VM),
        scratch_shapes=[pltpu.VMEM((16, ROWS), f32)],
        name="project",
    )(
        prior_len,
        accepted,
        tokens.T,
        norm_gain[None],
        w_query,
        w_key,
        w_value,
        w_gate.T,
        cum_gates,
    )
    arrived = lax.all_to_all(parts, KV, 0, 0, tiled=True)

    tp_count = lax.axis_size("tp")

    def across(x, bit):
        return lax.ppermute(x, "tp", [(i, i ^ bit) for i in range(tp_count)])

    w_0 = w_out.T
    w_4 = across(w_0, 4)
    w_2 = across(w_0, 2)
    w_6 = across(w_4, 2)
    w_even = pl.pallas_call(
        join_kernel,
        out_shape=jax.ShapeDtypeStruct((4, *w_0.shape), bf16),
        in_specs=[VM] * 4 + [ANY],
        out_specs=VM,
        compiler_params=limit(2),
        name="four",
    )(*far(w_0, w_4, w_2, w_6, parts))

    block = pl.pallas_call(
        share_kernel,
        out_shape=pltpu.VMEM((N_KV, PROPS, ROWS), bf16),
        in_specs=[SM, VM, ANY],
        out_specs=VM,
        compiler_params=limit(8),
        cost_estimate=pl.CostEstimate(
            flops=10_000_000_000, bytes_accessed=800_000, transcendentals=0
        ),
        name="share",
    )(*far(gate_bias), *near(arrived), *far(w_even))
    joined = lax.all_to_all(block, KV, 0, 0, tiled=True)

    sent, keys_copy = pl.pallas_call(
        attention_kernel,
        out_shape=(pltpu.VMEM((512, WIDTH), bf16), cache),
        in_specs=[SM, VM, VM, VM, VM],
        out_specs=(VM, ANY),
        scratch_shapes=[
            pltpu.VMEM((ROWS, 8), f32),
            pltpu.VMEM((SEQS, 2 * PROPS, LEN), f32),
            pltpu.VMEM((SEQS, 2 * PROPS, LEN), bf16),
            pltpu.VMEM((SEQS, 2 * PROPS, WIDTH), f32),
            pltpu.VMEM((SEQS, 2 * PROPS, WIDTH), f32),
            pltpu.VMEM((512, WIDTH), f32),
            pltpu.SemaphoreType.DMA((4,)),
        ],
        compiler_params=limit(12),
        name="attention",
    )(*far(parents.T), *near(joined, biases, keys_cache, values_cache))
    pieces = lax.all_to_all(sent.reshape(256, 2, WIDTH), (*KV, "tp"), 0, 0, tiled=True)

    combined = pl.pallas_call(
        combine_kernel,
        out_shape=jax.ShapeDtypeStruct((N_KV, PROPS, WIDTH), bf16),
        in_specs=[VM],
        out_specs=VM,
        scratch_shapes=[pltpu.VMEM((64, 8, WIDTH), f32), pltpu.VMEM((64, 8, WIDTH), f32)],
        compiler_params=limit(8),
        name="combine",
    )(*near(pieces.reshape(512, WIDTH)))
    shared = lax.all_to_all(combined, KV, 0, 0, tiled=True)
    w_odd = across(w_even, 1)

    keys_out, values_out = pl.pallas_call(
        write_kernel,
        out_shape=(cache, cache),
        in_specs=[SM, SM, VM, ANY, ANY, ANY],
        out_specs=(ANY, ANY),
        input_output_aliases={4: 0},
        scratch_shapes=[
            pltpu.VMEM((SEQS, WINDOW, WIDTH), bf16),
            pltpu.VMEM(keys_cache.shape, bf16),
            pltpu.VMEM((ROWS, 8), f32),
            pltpu.SemaphoreType.DMA((SEQS,)),
            pltpu.SemaphoreType.DMA((SEQS,)),
            pltpu.SemaphoreType.DMA((2, 8)),
        ],
        compiler_params=limit(8),
        cost_estimate=pl.CostEstimate(
            flops=2_000_000_000, bytes_accessed=100_000, transcendentals=0
        ),
        name="write",
    )(
        *far(prior_len, accepted),
        *near(joined),
        *far(combined, keys_copy, values_cache),
    )

    mixed_rows = pl.pallas_call(
        output_kernel,
        out_shape=jax.ShapeDtypeStruct((48, 64), bf16),
        in_specs=[VM] * 3,
        out_specs=VM,
        scratch_shapes=[pltpu.VMEM((512, WIDTH), f32)],
        compiler_params=limit(8),
        name="output",
    )(*near(shared.reshape(512, WIDTH), w_even, w_odd))
    return (mixed_rows, keys_out, values_out)


def solution(mesh):
    torus = Mesh(mesh.devices.reshape(8, 4, mesh.shape["tp"]), ("kv_0", "kv_1", "tp"))
    in_specs = (
        P(None, KV),
        P(KV),
        P(KV, "tp"),
        P(KV, "tp"),
        P(KV, "tp"),
        P(),
        P(),
        P("tp", KV),
        P(None, KV, "tp"),
        P(None, KV, "tp"),
        P(None, "tp", KV),
        P(),
        P(),
        P(),
    )
    out_specs = (P("tp", KV), P(None, KV, "tp"), P(None, KV, "tp"))
    return jax.shard_map(
        shards, mesh=torus, in_specs=in_specs, out_specs=out_specs, check_vma=False
    )
```
